32 devices in a mesh: grp: 2 (over y), fs: 4 (over z), tp: 4 (over x, core).
Axes of the slice: x: 2, y: 2, z: 4, core: 2. Of those that a mesh axis runs over, the one named last changes fastest.
Arguments:
- tokens: bfloat16 [3072, 2048], P(('grp', 'fs'), 'tp'), parts along dimension 0, may hold values from -6 to 6
- norm_gain: float32 [2048], P('fs'), may hold values from 0.1 to 1.9
- gate_weight: float32 [4, 2048, 1024], P(None, 'fs', 'tp'), may hold values from -0.125 to 0.125
- up_weight: float32 [4, 2048, 1024], P(None, 'fs', 'tp'), may hold values from -0.125 to 0.125
- down_weight: float32 [4, 2048, 1024], P(None, 'fs', 'tp'), may hold values from -0.5 to 0.5
- expert_ids: int32 [3072, 2], P(('grp', 'fs')), parts along dimension 0, may hold values from 0 to 3, as said below
- group_logits: float32 [3072, 2], P(('grp', 'fs')), parts along dimension 0, may hold values from -2.5 to 2.5
- pair_logits: float32 [3072, 2], P(('grp', 'fs')), parts along dimension 0, may hold values from -2.5 to 2.5
Outputs:
- mixed: bfloat16 [3072, 2048], P(('grp', 'fs'), 'tp'), parts along dimension 0
- gate_out: bfloat16 [8, 2048, 1024], P(('grp', 'fs'), None, 'tp'), parts along dimension 0
- up_out: bfloat16 [8, 2048, 1024], P(('grp', 'fs'), None, 'tp'), parts along dimension 0
- down_out: bfloat16 [8, 2048, 1024], P(('grp', 'fs'), None, 'tp'), parts along dimension 0
The draws below stay inside these ranges and needn't reach their ends.
There are 2 independent parts, one for each index of `grp`. The reference program is written for one: setup_inputs(seed, part) draws one part's arguments, and reference() takes and returns one part's arrays. A program takes and returns all parts, laid end to end along the dimension named above; an argument that names none is the same for every part. Nothing has to cross between parts.
Inputs may be any that keep to these rules, and one draw needn't show every extreme that they name: `expert_ids`: each row names two different experts of one group: both ids lie in the same run of 2 consecutive ids.
All inputs are finite; a program needn't handle non-finite values.
Results may differ from the reference program's by a relative error of at most 0.015.
Values may be sent and summed in bfloat16 or wider, within the bound.
A program may use at most 64 MiB of HBM per device.

```python
from functools import partial
import jax
import jax.numpy as jnp
from jax import lax

D = 2048
FF = 1024
GROUPS = 2
TOP = 2
TOK_DEV = 384
EXPERTS = 4
EXP_GROUP = 2
CAP = 240
TOKENS = 1536
N_FS = 4
N_TP = 4


def pick_by_weight(key, table):
    running = jnp.cumsum(table, axis=1)
    total = running[:, -1]
    draw = jax.random.randint(key, (table.shape[0],), 0, 1 << 30) % total
    return jnp.sum((running <= draw[:, None]).astype(jnp.int32), axis=1).astype(jnp.int32)


def draw_expert_ids(key, part):
    base = jax.random.fold_in(key, 11)
    key_hot, key_first, key_second = jax.random.split(base, 3)
    block_count = TOKENS // TOK_DEV
    block_keys = jax.random.split(key_hot, block_count)
    orders = jax.vmap(lambda single: jax.random.permutation(single, EXPERTS))(block_keys)
    block_table = 1 + 2 * (orders < EXPERTS // 2).astype(jnp.int32)
    token_block = jnp.arange(TOKENS, dtype=jnp.int32) // TOK_DEV
    token_table = block_table[token_block]
    first_pick = pick_by_weight(key_first, token_table)
    columns = jnp.arange(EXPERTS, dtype=jnp.int32)
    allowed = (columns[None, :] // EXP_GROUP == (first_pick // EXP_GROUP)[:, None]) & (columns[None, :] != first_pick[:, None])
    second_table = token_table * allowed.astype(jnp.int32)
    second_pick = pick_by_weight(key_second, second_table)
    return jnp.stack([first_pick, second_pick], axis=1).astype(jnp.int32)


def draw_tokens(key, part):
    base = jax.random.fold_in(key, 21)
    raw = jnp.clip(jax.random.normal(base, (TOKENS, D), jnp.float32), -3.0, 3.0)
    factor = 1.0 / jnp.sqrt(jnp.mean(raw * raw, axis=1, keepdims=True) + 1e-06)
    return jnp.clip(raw * factor, -6.0, 6.0).astype(jnp.bfloat16)


def draw_group_logits(key, part):
    base = jax.random.fold_in(key, 31)
    values = jnp.clip(0.6 * jax.random.normal(base, (TOKENS, GROUPS), jnp.float32), -2.5, 2.5)
    return values.astype(jnp.float32)


def draw_pair_logits(key, part):
    base = jax.random.fold_in(key, 41)
    values = jnp.clip(0.6 * jax.random.normal(base, (TOKENS, TOP), jnp.float32), -2.5, 2.5)
    return values.astype(jnp.float32)


def shard_levels(key, shape, cuts, low, high):
    def one(axis_at, blocks):
        steps = jax.random.uniform(jax.random.fold_in(jax.random.fold_in(key, 6), axis_at), (blocks,), jnp.float32, low / len(cuts), high / len(cuts))
        return jnp.repeat(jnp.exp(steps), shape[axis_at] // blocks).reshape((-1,) + (1,) * (len(shape) - axis_at - 1))

    level = one(*cuts[0])
    for cut in cuts[1:]:
        level = level * one(*cut)
    return level


def bell_draw(rng, extent, scale, most, cuts=(), kind=jnp.bfloat16):
    values = jax.random.normal(rng, extent, jnp.float32) * scale
    if len(cuts) > 0:
        values = shard_levels(rng, extent, cuts, -0.22, 0.18) * values
    return jnp.clip(values, min=-most, max=most).astype(kind)


def setup_inputs(seed: int = 0, part: int = 0) -> dict:
    key_of = jax.random.split(jax.random.key(seed), 9)
    own_keys = jax.random.split(jax.random.fold_in(key_of[8], part), 9)
    tokens = draw_tokens(jax.random.fold_in(jax.random.fold_in(key_of[8], part), 71), part)
    norm_gain = jnp.clip(1.0 + 0.18 * jax.random.normal(key_of[1], (D,), jnp.float32), 0.1, 1.9)
    gate_weight = bell_draw(key_of[2], (EXPERTS, D, FF), D ** -0.5, 0.125, ((1, 4), (2, 4)), jnp.float32)
    up_weight = bell_draw(key_of[3], (EXPERTS, D, FF), D ** -0.5, 0.125, ((1, 4), (2, 4)), jnp.float32)
    down_weight = bell_draw(key_of[4], (EXPERTS, D, FF), (FF // 8) ** -0.5, 0.5, ((1, 4), (2, 4)), jnp.float32)
    expert_ids = draw_expert_ids(jax.random.fold_in(jax.random.fold_in(key_of[8], part), 71), part)
    group_logits = draw_group_logits(jax.random.fold_in(jax.random.fold_in(key_of[8], part), 71), part)
    pair_logits = draw_pair_logits(jax.random.fold_in(jax.random.fold_in(key_of[8], part), 71), part)
    return dict(tokens=tokens, norm_gain=norm_gain, gate_weight=gate_weight, up_weight=up_weight, down_weight=down_weight, expert_ids=expert_ids, group_logits=group_logits, pair_logits=pair_logits)


def routing(block_ids, experts, capacity):
    entries = block_ids.reshape(-1).astype(jnp.int32)
    onehot = (entries[:, None] == jnp.arange(experts, dtype=jnp.int32)[None, :]).astype(jnp.int32)
    before = jnp.cumsum(onehot, axis=0) - onehot
    entry_rank = jnp.sum(before * onehot, axis=1)
    kept = entry_rank < capacity
    slot_index = jnp.where(kept, entries * capacity + entry_rank, experts * capacity)
    return slot_index.astype(jnp.int32), kept


def fill_slots(block_rows, slot_index, experts, capacity):
    entry_count = slot_index.shape[0]
    source_row = jnp.arange(entry_count, dtype=jnp.int32) // 2
    slot_row = jnp.zeros((experts * capacity + 1,), jnp.int32).at[slot_index].set(source_row)
    filled = jnp.zeros((experts * capacity + 1,), jnp.float32).at[slot_index].set(1.0)
    chosen = block_rows[slot_row[:experts * capacity]]
    return chosen * filled[:experts * capacity, None].astype(block_rows.dtype)


def route_weights(block_ids, group_logits, pair_logits, kept, exp_group):
    group_pick = block_ids[:, 0] // exp_group
    group_exp = jnp.exp(group_logits)
    columns = jnp.arange(group_logits.shape[1], dtype=jnp.int32)
    chosen = jnp.sum(jnp.where(columns[None, :] == group_pick[:, None], group_exp, 0.0), axis=1)
    chosen = chosen / jnp.sum(group_exp, axis=1)
    pair_exp = jnp.exp(pair_logits)
    weights = pair_exp / jnp.sum(pair_exp, axis=1, keepdims=True) * chosen[:, None]
    return weights * kept.reshape(-1, 2).astype(weights.dtype)


def expert_apply(operands):
    slot_rows, gate_matrix, up_matrix, down_matrix = operands
    gate = jnp.dot(slot_rows, gate_matrix, preferred_element_type=jnp.float32)
    up_part = jnp.dot(slot_rows, up_matrix, preferred_element_type=jnp.float32)
    hidden = (jax.nn.silu(gate) * up_part).astype(jnp.bfloat16)
    width = FF // N_TP
    total = jnp.zeros((slot_rows.shape[0], D), jnp.float32)
    for column in range(N_TP):
        term = lax.dot_general(hidden[:, column * width:(column + 1) * width],
                               down_matrix[:, column * width:(column + 1) * width],
                               (((1,), (1,)), ((), ())), preferred_element_type=jnp.float32)
        rounded = lax.optimization_barrier(term.astype(jnp.bfloat16))
        total = total + rounded.astype(jnp.float32)
    return total.astype(jnp.bfloat16)


def combine_block(returned, slot_index, weights):
    limit = returned.shape[0] - 1
    picked = returned[jnp.clip(slot_index, 0, limit)].astype(jnp.float32)
    picked = picked.reshape(weights.shape[0], 2, -1)
    return jnp.sum(picked * weights[:, :, None], axis=1).astype(jnp.bfloat16)


def reference(tokens, norm_gain, gate_weight, up_weight, down_weight, expert_ids, group_logits, pair_logits):
    scaled = norm_gain[None, :, None]
    gate_out = (scaled * gate_weight).astype(jnp.bfloat16)
    up_out = (scaled * up_weight).astype(jnp.bfloat16)
    down_out = down_weight.astype(jnp.bfloat16)
    id_blocks = expert_ids.reshape(N_FS, TOK_DEV, 2)
    token_blocks = tokens.reshape(N_FS, TOK_DEV, D)
    slot_index, kept = jax.vmap(partial(routing, experts=EXPERTS, capacity=CAP))(id_blocks)
    buffers = jax.vmap(partial(fill_slots, experts=EXPERTS, capacity=CAP))(token_blocks, slot_index)
    buffers = buffers.reshape(N_FS, EXPERTS, CAP, D).transpose(1, 0, 2, 3).reshape(EXPERTS, N_FS * CAP, D)
    results = lax.map(expert_apply, (buffers, gate_out, up_out, down_out))
    results = results.reshape(EXPERTS, N_FS, CAP, D).transpose(1, 0, 2, 3).reshape(N_FS, EXPERTS * CAP, D)
    weights = jax.vmap(partial(route_weights, exp_group=EXP_GROUP))(
        id_blocks, group_logits.reshape(N_FS, TOK_DEV, -1), pair_logits.reshape(N_FS, TOK_DEV, 2), kept)
    mixed = jax.vmap(combine_block)(results, slot_index, weights)
    return (mixed.reshape(TOKENS, D), gate_out, up_out, down_out)
```

```python
import functools

import jax
import jax.numpy as jnp
from jax import lax
from jax.experimental import pallas as pl
from jax.experimental.pallas import tpu as pltpu
from jax.sharding import PartitionSpec as P

MESH = pl.DeviceIdType.MESH
BF16 = jnp.bfloat16
F32 = jnp.float32


def each(count, step):
    if count <= 4:
        for i in range(count):
            step(i)
    else:
        lax.fori_loop(0, count, lambda i, c: (step(i), c)[1], 0)


def exchange_kernel(
    n_grp, n_fs, n_tp, capacity,
    tokens, gain, id_rows, group_logits, pair_logits, gate_in, up_in, down_in,
    mixed, gate_out, up_out, down_out,
    out_ref, raw, cast, ret, mix, piece, hidden, own, pair_send, pair_recv, x_send, x_recv, result,
    local_sem, raw_sem, slot_s, slot_r, wz_s, wz_r, wy_s, wy_r,
    gx_s, gx_r, gd_s, gd_r, gf_s, gf_r, pr_s, pr_r, xx_s, xx_r, rt_s, rt_r,
):
    g, f, t = lax.axis_index("grp"), lax.axis_index("fs"), lax.axis_index("tp")
    n_x = n_tp // 2
    chip, core = t // 2, lax.rem(t, 2)
    partner = chip * 2 + 1 - core
    width = piece.shape[3]
    block = cast.shape[2]
    tok_rows, padded = tokens.shape[0], out_ref.shape[1]
    experts = n_fs
    share = block // n_grp

    def fs_at(k):
        return lax.rem(f + k, n_fs)

    def outward(i):
        return jnp.where(f < n_fs // 2, i + 1, n_fs - 1 - i)

    def nearest(i):
        if n_fs != 4:
            return outward(i)
        first = jnp.where(f % 2 == 0, 1, 3)
        last = jnp.where(f == 0, 3, jnp.where(f == 3, 1, 2))
        return (first, 6 - first - last, last)[i]

    def grp_at(k):
        return lax.rem(g + k, n_grp)

    def chip_at(k):
        return lax.rem(chip + k, n_x)

    def rcopy(src, dst, ssem, rsem, axis, peer):
        return pltpu.make_async_remote_copy(
            src_ref=src, dst_ref=dst, send_sem=ssem, recv_sem=rsem,
            device_id={axis: peer}, device_id_type=MESH,
        )

    raw_copies = [
        pltpu.make_async_copy(w, raw.at[m], raw_sem.at[m])
        for m, w in enumerate((gate_in, up_in, down_in))
    ]
    for copy in raw_copies:
        copy.start()

    barrier = pltpu.get_barrier_semaphore()

    def greet(axis, peer):
        pl.semaphore_signal(barrier, inc=1, device_id={axis: peer}, device_id_type=MESH)

    each(n_fs - 1, lambda i: greet("fs", fs_at(i + 1)))
    each(n_grp - 1, lambda i: greet("grp", grp_at(i + 1)))
    each(n_x - 1, lambda i: greet("tp", chip_at(i + 1) * 2 + core))
    greet("tp", partner)

    def ints(shape, axis):
        return lax.broadcasted_iota(jnp.int32, shape, axis)

    def route(ids, axis):
        shape = (experts, tok_rows) if axis == 0 else (tok_rows, experts)
        named = [(ints(shape, axis) == i).astype(F32) for i in ids]
        square = (tok_rows, tok_rows)
        earlier = (ints(square, axis) < ints(square, 1 - axis)).astype(F32).astype(BF16)
        both = (named[0] + named[1]).astype(BF16)
        pair = (both, earlier) if axis == 0 else (earlier, both)
        before = jnp.dot(*pair, preferred_element_type=F32)
        picks, kept = [], []
        for i, name in zip(ids, named):
            rank = jnp.sum(before * name, axis=axis, keepdims=True)
            kept.append(rank < capacity)
            slot = i * padded + rank.astype(jnp.int32)
            picks.append(jnp.where(rank < capacity, slot, -1))
        return picks, kept

    row_picks, _ = route([id_rows[0:1, :], id_rows[1:2, :]], 0)

    def fill(k):
        e = fs_at(k)
        slot = ints((padded, tok_rows), 0) + e * padded
        named = (slot == row_picks[0]) | (slot == row_picks[1])
        place = jnp.where(named, 1.0, 0.0).astype(BF16)
        out_ref[e] = jnp.dot(place, tokens[...], preferred_element_type=F32).astype(BF16)

    each(n_fs - 1, lambda i: fill(i + 1))
    pl.semaphore_wait(barrier, n_fs - 1 + n_grp - 1 + n_x - 1 + 1)

    weights = (
        (cast.at[0], gate_out), (cast.at[1], up_out), (cast.at[2], down_out)
    )

    def slot_copy(k, source):
        return rcopy(out_ref.at[fs_at(k)], piece.at[t, source], slot_s.at[k],
                     slot_r.at[n_fs - k], "fs", fs_at(k))

    def slot_arrival(k):
        return rcopy(out_ref.at[f], piece.at[t, fs_at(k)], slot_s.at[k], slot_r.at[k], "fs", fs_at(k))

    each(n_fs - 1, lambda i: slot_copy(outward(i), f).start())
    fill(0)
    own_slots = pltpu.make_async_copy(out_ref.at[f], piece.at[t, f], local_sem.at[3])
    own_slots.start()

    def w_rows(source, part):
        return pl.ds(source * block + part * share, share)

    def wz_copy(m, k):
        w_in, w_out = weights[m]
        return rcopy(w_in.at[fs_at(k), pl.ds(g * share, share)], w_out.at[w_rows(f, g)],
                     wz_s.at[m, k], wz_r.at[m, n_fs - k], "fs", fs_at(k))

    def wz_arrival(m, k):
        w_in, w_out = weights[m]
        return rcopy(w_in.at[fs_at(k), pl.ds(g * share, share)], w_out.at[w_rows(fs_at(k), g)],
                     wz_s.at[m, k], wz_r.at[m, k], "fs", fs_at(k))

    def wy_copy(m, k, j):
        w_out = weights[m][1]
        rows = w_rows(fs_at(k), g)
        return rcopy(w_out.at[rows], w_out.at[rows], wy_s.at[m, k, j],
                     wy_r.at[m, k, n_grp - j], "grp", grp_at(j))

    def wy_arrival(m, k, j):
        w_out = weights[m][1]
        rows = w_rows(fs_at(k), grp_at(j))
        return rcopy(w_out.at[rows], w_out.at[rows], wy_s.at[m, k, j],
                     wy_r.at[m, k, j], "grp", grp_at(j))

    own_weights = []
    for m in range(3):
        w_in, w_out = weights[m]
        raw_copies[m].wait()

        def round_block(e):
            if m < 2:
                cast[m, e] = (gain[...] * raw[m, e]).astype(BF16)
            else:
                cast[m, e] = raw[m, e].astype(BF16)

        each(n_fs, round_block)
        copy = pltpu.make_async_copy(w_in.at[f], w_out.at[pl.ds(f * block, block)], local_sem.at[m])
        copy.start()
        own_weights.append(copy)

    for m in range(3):
        each(n_fs - 1, lambda i: wz_copy(m, outward(i)).start())

    def forward(m, k):
        wz_arrival(m, k).wait_recv()
        for j in range(1, n_grp):
            wy_copy(m, k, j).start()

    def gx_copy(k, j):
        src = piece.at[t, fs_at(k)]
        return rcopy(src, src, gx_s.at[k, j], gx_r.at[k, n_x - j], "tp", chip_at(j) * 2 + core)

    def gx_arrival(k, j):
        src = piece.at[chip_at(j) * 2 + core, fs_at(k)]
        return rcopy(src, src, gx_s.at[k, j], gx_r.at[k, j], "tp", chip_at(j) * 2 + core)

    def gd_copy(k):
        src = piece.at[t, fs_at(k)]
        return rcopy(src, src, gd_s.at[k], gd_r.at[k], "tp", partner)

    def gd_arrival(k):
        src = piece.at[partner, fs_at(k)]
        return rcopy(src, src, gd_s.at[k], gd_r.at[k], "tp", partner)

    def gf_copy(k, j):
        src = piece.at[chip_at(j) * 2 + core, fs_at(k)]
        return rcopy(src, src, gf_s.at[k, j], gf_r.at[k, j], "tp", partner)

    def gf_arrival(k, j):
        src = piece.at[chip_at(j) * 2 + 1 - core, fs_at(k)]
        return rcopy(src, src, gf_s.at[k, j], gf_r.at[k, j], "tp", partner)

    def spread(k):
        for j in range(1, n_x):
            gx_copy(k, j).start()
        gd_copy(k).start()

    own_slots.wait()
    spread(0)

    id_cols = jnp.transpose(id_rows[...])
    ids = [id_cols[:, k : k + 1] for k in range(2)]
    picks, kept = route(ids, 1)
    group_exp = jnp.exp(jnp.transpose(group_logits[...]))
    group_count = group_exp.shape[1]
    low = ints(group_exp.shape, 1) * (experts // group_count)
    member = (ids[0] >= low) & (ids[0] < low + experts // group_count)
    chosen = jnp.sum(jnp.where(member, group_exp, 0.0), axis=1, keepdims=True)
    chosen = chosen / jnp.sum(group_exp, axis=1, keepdims=True)
    pair_exp = jnp.exp(jnp.transpose(pair_logits[...]))
    pair_weight = pair_exp / jnp.sum(pair_exp, axis=1, keepdims=True) * chosen
    mix_weights = [
        jnp.where(kept[k], pair_weight[:, k : k + 1], 0.0) for k in range(2)
    ]

    def blend(k):
        e = fs_at(k)
        slot = ints((tok_rows, padded), 1) + e * padded
        named = (slot == picks[0]) | (slot == picks[1])
        place = jnp.where(named, 1.0, 0.0).astype(BF16)
        weight = jnp.where(ids[0] == e, mix_weights[0], 0.0)
        weight = weight + jnp.where(ids[1] == e, mix_weights[1], 0.0)
        return jnp.dot(place, ret[e], preferred_element_type=F32) * weight

    def spread_arrived(i):
        slot_arrival(nearest(i)).wait_recv()
        spread(nearest(i))

    each(n_fs - 1, spread_arrived)

    def hand_over(k):
        for j in range(1, n_x):
            gx_arrival(k, j).wait_recv()
            gf_copy(k, j).start()

    hand_over(0)

    each(n_fs - 1, lambda i: hand_over(nearest(i)))

    for m in range(3):
        each(n_fs - 1, lambda i: forward(m, nearest(i)))

    def all_in(m):
        own_weights[m].wait()
        for j in range(1, n_grp):
            each(n_fs - 1, lambda i: wy_arrival(m, i + 1, j).wait_recv())

    all_in(0)
    all_in(1)

    def make_hidden(k):
        source = fs_at(k)
        gd_arrival(k).wait_recv()
        for j in range(1, n_x):
            gf_arrival(k, j).wait_recv()
        gate = up = None
        for p in range(n_tp):
            rows = piece[p, source]
            cols = pl.ds(p * width, width)
            gate_part = jnp.dot(rows, gate_out[cols, :], preferred_element_type=F32)
            up_part = jnp.dot(rows, up_out[cols, :], preferred_element_type=F32)
            gate = gate_part if gate is None else gate + gate_part
            up = up_part if up is None else up + up_part
        hidden[k] = (gate / (1.0 + jnp.exp(-gate)) * up).astype(BF16)

    each(n_fs, lambda i: make_hidden(i))
    all_in(2)

    def term(k, j, to_core):
        column = (chip_at(j) * 2 + to_core) * width
        rows = down_out[pl.ds(pl.multiple_of(column, width), width), :]
        return lax.dot_general(hidden[k], rows, (((1,), (1,)), ((), ())), preferred_element_type=F32)

    def pr_copy(k):
        return rcopy(pair_send.at[k], pair_recv.at[k], pr_s.at[k], pr_r.at[k], "tp", partner)

    def stage_pair(k):
        for j in range(n_x):
            pair_send[k, j] = term(k, j, 1 - core).astype(BF16)
        pr_copy(k).start()
        for j in range(n_x):
            own[k, j] = term(k, j, core)

    def xx_copy(k, j):
        return rcopy(x_send.at[k, j], x_recv.at[k, n_x - j], xx_s.at[k, j], xx_r.at[k, n_x - j],
                     "tp", chip_at(j) * 2 + core)

    def xx_arrival(k, j):
        return rcopy(x_send.at[k, j], x_recv.at[k, j], xx_s.at[k, j], xx_r.at[k, j],
                     "tp", chip_at(j) * 2 + core)

    def stage_chip(k):
        pr_copy(k).wait_recv()
        for j in range(1, n_x):
            x_send[k, j] = (own[k, j] + pair_recv[k, j].astype(F32)).astype(BF16)
            xx_copy(k, j).start()
        own[k, 0] = own[k, 0] + pair_recv[k, 0].astype(F32)

    def rt_copy(k):
        return rcopy(result.at[k], ret.at[f], rt_s.at[k], rt_r.at[n_fs - k], "fs", fs_at(k))

    def rt_arrival(k):
        return rcopy(result.at[k], ret.at[fs_at(k)], rt_s.at[k], rt_r.at[k], "fs", fs_at(k))

    def total(k):
        acc = own[k, 0]
        for j in range(1, n_x):
            xx_arrival(k, j).wait_recv()
            acc = acc + x_recv[k, j].astype(F32)
        return acc.astype(BF16)

    def stage_home(k):
        result[k] = total(k)
        rt_copy(k).start()

    def order(i):
        return lax.rem(outward(i) + n_fs, n_fs)

    stage_pair(order(0))

    def pair_and_chip(i):
        stage_pair(order(i + 1))
        stage_chip(order(i))

    each(n_fs - 1, pair_and_chip)
    stage_chip(order(n_fs - 1))
    each(n_fs - 1, lambda i: stage_home(order(i)))
    ret[f] = total(0)
    mix[...] = blend(0)

    def collect(i):
        k = nearest(i)
        rt_arrival(k).wait_recv()
        mix[...] += blend(k)

    each(n_fs - 1, collect)
    mixed[...] = mix[...].astype(BF16)

    def drain_peer(i):
        k = i + 1
        slot_copy(k, f).wait_send()
        rt_copy(k).wait_send()
        for m in range(3):
            wz_copy(m, k).wait_send()
            for j in range(1, n_grp):
                wy_copy(m, k, j).wait_send()

    def drain_chunk(k):
        gd_copy(k).wait_send()
        pr_copy(k).wait_send()
        for j in range(1, n_x):
            gx_copy(k, j).wait_send()
            gf_copy(k, j).wait_send()
            xx_copy(k, j).wait_send()

    each(n_fs - 1, drain_peer)
    each(n_fs, drain_chunk)


def body(
    tokens, norm_gain, gate_weight, up_weight, down_weight, expert_ids, group_logits, pair_logits
):
    n_grp, n_fs, n_tp = (lax.axis_size(a) for a in ("grp", "fs", "tp"))
    n_x = n_tp // 2
    experts, block, hid = gate_weight.shape
    tok_rows, width = tokens.shape
    capacity = 5 * tok_rows * 2 // (4 * experts)
    cap = -(-capacity // 16) * 16
    vmem = pl.BlockSpec(memory_space=pltpu.VMEM)
    hbm = pl.BlockSpec(memory_space=pl.ANY)
    dma = pltpu.SemaphoreType.DMA
    matrix = jax.ShapeDtypeStruct((n_fs * block, hid), BF16)
    chunk = (n_fs, n_x, cap, width)
    sem_shapes = [
        (4,), (3,), (n_fs,), (n_fs,), (3, n_fs), (3, n_fs), (3, n_fs, n_grp), (3, n_fs, n_grp),
        (n_fs, n_x), (n_fs, n_x), (n_fs,), (n_fs,), (n_fs, n_x), (n_fs, n_x),
        (n_fs,), (n_fs,), (n_fs, n_x), (n_fs, n_x), (n_fs,), (n_fs,),
    ]
    mixed, *matrices = pl.pallas_call(
        functools.partial(exchange_kernel, n_grp, n_fs, n_tp, capacity),
        out_shape=(jax.ShapeDtypeStruct((tok_rows, width), BF16), matrix, matrix, matrix),
        in_specs=[vmem] * 5 + [hbm] * 3,
        out_specs=(vmem,) * 4,
        scratch_shapes=[
            pltpu.VMEM((n_fs, cap, width), BF16),
            pltpu.VMEM((3, n_fs, block, hid), F32),
            pltpu.VMEM((3, n_fs, block, hid), BF16),
            pltpu.VMEM((n_fs, cap, width), BF16),
            pltpu.VMEM((tok_rows, width), F32),
            pltpu.VMEM((n_tp, n_fs, cap, width), BF16),
            pltpu.VMEM((n_fs, cap, hid), BF16),
            pltpu.VMEM(chunk, F32),
            pltpu.VMEM(chunk, BF16),
            pltpu.VMEM(chunk, BF16),
            pltpu.VMEM(chunk, BF16),
            pltpu.VMEM(chunk, BF16),
            pltpu.VMEM((n_fs, cap, width), BF16),
        ] + [dma(s) for s in sem_shapes],
        compiler_params=pltpu.CompilerParams(
            collective_id=0, has_side_effects=True, vmem_limit_bytes=48 * 1024 * 1024
        ),
    )(
        tokens, norm_gain[:, None], expert_ids.T, group_logits.T, pair_logits.T,
        gate_weight, up_weight, down_weight,
    )
    return (mixed, *(m[None] for m in matrices))


def pair_kernel(
    n_grp, n_fs, n_tp, capacity,
    tokens_in, gain_in, ids_in, group_in, pair_in, gate_in, up_in, down_in,
    mixed, gate_out, up_out, down_out,
    tokens, gain, id_rows, group_logits, pair_logits, gain_col,
    raw_own, raw_far, cast, slots, place, back_place, wsend, wrecv, wcol,
    piece, acc, hid, dwn, part_send, part_recv, keep, home_send, home, own_home, mix,
    in_sem, raw_sem,
    sl_s, sl_r, wm_s, wm_r, wz_s, wz_r, wy_s, wy_r, tx_s, tx_r, td_s, td_r, tf_s, tf_r,
    dw_s, dw_r, hx_s, hx_r, hd_s, hd_r, hf_s, hf_r, pt_s, pt_r, hm_s, hm_r,
):
    g, f, t = lax.axis_index("grp"), lax.axis_index("fs"), lax.axis_index("tp")
    cap, width = piece.shape[2], piece.shape[3]
    block, hidden_units = raw_own.shape[1], raw_own.shape[2]
    share = raw_far.shape[2]
    tok_rows = tokens.shape[0]
    lanes = place.shape[1]
    pair = n_fs // 2

    def flip(i, k):
        return (i, i + 1 - 2 * lax.rem(i, 2), lax.rem(i + 2, 4), 3 - i)[k]

    def fs_at(k):
        return flip(f, k)

    def tp_at(j):
        return flip(t, j)

    other_grp = 1 - g

    def rcopy(src, dst, ssem, rsem, axis, peer):
        return pltpu.make_async_remote_copy(
            src_ref=src, dst_ref=dst, send_sem=ssem, recv_sem=rsem,
            device_id={axis: peer}, device_id_type=MESH,
        )

    small = [
        pltpu.make_async_copy(src, dst, in_sem.at[i])
        for i, (src, dst) in enumerate((
            (ids_in, id_rows), (tokens_in, tokens), (gain_in, gain),
            (group_in, group_logits), (pair_in, pair_logits),
        ))
    ]
    w_in = (gate_in, up_in, down_in)
    w_out = (gate_out, up_out, down_out)

    def far_load(m, k):
        return pltpu.make_async_copy(
            w_in[m].at[fs_at(k), pl.ds(g * share, share)], raw_far.at[m, k - 1], raw_sem.at[m, k]
        )

    def own_load(m):
        return pltpu.make_async_copy(w_in[m].at[f], raw_own.at[m], raw_sem.at[m, 0])

    for copy in small:
        copy.start()
    for m in (2, 0, 1):
        for k in (1, 2, 3):
            far_load(m, k).start()
    for m in (2, 0, 1):
        own_load(m).start()

    barrier = pltpu.get_barrier_semaphore()

    def greet(axis, peer):
        pl.semaphore_signal(barrier, inc=1, device_id={axis: peer}, device_id_type=MESH)

    for k in (1, 2, 3):
        greet("fs", fs_at(k))
        greet("tp", tp_at(k))
    greet("grp", other_grp)

    def ints(shape, axis):
        return lax.broadcasted_iota(jnp.int32, shape, axis)

    own_base = (f - lax.rem(f, 2))
    far_base = lax.rem(own_base + 2, 4)
    bases = (own_base, far_base)

    small[0].wait()
    first, second = id_rows[0:1, :], id_rows[1:2, :]
    members = [(first >= b) & (first < b + 2) for b in bases]
    square = (tok_rows, tok_rows)
    earlier = (ints(square, 0) < ints(square, 1)).astype(F32).astype(BF16)
    named = jnp.where(ints((8, tok_rows), 0) < 4, members[0].astype(F32), members[1].astype(F32))
    before = jnp.dot(named.astype(BF16), earlier, preferred_element_type=F32)
    ranks = [before[0:1, :], before[4:5, :]]
    kept = [m & (r < capacity) for m, r in zip(members, ranks)]
    seat = [jnp.where(k, r.astype(jnp.int32), -1) for k, r in zip(kept, ranks)]

    small[1].wait()

    def fill(i):
        one_hot = jnp.where(ints((lanes, tok_rows), 0) == seat[i], 1.0, 0.0)
        place[i] = one_hot.astype(BF16)
        rows = jnp.dot(place[i, 0:cap, :], tokens[...], preferred_element_type=F32).astype(BF16)
        slots[i] = rows
        return rows

    def slot_copy(k):
        src = slots.at[0] if k == 1 else slots.at[1]
        return rcopy(src, piece.at[t, k], sl_s.at[k], sl_r.at[k], "fs", fs_at(k))

    def relay_copy():
        return rcopy(piece.at[t, 2], piece.at[t, 3], sl_s.at[3], sl_r.at[3], "fs", fs_at(1))

    fill(1)
    pl.semaphore_wait(barrier, 3 + 3 + 1)
    slot_copy(2).start()
    piece[t, 0] = fill(0)
    slot_copy(1).start()

    def tx_copy(k):
        src = piece.at[t, k]
        return rcopy(src, src, tx_s.at[k], tx_r.at[k], "tp", tp_at(2))

    def td_copy(k):
        src = piece.at[t, k]
        return rcopy(src, src, td_s.at[k], td_r.at[k], "tp", tp_at(1))

    def tf_copy(k):
        src = piece.at[tp_at(2), k]
        return rcopy(src, src, tf_s.at[k], tf_r.at[k], "tp", tp_at(1))

    def tx_arrival(k):
        src = piece.at[tp_at(2), k]
        return rcopy(src, src, tx_s.at[k], tx_r.at[k], "tp", tp_at(2))

    def td_arrival(k):
        src = piece.at[tp_at(1), k]
        return rcopy(src, src, td_s.at[k], td_r.at[k], "tp", tp_at(1))

    def tf_arrival(k):
        src = piece.at[tp_at(3), k]
        return rcopy(src, src, tf_s.at[k], tf_r.at[k], "tp", tp_at(1))

    def spread(k):
        tx_copy(k).start()
        td_copy(k).start()

    spread(0)

    def w_rows(source, part):
        return pl.ds(source * block + part * share, share)

    def wz_copy(m, k):
        return rcopy(cast.at[m, k - 1], w_out[m].at[w_rows(f, g)],
                     wz_s.at[m, k], wz_r.at[m, k], "fs", fs_at(k))

    def wz_arrival(m, k):
        return rcopy(cast.at[m, k - 1], w_out[m].at[w_rows(fs_at(k), g)],
                     wz_s.at[m, k], wz_r.at[m, k], "fs", fs_at(k))

    def wy_copy(m, k):
        rows = w_out[m].at[w_rows(fs_at(k), g)]
        return rcopy(rows, rows, wy_s.at[m, k], wy_r.at[m, k], "grp", other_grp)

    def wy_arrival(m, k):
        rows = w_out[m].at[w_rows(fs_at(k), other_grp)]
        return rcopy(rows, rows, wy_s.at[m, k], wy_r.at[m, k], "grp", other_grp)

    small[2].wait()
    gain_col[...] = jnp.transpose(jnp.broadcast_to(gain[...], (8, block)))[:, 0:1]
    far_gain = gain_col[pl.ds(g * share, share), :]

    def send_far(m, k):
        far_load(m, k).wait()
        values = raw_far[m, k - 1]
        if m < 2:
            values = far_gain * values
        cast[m, k - 1] = values.astype(BF16)
        wz_copy(m, k).start()

    def round_own(m):
        own_load(m).wait()
        values = raw_own[m]
        if m < 2:
            values = gain_col[...] * values
        w_out[m][pl.ds(f * block, block), :] = values.astype(BF16)

    for k in (1, 2, 3):
        send_far(2, k)
    for m in (0, 1):
        send_far(m, 1)

    small[3].wait()
    small[4].wait()
    group_exp = jnp.exp(group_logits[...])
    group_sum = jnp.sum(group_exp, axis=0, keepdims=True)
    pair_exp = jnp.exp(pair_logits[...])
    pair_weight = pair_exp / jnp.sum(pair_exp, axis=0, keepdims=True)
    group_count = group_exp.shape[0]

    def wm_copy(k):
        return rcopy(wsend.at[k // 2], wrecv.at[k], wm_s.at[k], wm_r.at[k], "fs", fs_at(k))

    chosen = jnp.zeros_like(group_sum)
    for i in range(group_count):
        chosen = chosen + jnp.where((first >= 2 * i) & (first < 2 * i + 2), group_exp[i : i + 1, :], 0.0)
    mix_weight = pair_weight * (chosen / group_sum)
    for i in range(2):
        expert = bases[i] + ints((8, tok_rows), 0)
        rest = jnp.where(first == expert, mix_weight[0:1, :], 0.0)
        rest = rest + jnp.where(second == expert, mix_weight[1:2, :], 0.0)
        total = None
        for _ in range(3):
            head = rest.astype(BF16)
            rest = rest - head.astype(F32)
            term = lax.dot_general(head, place[i], (((1,), (1,)), ((), ())), preferred_element_type=F32)
            total = term if total is None else total + term
        wsend[i] = total
    for k in (1, 2, 3):
        wm_copy(k).start()

    for i in range(2):
        back_place[i] = jnp.transpose(place[i].astype(F32))[:, 0:cap].astype(BF16)

    def seat_weights(k, rows):
        cols = jnp.transpose(rows)
        wcol[k] = jnp.where(lax.rem(f, 2) == 0, cols[0:cap, 0:1], cols[0:cap, 1:2])

    seat_weights(0, wsend[0])
    round_own(2)

    def slot_arrival(k):
        return rcopy(slots.at[0], piece.at[t, k], sl_s.at[k], sl_r.at[k], "fs", fs_at(k))

    slot_arrival(2).wait_recv()
    relay_copy().start()
    spread(2)
    for k in (2, 3):
        for m in (0, 1):
            send_far(m, k)
    for m in (0, 1):
        round_own(m)
    slot_arrival(1).wait_recv()
    spread(1)

    def hand_over(k):
        tx_arrival(k).wait_recv()
        tf_copy(k).start()

    hand_over(0)
    for k in (1, 2, 3):
        wz_arrival(2, k).wait_recv()
        wy_copy(2, k).start()
    hand_over(2)
    hand_over(1)
    slot_arrival(3).wait_recv()
    spread(3)

    def dw_copy(j):
        src = down_out.at[pl.ds(tp_at(j) * block, block)]
        return rcopy(src, dwn.at[j], dw_s.at[j], dw_r.at[j], "tp", tp_at(j))

    for k in (1, 2, 3):
        wy_arrival(2, k).wait_recv()
    for j in (1, 2, 3):
        dw_copy(j).start()
    for k in (1, 2, 3):
        wm_copy(k).wait_recv()
        seat_weights(k, wrecv[k])

    for m in (0, 1):
        wz_arrival(m, 1).wait_recv()
        wy_copy(m, 1).start()
    hand_over(3)
    for k in (0, 2, 1, 3):
        td_arrival(k).wait_recv()
        tf_arrival(k).wait_recv()

    def products(k, source):
        rows = piece[source, k]
        cols = pl.ds(source * block, block)
        gate = jnp.dot(rows, gate_out[cols, :], preferred_element_type=F32)
        up = jnp.dot(rows, up_out[cols, :], preferred_element_type=F32)
        return gate, up

    def first_products(k, c):
        gate, up = products(k, f)
        acc[0, k], acc[1, k] = gate, up
        return c

    def more_products(kk):
        def step(k, c):
            gate, up = products(k, fs_at(kk))
            acc[0, k] += gate
            acc[1, k] += up
            return c
        return step

    lax.fori_loop(0, n_fs, first_products, 0)
    for m in (0, 1):
        wz_arrival(m, 2).wait_recv()
        wy_copy(m, 2).start()
    for m in (0, 1):
        wy_arrival(m, 1).wait_recv()
    lax.fori_loop(0, n_fs, more_products(1), 0)
    for m in (0, 1):
        wz_arrival(m, 3).wait_recv()
        wy_copy(m, 3).start()
    for m in (0, 1):
        wy_arrival(m, 2).wait_recv()
    lax.fori_loop(0, n_fs, more_products(2), 0)
    for m in (0, 1):
        wy_arrival(m, 3).wait_recv()

    def h_copy(j, k, ssem, rsem, source):
        return rcopy(hid.at[source, k], hid.at[source ^ j, k], ssem.at[k], rsem.at[k], "tp", tp_at(j))

    def hx_copy(k):
        return h_copy(2, k, hx_s, hx_r, 0)

    def hd_copy(k):
        return h_copy(1, k, hd_s, hd_r, 0)

    def hf_copy(k):
        return h_copy(1, k, hf_s, hf_r, 2)

    order = (3, 2, 1, 0)
    for k in order:
        gate, up = products(k, fs_at(3))
        gate = acc[0, k] + gate
        up = acc[1, k] + up
        hid[0, k] = (gate / (1.0 + jnp.exp(-gate)) * up * wcol[k]).astype(BF16)
        hx_copy(k).start()
        hd_copy(k).start()

    for j in (1, 2, 3):
        dw_copy(j).wait_recv()

    def pass_on(k):
        hx_copy(k).wait_recv()
        hf_copy(k).start()

    def result(k):
        hd_copy(k).wait_recv()
        hf_copy(k).wait_recv()
        total = None
        for j in range(n_tp):
            rows = down_out[pl.ds(t * block, block), :] if j == 0 else dwn[j]
            term = lax.dot_general(hid[j, k], rows, (((1,), (1,)), ((), ())), preferred_element_type=F32)
            total = term if total is None else total + term
        return total

    def part_copy(i):
        return rcopy(part_send.at[i], part_recv.at[i], pt_s.at[i], pt_r.at[i], "fs", fs_at(1))

    def home_copy():
        return rcopy(home_send, home, hm_s.at[0], hm_r.at[0], "fs", fs_at(2))

    pass_on(3)
    part_send[0] = result(3).astype(BF16)
    part_copy(0).start()
    pass_on(2)
    keep[...] = result(2)
    pass_on(1)
    part_send[1] = result(1).astype(BF16)
    part_copy(0).wait_recv()
    home_send[...] = (keep[...] + part_recv[0].astype(F32)).astype(BF16)
    home_copy().start()
    part_copy(1).start()
    pass_on(0)
    keep[...] = result(0)
    part_copy(1).wait_recv()
    own_home[...] = (keep[...] + part_recv[1].astype(F32)).astype(BF16)
    mix[...] = jnp.dot(back_place[0], own_home[...], preferred_element_type=F32)
    home_copy().wait_recv()
    far = jnp.dot(back_place[1], home[...], preferred_element_type=F32)
    mixed[...] = (mix[...] + far).astype(BF16)

    for k in (1, 2):
        slot_copy(k).wait_send()
    relay_copy().wait_send()
    for k in (1, 2, 3):
        wm_copy(k).wait_send()
        dw_copy(k).wait_send()
        for m in range(3):
            wz_copy(m, k).wait_send()
            wy_copy(m, k).wait_send()
    for k in range(n_fs):
        tx_copy(k).wait_send()
        td_copy(k).wait_send()
        tf_copy(k).wait_send()
        hx_copy(k).wait_send()
        hd_copy(k).wait_send()
        hf_copy(k).wait_send()
    for i in range(2):
        part_copy(i).wait_send()
    home_copy().wait_send()


def pair_body(
    tokens, norm_gain, gate_weight, up_weight, down_weight, expert_ids, group_logits, pair_logits
):
    n_grp, n_fs, n_tp = (lax.axis_size(a) for a in ("grp", "fs", "tp"))
    experts, block, hid = gate_weight.shape
    tok_rows, width = tokens.shape
    share = block // n_grp
    capacity = 5 * tok_rows * 2 // (4 * experts)
    cap = -(-capacity // 16) * 16
    lanes = -(-cap // 128) * 128
    vmem = pl.BlockSpec(memory_space=pltpu.VMEM)
    hbm = pl.BlockSpec(memory_space=pl.ANY)
    dma = pltpu.SemaphoreType.DMA
    matrix = jax.ShapeDtypeStruct((n_fs * block, hid), BF16)
    rows = (cap, width)
    sem_shapes = [
        (5,), (3, n_fs),
        (n_fs,), (n_fs,), (n_fs,), (n_fs,), (3, n_fs), (3, n_fs), (3, n_fs), (3, n_fs),
        (n_fs,), (n_fs,), (n_fs,), (n_fs,), (n_fs,), (n_fs,),
        (n_tp,), (n_tp,), (n_fs,), (n_fs,), (n_fs,), (n_fs,), (n_fs,), (n_fs,),
        (2,), (2,), (1,), (1,),
    ]
    mixed, *matrices = pl.pallas_call(
        functools.partial(pair_kernel, n_grp, n_fs, n_tp, capacity),
        out_shape=(jax.ShapeDtypeStruct((tok_rows, width), BF16), matrix, matrix, matrix),
        in_specs=[hbm] * 8,
        out_specs=(vmem,) * 4,
        scratch_shapes=[
            pltpu.VMEM((tok_rows, width), BF16),
            pltpu.VMEM((1, block), F32),
            pltpu.VMEM((2, tok_rows), jnp.int32),
            pltpu.VMEM((group_logits.shape[1], tok_rows), F32),
            pltpu.VMEM((2, tok_rows), F32),
            pltpu.VMEM((block, 1), F32),
            pltpu.VMEM((3, block, hid), F32),
            pltpu.VMEM((3, n_fs - 1, share, hid), F32),
            pltpu.VMEM((3, n_fs - 1, share, hid), BF16),
            pltpu.VMEM((2, *rows), BF16),
            pltpu.VMEM((2, lanes, tok_rows), BF16),
            pltpu.VMEM((2, tok_rows, cap), BF16),
            pltpu.VMEM((2, 8, lanes), F32),
            pltpu.VMEM((n_fs, 8, lanes), F32),
            pltpu.VMEM((n_fs, cap, 1), F32),
            pltpu.VMEM((n_tp, n_fs, *rows), BF16),
            pltpu.VMEM((2, n_fs, cap, hid), F32),
            pltpu.VMEM((n_tp, n_fs, cap, hid), BF16),
            pltpu.VMEM((n_tp, block, hid), BF16),
            pltpu.VMEM((2, *rows), BF16),
            pltpu.VMEM((2, *rows), BF16),
            pltpu.VMEM(rows, F32),
            pltpu.VMEM(rows, BF16),
            pltpu.VMEM(rows, BF16),
            pltpu.VMEM(rows, BF16),
            pltpu.VMEM((tok_rows, width), F32),
        ] + [dma(s) for s in sem_shapes],
        compiler_params=pltpu.CompilerParams(
            collective_id=0, has_side_effects=True, vmem_limit_bytes=56 * 1024 * 1024
        ),
    )(
        tokens, norm_gain[None, :], expert_ids.T, group_logits.T, pair_logits.T,
        gate_weight, up_weight, down_weight,
    )
    return (mixed, *(m[None] for m in matrices))


def paired(mesh, tokens, gate_weight, expert_ids, group_logits):
    n_grp, n_fs, n_tp = (mesh.shape[a] for a in ("grp", "fs", "tp"))
    experts, features, _ = gate_weight.shape
    return (
        experts // group_logits.shape[1] == expert_ids.shape[1] == 2
        and n_fs == n_tp == experts == 4
        and n_grp == 2
    )


def solution(mesh):
    placed = (
        P(("grp", "fs"), "tp"),
        P("fs"),
        P(None, "fs", "tp"),
        P(None, "fs", "tp"),
        P(None, "fs", "tp"),
        P(("grp", "fs"), None),
        P(("grp", "fs"), None),
        P(("grp", "fs"), None),
    )

    def run(tokens, norm_gain, gate_weight, up_weight, down_weight, expert_ids, group_logits, pair_logits):
        args = (tokens, norm_gain, gate_weight, up_weight, down_weight, expert_ids, group_logits, pair_logits)
        special = paired(mesh, tokens, gate_weight, expert_ids, group_logits)
        return jax.shard_map(
            pair_body if special else body,
            mesh=mesh,
            in_specs=placed,
            out_specs=(
                P(("grp", "fs"), "tp"),
                P(("grp", "fs"), None, "tp"),
                P(("grp", "fs"), None, "tp"),
                P(("grp", "fs"), None, "tp"),
            ),
            check_vma=False,
        )(*args)

    return run
```

```python
import functools

import jax
import jax.numpy as jnp
from jax import lax
from jax.experimental import pallas as pl
from jax.experimental.pallas import tpu as pltpu
from jax.sharding import PartitionSpec as P

MESH = pl.DeviceIdType.MESH
BF16 = jnp.bfloat16
F32 = jnp.float32
scope = jax.named_scope


def each(count, step):
    if count <= 4:
        for i in range(count):
            step(i)
    else:
        lax.fori_loop(0, count, lambda i, c: (step(i), c)[1], 0)


def exchange_kernel(
    n_grp, n_fs, n_tp, capacity,
    tokens, gain, id_rows, group_logits, pair_logits, gate_in, up_in, down_in,
    mixed, gate_out, up_out, down_out,
    out_ref, raw, cast, ret, mix, piece, hidden, own, pair_send, pair_recv, x_send, x_recv, result,
    local_sem, raw_sem, slot_s, slot_r, wz_s, wz_r, wy_s, wy_r,
    gx_s, gx_r, gd_s, gd_r, gf_s, gf_r, pr_s, pr_r, xx_s, xx_r, rt_s, rt_r,
):
    g, f, t = lax.axis_index("grp"), lax.axis_index("fs"), lax.axis_index("tp")
    n_x = n_tp // 2
    chip, core = t // 2, lax.rem(t, 2)
    partner = chip * 2 + 1 - core
    width = piece.shape[3]
    block = cast.shape[2]
    tok_rows, padded = tokens.shape[0], out_ref.shape[1]
    experts = n_fs
    share = block // n_grp

    def fs_at(k):
        return lax.rem(f + k, n_fs)

    def outward(i):
        return jnp.where(f < n_fs // 2, i + 1, n_fs - 1 - i)

    def nearest(i):
        if n_fs != 4:
            return outward(i)
        first = jnp.where(f % 2 == 0, 1, 3)
        last = jnp.where(f == 0, 3, jnp.where(f == 3, 1, 2))
        return (first, 6 - first - last, last)[i]

    def grp_at(k):
        return lax.rem(g + k, n_grp)

    def chip_at(k):
        return lax.rem(chip + k, n_x)

    def rcopy(src, dst, ssem, rsem, axis, peer):
        return pltpu.make_async_remote_copy(
            src_ref=src, dst_ref=dst, send_sem=ssem, recv_sem=rsem,
            device_id={axis: peer}, device_id_type=MESH,
        )

    raw_copies = [
        pltpu.make_async_copy(w, raw.at[m], raw_sem.at[m])
        for m, w in enumerate((gate_in, up_in, down_in))
    ]
    for copy in raw_copies:
        copy.start()

    barrier = pltpu.get_barrier_semaphore()

    def greet(axis, peer):
        pl.semaphore_signal(barrier, inc=1, device_id={axis: peer}, device_id_type=MESH)

    each(n_fs - 1, lambda i: greet("fs", fs_at(i + 1)))
    each(n_grp - 1, lambda i: greet("grp", grp_at(i + 1)))
    each(n_x - 1, lambda i: greet("tp", chip_at(i + 1) * 2 + core))
    greet("tp", partner)

    def ints(shape, axis):
        return lax.broadcasted_iota(jnp.int32, shape, axis)

    def route(ids, axis):
        shape = (experts, tok_rows) if axis == 0 else (tok_rows, experts)
        named = [(ints(shape, axis) == i).astype(F32) for i in ids]
        square = (tok_rows, tok_rows)
        earlier = (ints(square, axis) < ints(square, 1 - axis)).astype(F32).astype(BF16)
        both = (named[0] + named[1]).astype(BF16)
        pair = (both, earlier) if axis == 0 else (earlier, both)
        before = jnp.dot(*pair, preferred_element_type=F32)
        picks, kept = [], []
        for i, name in zip(ids, named):
            rank = jnp.sum(before * name, axis=axis, keepdims=True)
            kept.append(rank < capacity)
            slot = i * padded + rank.astype(jnp.int32)
            picks.append(jnp.where(rank < capacity, slot, -1))
        return picks, kept

    row_picks, _ = route([id_rows[0:1, :], id_rows[1:2, :]], 0)

    def fill(k):
        e = fs_at(k)
        slot = ints((padded, tok_rows), 0) + e * padded
        named = (slot == row_picks[0]) | (slot == row_picks[1])
        place = jnp.where(named, 1.0, 0.0).astype(BF16)
        out_ref[e] = jnp.dot(place, tokens[...], preferred_element_type=F32).astype(BF16)

    each(n_fs - 1, lambda i: fill(i + 1))
    pl.semaphore_wait(barrier, n_fs - 1 + n_grp - 1 + n_x - 1 + 1)

    weights = (
        (cast.at[0], gate_out), (cast.at[1], up_out), (cast.at[2], down_out)
    )

    def slot_copy(k, source):
        return rcopy(out_ref.at[fs_at(k)], piece.at[t, source], slot_s.at[k],
                     slot_r.at[n_fs - k], "fs", fs_at(k))

    def slot_arrival(k):
        return rcopy(out_ref.at[f], piece.at[t, fs_at(k)], slot_s.at[k], slot_r.at[k], "fs", fs_at(k))

    each(n_fs - 1, lambda i: slot_copy(outward(i), f).start())
    fill(0)
    own_slots = pltpu.make_async_copy(out_ref.at[f], piece.at[t, f], local_sem.at[3])
    own_slots.start()

    def w_rows(source, part):
        return pl.ds(source * block + part * share, share)

    def wz_copy(m, k):
        w_in, w_out = weights[m]
        return rcopy(w_in.at[fs_at(k), pl.ds(g * share, share)], w_out.at[w_rows(f, g)],
                     wz_s.at[m, k], wz_r.at[m, n_fs - k], "fs", fs_at(k))

    def wz_arrival(m, k):
        w_in, w_out = weights[m]
        return rcopy(w_in.at[fs_at(k), pl.ds(g * share, share)], w_out.at[w_rows(fs_at(k), g)],
                     wz_s.at[m, k], wz_r.at[m, k], "fs", fs_at(k))

    def wy_copy(m, k, j):
        w_out = weights[m][1]
        rows = w_rows(fs_at(k), g)
        return rcopy(w_out.at[rows], w_out.at[rows], wy_s.at[m, k, j],
                     wy_r.at[m, k, n_grp - j], "grp", grp_at(j))

    def wy_arrival(m, k, j):
        w_out = weights[m][1]
        rows = w_rows(fs_at(k), grp_at(j))
        return rcopy(w_out.at[rows], w_out.at[rows], wy_s.at[m, k, j],
                     wy_r.at[m, k, j], "grp", grp_at(j))

    own_weights = []
    for m in range(3):
        w_in, w_out = weights[m]
        raw_copies[m].wait()

        def round_block(e):
            if m < 2:
                cast[m, e] = (gain[...] * raw[m, e]).astype(BF16)
            else:
                cast[m, e] = raw[m, e].astype(BF16)

        each(n_fs, round_block)
        copy = pltpu.make_async_copy(w_in.at[f], w_out.at[pl.ds(f * block, block)], local_sem.at[m])
        copy.start()
        own_weights.append(copy)

    for m in range(3):
        each(n_fs - 1, lambda i: wz_copy(m, outward(i)).start())

    def forward(m, k):
        wz_arrival(m, k).wait_recv()
        for j in range(1, n_grp):
            wy_copy(m, k, j).start()

    def gx_copy(k, j):
        src = piece.at[t, fs_at(k)]
        return rcopy(src, src, gx_s.at[k, j], gx_r.at[k, n_x - j], "tp", chip_at(j) * 2 + core)

    def gx_arrival(k, j):
        src = piece.at[chip_at(j) * 2 + core, fs_at(k)]
        return rcopy(src, src, gx_s.at[k, j], gx_r.at[k, j], "tp", chip_at(j) * 2 + core)

    def gd_copy(k):
        src = piece.at[t, fs_at(k)]
        return rcopy(src, src, gd_s.at[k], gd_r.at[k], "tp", partner)

    def gd_arrival(k):
        src = piece.at[partner, fs_at(k)]
        return rcopy(src, src, gd_s.at[k], gd_r.at[k], "tp", partner)

    def gf_copy(k, j):
        src = piece.at[chip_at(j) * 2 + core, fs_at(k)]
        return rcopy(src, src, gf_s.at[k, j], gf_r.at[k, j], "tp", partner)

    def gf_arrival(k, j):
        src = piece.at[chip_at(j) * 2 + 1 - core, fs_at(k)]
        return rcopy(src, src, gf_s.at[k, j], gf_r.at[k, j], "tp", partner)

    def spread(k):
        for j in range(1, n_x):
            gx_copy(k, j).start()
        gd_copy(k).start()

    own_slots.wait()
    spread(0)

    id_cols = jnp.transpose(id_rows[...])
    ids = [id_cols[:, k : k + 1] for k in range(2)]
    picks, kept = route(ids, 1)
    group_exp = jnp.exp(jnp.transpose(group_logits[...]))
    group_count = group_exp.shape[1]
    low = ints(group_exp.shape, 1) * (experts // group_count)
    member = (ids[0] >= low) & (ids[0] < low + experts // group_count)
    chosen = jnp.sum(jnp.where(member, group_exp, 0.0), axis=1, keepdims=True)
    chosen = chosen / jnp.sum(group_exp, axis=1, keepdims=True)
    pair_exp = jnp.exp(jnp.transpose(pair_logits[...]))
    pair_weight = pair_exp / jnp.sum(pair_exp, axis=1, keepdims=True) * chosen
    mix_weights = [
        jnp.where(kept[k], pair_weight[:, k : k + 1], 0.0) for k in range(2)
    ]

    def blend(k):
        e = fs_at(k)
        slot = ints((tok_rows, padded), 1) + e * padded
        named = (slot == picks[0]) | (slot == picks[1])
        place = jnp.where(named, 1.0, 0.0).astype(BF16)
        weight = jnp.where(ids[0] == e, mix_weights[0], 0.0)
        weight = weight + jnp.where(ids[1] == e, mix_weights[1], 0.0)
        return jnp.dot(place, ret[e], preferred_element_type=F32) * weight

    def spread_arrived(i):
        slot_arrival(nearest(i)).wait_recv()
        spread(nearest(i))

    each(n_fs - 1, spread_arrived)

    def hand_over(k):
        for j in range(1, n_x):
            gx_arrival(k, j).wait_recv()
            gf_copy(k, j).start()

    hand_over(0)

    each(n_fs - 1, lambda i: hand_over(nearest(i)))

    for m in range(3):
        each(n_fs - 1, lambda i: forward(m, nearest(i)))

    def all_in(m):
        own_weights[m].wait()
        for j in range(1, n_grp):
            each(n_fs - 1, lambda i: wy_arrival(m, i + 1, j).wait_recv())

    all_in(0)
    all_in(1)

    def make_hidden(k):
        source = fs_at(k)
        gd_arrival(k).wait_recv()
        for j in range(1, n_x):
            gf_arrival(k, j).wait_recv()
        gate = up = None
        for p in range(n_tp):
            rows = piece[p, source]
            cols = pl.ds(p * width, width)
            gate_part = jnp.dot(rows, gate_out[cols, :], preferred_element_type=F32)
            up_part = jnp.dot(rows, up_out[cols, :], preferred_element_type=F32)
            gate = gate_part if gate is None else gate + gate_part
            up = up_part if up is None else up + up_part
        hidden[k] = (gate / (1.0 + jnp.exp(-gate)) * up).astype(BF16)

    each(n_fs, lambda i: make_hidden(i))
    all_in(2)

    def term(k, j, to_core):
        column = (chip_at(j) * 2 + to_core) * width
        rows = down_out[pl.ds(pl.multiple_of(column, width), width), :]
        return lax.dot_general(hidden[k], rows, (((1,), (1,)), ((), ())), preferred_element_type=F32)

    def pr_copy(k):
        return rcopy(pair_send.at[k], pair_recv.at[k], pr_s.at[k], pr_r.at[k], "tp", partner)

    def stage_pair(k):
        for j in range(n_x):
            pair_send[k, j] = term(k, j, 1 - core).astype(BF16)
        pr_copy(k).start()
        for j in range(n_x):
            own[k, j] = term(k, j, core)

    def xx_copy(k, j):
        return rcopy(x_send.at[k, j], x_recv.at[k, n_x - j], xx_s.at[k, j], xx_r.at[k, n_x - j],
                     "tp", chip_at(j) * 2 + core)

    def xx_arrival(k, j):
        return rcopy(x_send.at[k, j], x_recv.at[k, j], xx_s.at[k, j], xx_r.at[k, j],
                     "tp", chip_at(j) * 2 + core)

    def stage_chip(k):
        pr_copy(k).wait_recv()
        for j in range(1, n_x):
            x_send[k, j] = (own[k, j] + pair_recv[k, j].astype(F32)).astype(BF16)
            xx_copy(k, j).start()
        own[k, 0] = own[k, 0] + pair_recv[k, 0].astype(F32)

    def rt_copy(k):
        return rcopy(result.at[k], ret.at[f], rt_s.at[k], rt_r.at[n_fs - k], "fs", fs_at(k))

    def rt_arrival(k):
        return rcopy(result.at[k], ret.at[fs_at(k)], rt_s.at[k], rt_r.at[k], "fs", fs_at(k))

    def total(k):
        acc = own[k, 0]
        for j in range(1, n_x):
            xx_arrival(k, j).wait_recv()
            acc = acc + x_recv[k, j].astype(F32)
        return acc.astype(BF16)

    def stage_home(k):
        result[k] = total(k)
        rt_copy(k).start()

    def order(i):
        return lax.rem(outward(i) + n_fs, n_fs)

    stage_pair(order(0))

    def pair_and_chip(i):
        stage_pair(order(i + 1))
        stage_chip(order(i))

    each(n_fs - 1, pair_and_chip)
    stage_chip(order(n_fs - 1))
    each(n_fs - 1, lambda i: stage_home(order(i)))
    ret[f] = total(0)
    mix[...] = blend(0)

    def collect(i):
        k = nearest(i)
        rt_arrival(k).wait_recv()
        mix[...] += blend(k)

    each(n_fs - 1, collect)
    mixed[...] = mix[...].astype(BF16)

    def drain_peer(i):
        k = i + 1
        slot_copy(k, f).wait_send()
        rt_copy(k).wait_send()
        for m in range(3):
            wz_copy(m, k).wait_send()
            for j in range(1, n_grp):
                wy_copy(m, k, j).wait_send()

    def drain_chunk(k):
        gd_copy(k).wait_send()
        pr_copy(k).wait_send()
        for j in range(1, n_x):
            gx_copy(k, j).wait_send()
            gf_copy(k, j).wait_send()
            xx_copy(k, j).wait_send()

    each(n_fs - 1, drain_peer)
    each(n_fs, drain_chunk)


def body(
    tokens, norm_gain, gate_weight, up_weight, down_weight, expert_ids, group_logits, pair_logits
):
    n_grp, n_fs, n_tp = (lax.axis_size(a) for a in ("grp", "fs", "tp"))
    n_x = n_tp // 2
    experts, block, hid = gate_weight.shape
    tok_rows, width = tokens.shape
    capacity = 5 * tok_rows * 2 // (4 * experts)
    cap = -(-capacity // 16) * 16
    vmem = pl.BlockSpec(memory_space=pltpu.VMEM)
    hbm = pl.BlockSpec(memory_space=pl.ANY)
    dma = pltpu.SemaphoreType.DMA
    matrix = jax.ShapeDtypeStruct((n_fs * block, hid), BF16)
    chunk = (n_fs, n_x, cap, width)
    sem_shapes = [
        (4,), (3,), (n_fs,), (n_fs,), (3, n_fs), (3, n_fs), (3, n_fs, n_grp), (3, n_fs, n_grp),
        (n_fs, n_x), (n_fs, n_x), (n_fs,), (n_fs,), (n_fs, n_x), (n_fs, n_x),
        (n_fs,), (n_fs,), (n_fs, n_x), (n_fs, n_x), (n_fs,), (n_fs,),
    ]
    mixed, *matrices = pl.pallas_call(
        functools.partial(exchange_kernel, n_grp, n_fs, n_tp, capacity),
        out_shape=(jax.ShapeDtypeStruct((tok_rows, width), BF16), matrix, matrix, matrix),
        in_specs=[vmem] * 5 + [hbm] * 3,
        out_specs=(vmem,) * 4,
        scratch_shapes=[
            pltpu.VMEM((n_fs, cap, width), BF16),
            pltpu.VMEM((3, n_fs, block, hid), F32),
            pltpu.VMEM((3, n_fs, block, hid), BF16),
            pltpu.VMEM((n_fs, cap, width), BF16),
            pltpu.VMEM((tok_rows, width), F32),
            pltpu.VMEM((n_tp, n_fs, cap, width), BF16),
            pltpu.VMEM((n_fs, cap, hid), BF16),
            pltpu.VMEM(chunk, F32),
            pltpu.VMEM(chunk, BF16),
            pltpu.VMEM(chunk, BF16),
            pltpu.VMEM(chunk, BF16),
            pltpu.VMEM(chunk, BF16),
            pltpu.VMEM((n_fs, cap, width), BF16),
        ] + [dma(s) for s in sem_shapes],
        compiler_params=pltpu.CompilerParams(
            collective_id=0, has_side_effects=True, vmem_limit_bytes=48 * 1024 * 1024
        ),
    )(
        tokens, norm_gain[:, None], expert_ids.T, group_logits.T, pair_logits.T,
        gate_weight, up_weight, down_weight,
    )
    return (mixed, *(m[None] for m in matrices))


def pair_kernel(
    n_grp, n_fs, n_tp, capacity,
    tokens_in, gain_in, ids_in, group_in, pair_in, gate_in, up_in, down_in,
    mixed, gate_out, up_out, down_out,
    tokens, gain, id_rows, group_logits, pair_logits, gain_col,
    raw_own, raw_far, cast, slots, place, back_place, wsend, wrecv, wcol,
    piece, acc, hid, dwn, part_send, part_recv, keep, home_send, home, own_home, mix,
    in_sem, raw_sem,
    sl_s, sl_r, wm_s, wm_r, wz_s, wz_r, wy_s, wy_r, tx_s, tx_r, td_s, td_r, tf_s, tf_r,
    dw_s, dw_r, hx_s, hx_r, hd_s, hd_r, hf_s, hf_r, pt_s, pt_r, hm_s, hm_r,
):
    g, f, t = lax.axis_index("grp"), lax.axis_index("fs"), lax.axis_index("tp")
    cap, width = piece.shape[2], piece.shape[3]
    block, hidden_units = raw_own.shape[1], raw_own.shape[2]
    share = raw_far.shape[2]
    tok_rows = tokens.shape[0]
    lanes = place.shape[1]
    pair = n_fs // 2

    def flip(i, k):
        return (i, i + 1 - 2 * lax.rem(i, 2), lax.rem(i + 2, 4), 3 - i)[k]

    def fs_at(k):
        return flip(f, k)

    def tp_at(j):
        return flip(t, j)

    other_grp = 1 - g

    def rcopy(src, dst, ssem, rsem, axis, peer):
        return pltpu.make_async_remote_copy(
            src_ref=src, dst_ref=dst, send_sem=ssem, recv_sem=rsem,
            device_id={axis: peer}, device_id_type=MESH,
        )

    small = [
        pltpu.make_async_copy(src, dst, in_sem.at[i])
        for i, (src, dst) in enumerate((
            (ids_in, id_rows), (tokens_in, tokens), (gain_in, gain),
            (group_in, group_logits), (pair_in, pair_logits),
        ))
    ]
    w_in = (gate_in, up_in, down_in)
    w_out = (gate_out, up_out, down_out)

    def far_load(m, k):
        return pltpu.make_async_copy(
            w_in[m].at[fs_at(k), pl.ds(g * share, share)], raw_far.at[m, k - 1], raw_sem.at[m, k]
        )

    def own_load(m):
        return pltpu.make_async_copy(w_in[m].at[f], raw_own.at[m], raw_sem.at[m, 0])

    for copy in small:
        copy.start()
    for m in (2, 0, 1):
        for k in (1, 2, 3):
            far_load(m, k).start()
    for m in (2, 0, 1):
        own_load(m).start()

    barrier = pltpu.get_barrier_semaphore()

    def greet(axis, peer):
        pl.semaphore_signal(barrier, inc=1, device_id={axis: peer}, device_id_type=MESH)

    for k in (1, 2, 3):
        greet("fs", fs_at(k))
        greet("tp", tp_at(k))
    greet("grp", other_grp)

    def ints(shape, axis):
        return lax.broadcasted_iota(jnp.int32, shape, axis)

    own_base = (f - lax.rem(f, 2))
    far_base = lax.rem(own_base + 2, 4)
    bases = (own_base, far_base)

    with scope("small_0_wait"):
        small[0].wait()
    first, second = id_rows[0:1, :], id_rows[1:2, :]
    members = [(first >= b) & (first < b + 2) for b in bases]
    square = (tok_rows, tok_rows)
    earlier = (ints(square, 0) < ints(square, 1)).astype(F32).astype(BF16)
    named = jnp.where(ints((8, tok_rows), 0) < 4, members[0].astype(F32), members[1].astype(F32))
    before = jnp.dot(named.astype(BF16), earlier, preferred_element_type=F32)
    ranks = [before[0:1, :], before[4:5, :]]
    kept = [m & (r < capacity) for m, r in zip(members, ranks)]
    seat = [jnp.where(k, r.astype(jnp.int32), -1) for k, r in zip(kept, ranks)]

    with scope("small_1_wait"):
        small[1].wait()

    def fill(i):
        one_hot = jnp.where(ints((lanes, tok_rows), 0) == seat[i], 1.0, 0.0)
        place[i] = one_hot.astype(BF16)
        rows = jnp.dot(place[i, 0:cap, :], tokens[...], preferred_element_type=F32).astype(BF16)
        slots[i] = rows
        return rows

    def slot_copy(k):
        src = slots.at[0] if k == 1 else slots.at[1]
        return rcopy(src, piece.at[t, k], sl_s.at[k], sl_r.at[k], "fs", fs_at(k))

    def relay_copy():
        return rcopy(piece.at[t, 2], piece.at[t, 3], sl_s.at[3], sl_r.at[3], "fs", fs_at(1))

    fill(1)
    with scope("pl_semaphore_wait_barrier_3_3_1"):
        pl.semaphore_wait(barrier, 3 + 3 + 1)
    slot_copy(2).start()
    piece[t, 0] = fill(0)
    slot_copy(1).start()

    def tx_copy(k):
        src = piece.at[t, k]
        return rcopy(src, src, tx_s.at[k], tx_r.at[k], "tp", tp_at(2))

    def td_copy(k):
        src = piece.at[t, k]
        return rcopy(src, src, td_s.at[k], td_r.at[k], "tp", tp_at(1))

    def tf_copy(k):
        src = piece.at[tp_at(2), k]
        return rcopy(src, src, tf_s.at[k], tf_r.at[k], "tp", tp_at(1))

    def tx_arrival(k):
        src = piece.at[tp_at(2), k]
        return rcopy(src, src, tx_s.at[k], tx_r.at[k], "tp", tp_at(2))

    def td_arrival(k):
        src = piece.at[tp_at(1), k]
        return rcopy(src, src, td_s.at[k], td_r.at[k], "tp", tp_at(1))

    def tf_arrival(k):
        src = piece.at[tp_at(3), k]
        return rcopy(src, src, tf_s.at[k], tf_r.at[k], "tp", tp_at(1))

    def spread(k):
        tx_copy(k).start()
        td_copy(k).start()

    spread(0)

    def w_rows(source, part):
        return pl.ds(source * block + part * share, share)

    def wz_copy(m, k):
        return rcopy(cast.at[m, k - 1], w_out[m].at[w_rows(f, g)],
                     wz_s.at[m, k], wz_r.at[m, k], "fs", fs_at(k))

    def wz_arrival(m, k):
        return rcopy(cast.at[m, k - 1], w_out[m].at[w_rows(fs_at(k), g)],
                     wz_s.at[m, k], wz_r.at[m, k], "fs", fs_at(k))

    def wy_copy(m, k):
        rows = w_out[m].at[w_rows(fs_at(k), g)]
        return rcopy(rows, rows, wy_s.at[m, k], wy_r.at[m, k], "grp", other_grp)

    def wy_arrival(m, k):
        rows = w_out[m].at[w_rows(fs_at(k), other_grp)]
        return rcopy(rows, rows, wy_s.at[m, k], wy_r.at[m, k], "grp", other_grp)

    with scope("small_2_wait"):
        small[2].wait()
    gain_col[...] = jnp.transpose(jnp.broadcast_to(gain[...], (8, block)))[:, 0:1]
    far_gain = gain_col[pl.ds(g * share, share), :]

    def send_far(m, k):
        with scope("far_load_m_k_wait"):
            far_load(m, k).wait()
        values = raw_far[m, k - 1]
        if m < 2:
            values = far_gain * values
        cast[m, k - 1] = values.astype(BF16)
        wz_copy(m, k).start()

    def round_own(m):
        with scope("own_load_m_wait"):
            own_load(m).wait()
        values = raw_own[m]
        if m < 2:
            values = gain_col[...] * values
        w_out[m][pl.ds(f * block, block), :] = values.astype(BF16)

    for k in (2, 3):
        send_far(2, k)

    with scope("small_3_wait"):
        small[3].wait()
    with scope("small_4_wait"):
        small[4].wait()
    group_exp = jnp.exp(group_logits[...])
    group_sum = jnp.sum(group_exp, axis=0, keepdims=True)
    pair_exp = jnp.exp(pair_logits[...])
    pair_weight = pair_exp / jnp.sum(pair_exp, axis=0, keepdims=True)
    group_count = group_exp.shape[0]

    def wm_copy(k):
        return rcopy(wsend.at[k // 2], wrecv.at[k], wm_s.at[k], wm_r.at[k], "fs", fs_at(k))

    chosen = jnp.zeros_like(group_sum)
    for i in range(group_count):
        chosen = chosen + jnp.where((first >= 2 * i) & (first < 2 * i + 2), group_exp[i : i + 1, :], 0.0)
    mix_weight = pair_weight * (chosen / group_sum)
    for i in range(2):
        expert = bases[i] + ints((8, tok_rows), 0)
        rest = jnp.where(first == expert, mix_weight[0:1, :], 0.0)
        rest = rest + jnp.where(second == expert, mix_weight[1:2, :], 0.0)
        total = None
        for _ in range(3):
            head = rest.astype(BF16)
            rest = rest - head.astype(F32)
            term = lax.dot_general(head, place[i], (((1,), (1,)), ((), ())), preferred_element_type=F32)
            total = term if total is None else total + term
        wsend[i] = total
    for k in (1, 2, 3):
        wm_copy(k).start()

    def slot_arrival(k):
        return rcopy(slots.at[0], piece.at[t, k], sl_s.at[k], sl_r.at[k], "fs", fs_at(k))

    with scope("cross"):
        slot_arrival(2).wait_recv()
    relay_copy().start()
    spread(2)
    send_far(2, 1)
    for k in (1, 2, 3):
        for m in (0, 1):
            send_far(m, k)

    def hand_over(k):
        with scope("hand%d" % k):
            tx_arrival(k).wait_recv()
        tf_copy(k).start()

    def forward(m, k):
        with scope("forward%d%d" % (m, k)):
            wz_arrival(m, k).wait_recv()
        wy_copy(m, k).start()

    def arrived(m, k):
        with scope("arrived%d%d" % (m, k)):
            wy_arrival(m, k).wait_recv()

    def land(k):
        with scope("land%d" % k):
            slot_arrival(k).wait_recv()
        spread(k)

    def seat_weights(k, rows):
        cols = jnp.transpose(rows)
        wcol[k] = jnp.where(lax.rem(f, 2) == 0, cols[0:cap, 0:1], cols[0:cap, 1:2])

    hand_over(0)
    round_own(2)
    for i in range(2):
        back_place[i] = jnp.transpose(place[i].astype(F32))[:, 0:cap].astype(BF16)
    seat_weights(0, wsend[0])
    land(1)
    forward(2, 2)
    forward(2, 3)
    hand_over(2)
    land(3)
    forward(2, 1)
    hand_over(1)
    for m in (0, 1):
        round_own(m)
    forward(0, 1)
    forward(1, 1)
    hand_over(3)

    def dw_copy(j):
        src = down_out.at[pl.ds(tp_at(j) * block, block)]
        return rcopy(src, dwn.at[j], dw_s.at[j], dw_r.at[j], "tp", tp_at(j))

    for k in (2, 3, 1):
        arrived(2, k)
    for j in (3, 2, 1):
        dw_copy(j).start()
    with scope("weights_in"):
        for k in (1, 2, 3):
            wm_copy(k).wait_recv()
            seat_weights(k, wrecv[k])
    with scope("rows_in"):
        for k in (0, 2, 1, 3):
            td_arrival(k).wait_recv()
            tf_arrival(k).wait_recv()

    def products(k, source):
        rows = piece[source, k]
        cols = pl.ds(source * block, block)
        gate = jnp.dot(rows, gate_out[cols, :], preferred_element_type=F32)
        up = jnp.dot(rows, up_out[cols, :], preferred_element_type=F32)
        return gate, up

    def first_products(k, c):
        gate, up = products(k, f)
        acc[0, k], acc[1, k] = gate, up
        return c

    def more_products(kk):
        def step(k, c):
            gate, up = products(k, fs_at(kk))
            acc[0, k] += gate
            acc[1, k] += up
            return c
        return step

    with scope("products0"):
        lax.fori_loop(0, n_fs, first_products, 0)
    forward(0, 2)
    forward(1, 2)
    for m in (0, 1):
        arrived(m, 1)
    with scope("products1"):
        lax.fori_loop(0, n_fs, more_products(1), 0)
    forward(0, 3)
    for m in (0, 1):
        arrived(m, 2)
    with scope("products2"):
        lax.fori_loop(0, n_fs, more_products(2), 0)
    forward(1, 3)
    for m in (0, 1):
        arrived(m, 3)

    def h_copy(j, k, ssem, rsem, source):
        return rcopy(hid.at[source, k], hid.at[source ^ j, k], ssem.at[k], rsem.at[k], "tp", tp_at(j))

    def hx_copy(k):
        return h_copy(2, k, hx_s, hx_r, 0)

    def hd_copy(k):
        return h_copy(1, k, hd_s, hd_r, 0)

    def hf_copy(k):
        return h_copy(1, k, hf_s, hf_r, 2)

    for k in (3, 2, 1, 0):
        with scope("hidden%d" % k):
            gate, up = products(k, fs_at(3))
            gate = acc[0, k] + gate
            up = acc[1, k] + up
            hid[0, k] = (gate / (1.0 + jnp.exp(-gate)) * up * wcol[k]).astype(BF16)
            hx_copy(k).start()
            hd_copy(k).start()

    with scope("dw"):
        for j in (1, 2, 3):
            dw_copy(j).wait_recv()

    def ready(k):
        with scope("hx%d" % k):
            hx_copy(k).wait_recv()
        hf_copy(k).start()
        with scope("hf%d" % k):
            hd_copy(k).wait_recv()
            hf_copy(k).wait_recv()

    halves = part_send.shape[1]
    strip = width // halves

    def result(k, c):
        total = None
        for j in range(n_tp):
            if j == 0:
                rows = down_out[pl.ds(t * block + c * strip, strip), :]
            else:
                rows = dwn[j, c * strip : (c + 1) * strip, :]
            term = lax.dot_general(hid[j, k], rows, (((1,), (1,)), ((), ())), preferred_element_type=F32)
            total = term if total is None else total + term
        return total

    def part_copy(i, c):
        return rcopy(part_send.at[i, c], part_recv.at[i, c], pt_s.at[i, c], pt_r.at[i, c], "fs", fs_at(1))

    def home_copy(c):
        return rcopy(home_send.at[c], home.at[c], hm_s.at[c], hm_r.at[c], "fs", fs_at(2))

    strips = range(halves)
    for i, (ours, theirs) in enumerate(((3, 2), (1, 0))):
        ready(ours)
        for c in strips:
            part_send[i, c] = result(ours, c).astype(BF16)
            part_copy(i, c).start()
        if i == 0:
            ready(theirs)
            for c in strips:
                keep[c] = result(theirs, c)
    for c in strips:
        with scope("part0%d" % c):
            part_copy(0, c).wait_recv()
        home_send[c] = (keep[c] + part_recv[0, c].astype(F32)).astype(BF16)
        home_copy(c).start()
    ready(0)
    for c in strips:
        keep[c] = result(0, c)
    for c in strips:
        with scope("part1%d" % c):
            part_copy(1, c).wait_recv()
        own_home[c] = (keep[c] + part_recv[1, c].astype(F32)).astype(BF16)
        mix[c] = jnp.dot(back_place[0], own_home[c], preferred_element_type=F32)
    for c in strips:
        with scope("home%d" % c):
            home_copy(c).wait_recv()
        far = jnp.dot(back_place[1], home[c], preferred_element_type=F32)
        mixed[:, c * strip : (c + 1) * strip] = (mix[c] + far).astype(BF16)

    for k in (1, 2):
        slot_copy(k).wait_send()
    relay_copy().wait_send()
    for k in (1, 2, 3):
        wm_copy(k).wait_send()
        dw_copy(k).wait_send()
        for m in range(3):
            wz_copy(m, k).wait_send()
            wy_copy(m, k).wait_send()
    for k in range(n_fs):
        tx_copy(k).wait_send()
        td_copy(k).wait_send()
        tf_copy(k).wait_send()
        hx_copy(k).wait_send()
        hd_copy(k).wait_send()
        hf_copy(k).wait_send()
    for c in strips:
        for i in range(2):
            part_copy(i, c).wait_send()
        home_copy(c).wait_send()


def pair_body(
    tokens, norm_gain, gate_weight, up_weight, down_weight, expert_ids, group_logits, pair_logits
):
    n_grp, n_fs, n_tp = (lax.axis_size(a) for a in ("grp", "fs", "tp"))
    experts, block, hid = gate_weight.shape
    tok_rows, width = tokens.shape
    share = block // n_grp
    capacity = 5 * tok_rows * 2 // (4 * experts)
    cap = -(-capacity // 16) * 16
    lanes = -(-cap // 128) * 128
    vmem = pl.BlockSpec(memory_space=pltpu.VMEM)
    hbm = pl.BlockSpec(memory_space=pltpu.HBM)
    dma = pltpu.SemaphoreType.DMA
    matrix = jax.ShapeDtypeStruct((n_fs * block, hid), BF16)
    rows = (cap, width)
    halves = 2
    strips = (halves, cap, width // halves)
    sem_shapes = [
        (5,), (3, n_fs),
        (n_fs,), (n_fs,), (n_fs,), (n_fs,), (3, n_fs), (3, n_fs), (3, n_fs), (3, n_fs),
        (n_fs,), (n_fs,), (n_fs,), (n_fs,), (n_fs,), (n_fs,),
        (n_tp,), (n_tp,), (n_fs,), (n_fs,), (n_fs,), (n_fs,), (n_fs,), (n_fs,),
        (2, halves), (2, halves), (halves,), (halves,),
    ]
    mixed, *matrices = pl.pallas_call(
        functools.partial(pair_kernel, n_grp, n_fs, n_tp, capacity),
        out_shape=(jax.ShapeDtypeStruct((tok_rows, width), BF16), matrix, matrix, matrix),
        in_specs=[hbm] * 8,
        out_specs=(vmem,) * 4,
        scratch_shapes=[
            pltpu.VMEM((tok_rows, width), BF16),
            pltpu.VMEM((1, block), F32),
            pltpu.VMEM((2, tok_rows), jnp.int32),
            pltpu.VMEM((group_logits.shape[1], tok_rows), F32),
            pltpu.VMEM((2, tok_rows), F32),
            pltpu.VMEM((block, 1), F32),
            pltpu.VMEM((3, block, hid), F32),
            pltpu.VMEM((3, n_fs - 1, share, hid), F32),
            pltpu.VMEM((3, n_fs - 1, share, hid), BF16),
            pltpu.VMEM((2, *rows), BF16),
            pltpu.VMEM((2, lanes, tok_rows), BF16),
            pltpu.VMEM((2, tok_rows, cap), BF16),
            pltpu.VMEM((2, 8, lanes), F32),
            pltpu.VMEM((n_fs, 8, lanes), F32),
            pltpu.VMEM((n_fs, cap, 1), F32),
            pltpu.VMEM((n_tp, n_fs, *rows), BF16),
            pltpu.VMEM((2, n_fs, cap, hid), F32),
            pltpu.VMEM((n_tp, n_fs, cap, hid), BF16),
            pltpu.VMEM((n_tp, block, hid), BF16),
            pltpu.VMEM((2, *strips), BF16),
            pltpu.VMEM((2, *strips), BF16),
            pltpu.VMEM(strips, F32),
            pltpu.VMEM(strips, BF16),
            pltpu.VMEM(strips, BF16),
            pltpu.VMEM(strips, BF16),
            pltpu.VMEM((halves, tok_rows, width // halves), F32),
        ] + [dma(s) for s in sem_shapes],
        compiler_params=pltpu.CompilerParams(
            collective_id=0, has_side_effects=True, vmem_limit_bytes=40 * 1024 * 1024
        ),
    )(*(pltpu.with_memory_space_constraint(x, pltpu.HBM) for x in (
        tokens, norm_gain[None, :], expert_ids.T, group_logits.T, pair_logits.T,
        gate_weight, up_weight, down_weight,
    )))
    return write_out(mixed, *matrices)


def write_kernel(mixed, gate, up, down, *rest):
    outs, sem = rest[:4], rest[4]
    copies = [
        pltpu.make_async_copy(src, dst, sem.at[i])
        for i, (src, dst) in enumerate(zip(
            (gate, up, down, mixed), (outs[1].at[0], outs[2].at[0], outs[3].at[0], outs[0])
        ))
    ]
    for copy in copies:
        copy.start()
    for copy in copies:
        copy.wait()


def write_out(mixed, *matrices):
    return pl.pallas_call(
        write_kernel,
        out_shape=(
            jax.ShapeDtypeStruct(mixed.shape, BF16),
            *(jax.ShapeDtypeStruct((1, *m.shape), BF16) for m in matrices),
        ),
        in_specs=[pl.BlockSpec(memory_space=pltpu.VMEM)] * 4,
        out_specs=(pl.BlockSpec(memory_space=pltpu.HBM),) * 4,
        scratch_shapes=[pltpu.SemaphoreType.DMA((4,))],
        compiler_params=pltpu.CompilerParams(vmem_limit_bytes=1024 * 1024),
    )(mixed, *matrices)


def paired(mesh, tokens, gate_weight, expert_ids, group_logits):
    n_grp, n_fs, n_tp = (mesh.shape[a] for a in ("grp", "fs", "tp"))
    experts, features, _ = gate_weight.shape
    return (
        experts // group_logits.shape[1] == expert_ids.shape[1] == 2
        and n_fs == n_tp == experts == 4
        and n_grp == 2
    )


def solution(mesh):
    placed = (
        P(("grp", "fs"), "tp"),
        P("fs"),
        P(None, "fs", "tp"),
        P(None, "fs", "tp"),
        P(None, "fs", "tp"),
        P(("grp", "fs"), None),
        P(("grp", "fs"), None),
        P(("grp", "fs"), None),
    )

    def run(tokens, norm_gain, gate_weight, up_weight, down_weight, expert_ids, group_logits, pair_logits):
        args = (tokens, norm_gain, gate_weight, up_weight, down_weight, expert_ids, group_logits, pair_logits)
        special = paired(mesh, tokens, gate_weight, expert_ids, group_logits)
        return jax.shard_map(
            pair_body if special else body,
            mesh=mesh,
            in_specs=placed,
            out_specs=(
                P(("grp", "fs"), "tp"),
                P(("grp", "fs"), None, "tp"),
                P(("grp", "fs"), None, "tp"),
                P(("grp", "fs"), None, "tp"),
            ),
            check_vma=False,
        )(*args)

    return run
```

```python
import functools

import jax
import jax.numpy as jnp
from jax import lax
from jax.experimental import pallas as pl
from jax.experimental.pallas import tpu as pltpu
from jax.sharding import PartitionSpec as P

MESH = pl.DeviceIdType.MESH
BF16 = jnp.bfloat16
F32 = jnp.float32
scope = jax.named_scope


def each(count, step):
    if count <= 4:
        for i in range(count):
            step(i)
    else:
        lax.fori_loop(0, count, lambda i, c: (step(i), c)[1], 0)


def exchange_kernel(
    n_grp, n_fs, n_tp, capacity,
    tokens, gain, id_rows, group_logits, pair_logits, gate_in, up_in, down_in,
    mixed, gate_out, up_out, down_out,
    out_ref, raw, cast, ret, mix, piece, hidden, own, pair_send, pair_recv, x_send, x_recv, result,
    local_sem, raw_sem, slot_s, slot_r, wz_s, wz_r, wy_s, wy_r,
    gx_s, gx_r, gd_s, gd_r, gf_s, gf_r, pr_s, pr_r, xx_s, xx_r, rt_s, rt_r,
):
    g, f, t = lax.axis_index("grp"), lax.axis_index("fs"), lax.axis_index("tp")
    n_x = n_tp // 2
    chip, core = t // 2, lax.rem(t, 2)
    partner = chip * 2 + 1 - core
    width = piece.shape[3]
    block = cast.shape[2]
    tok_rows, padded = tokens.shape[0], out_ref.shape[1]
    experts = n_fs
    share = block // n_grp

    def fs_at(k):
        return lax.rem(f + k, n_fs)

    def outward(i):
        return jnp.where(f < n_fs // 2, i + 1, n_fs - 1 - i)

    def nearest(i):
        if n_fs != 4:
            return outward(i)
        first = jnp.where(f % 2 == 0, 1, 3)
        last = jnp.where(f == 0, 3, jnp.where(f == 3, 1, 2))
        return (first, 6 - first - last, last)[i]

    def grp_at(k):
        return lax.rem(g + k, n_grp)

    def chip_at(k):
        return lax.rem(chip + k, n_x)

    def rcopy(src, dst, ssem, rsem, axis, peer):
        return pltpu.make_async_remote_copy(
            src_ref=src, dst_ref=dst, send_sem=ssem, recv_sem=rsem,
            device_id={axis: peer}, device_id_type=MESH,
        )

    raw_copies = [
        pltpu.make_async_copy(w, raw.at[m], raw_sem.at[m])
        for m, w in enumerate((gate_in, up_in, down_in))
    ]
    for copy in raw_copies:
        copy.start()

    barrier = pltpu.get_barrier_semaphore()

    def greet(axis, peer):
        pl.semaphore_signal(barrier, inc=1, device_id={axis: peer}, device_id_type=MESH)

    each(n_fs - 1, lambda i: greet("fs", fs_at(i + 1)))
    each(n_grp - 1, lambda i: greet("grp", grp_at(i + 1)))
    each(n_x - 1, lambda i: greet("tp", chip_at(i + 1) * 2 + core))
    greet("tp", partner)

    def ints(shape, axis):
        return lax.broadcasted_iota(jnp.int32, shape, axis)

    def route(ids, axis):
        shape = (experts, tok_rows) if axis == 0 else (tok_rows, experts)
        named = [(ints(shape, axis) == i).astype(F32) for i in ids]
        square = (tok_rows, tok_rows)
        earlier = (ints(square, axis) < ints(square, 1 - axis)).astype(F32).astype(BF16)
        both = (named[0] + named[1]).astype(BF16)
        pair = (both, earlier) if axis == 0 else (earlier, both)
        before = jnp.dot(*pair, preferred_element_type=F32)
        picks, kept = [], []
        for i, name in zip(ids, named):
            rank = jnp.sum(before * name, axis=axis, keepdims=True)
            kept.append(rank < capacity)
            slot = i * padded + rank.astype(jnp.int32)
            picks.append(jnp.where(rank < capacity, slot, -1))
        return picks, kept

    row_picks, _ = route([id_rows[0:1, :], id_rows[1:2, :]], 0)

    def fill(k):
        e = fs_at(k)
        slot = ints((padded, tok_rows), 0) + e * padded
        named = (slot == row_picks[0]) | (slot == row_picks[1])
        place = jnp.where(named, 1.0, 0.0).astype(BF16)
        out_ref[e] = jnp.dot(place, tokens[...], preferred_element_type=F32).astype(BF16)

    each(n_fs - 1, lambda i: fill(i + 1))
    pl.semaphore_wait(barrier, n_fs - 1 + n_grp - 1 + n_x - 1 + 1)

    weights = (
        (cast.at[0], gate_out), (cast.at[1], up_out), (cast.at[2], down_out)
    )

    def slot_copy(k, source):
        return rcopy(out_ref.at[fs_at(k)], piece.at[t, source], slot_s.at[k],
                     slot_r.at[n_fs - k], "fs", fs_at(k))

    def slot_arrival(k):
        return rcopy(out_ref.at[f], piece.at[t, fs_at(k)], slot_s.at[k], slot_r.at[k], "fs", fs_at(k))

    each(n_fs - 1, lambda i: slot_copy(outward(i), f).start())
    fill(0)
    own_slots = pltpu.make_async_copy(out_ref.at[f], piece.at[t, f], local_sem.at[3])
    own_slots.start()

    def w_rows(source, part):
        return pl.ds(source * block + part * share, share)

    def wz_copy(m, k):
        w_in, w_out = weights[m]
        return rcopy(w_in.at[fs_at(k), pl.ds(g * share, share)], w_out.at[w_rows(f, g)],
                     wz_s.at[m, k], wz_r.at[m, n_fs - k], "fs", fs_at(k))

    def wz_arrival(m, k):
        w_in, w_out = weights[m]
        return rcopy(w_in.at[fs_at(k), pl.ds(g * share, share)], w_out.at[w_rows(fs_at(k), g)],
                     wz_s.at[m, k], wz_r.at[m, k], "fs", fs_at(k))

    def wy_copy(m, k, j):
        w_out = weights[m][1]
        rows = w_rows(fs_at(k), g)
        return rcopy(w_out.at[rows], w_out.at[rows], wy_s.at[m, k, j],
                     wy_r.at[m, k, n_grp - j], "grp", grp_at(j))

    def wy_arrival(m, k, j):
        w_out = weights[m][1]
        rows = w_rows(fs_at(k), grp_at(j))
        return rcopy(w_out.at[rows], w_out.at[rows], wy_s.at[m, k, j],
                     wy_r.at[m, k, j], "grp", grp_at(j))

    own_weights = []
    for m in range(3):
        w_in, w_out = weights[m]
        raw_copies[m].wait()

        def round_block(e):
            if m < 2:
                cast[m, e] = (gain[...] * raw[m, e]).astype(BF16)
            else:
                cast[m, e] = raw[m, e].astype(BF16)

        each(n_fs, round_block)
        copy = pltpu.make_async_copy(w_in.at[f], w_out.at[pl.ds(f * block, block)], local_sem.at[m])
        copy.start()
        own_weights.append(copy)

    for m in range(3):
        each(n_fs - 1, lambda i: wz_copy(m, outward(i)).start())

    def forward(m, k):
        wz_arrival(m, k).wait_recv()
        for j in range(1, n_grp):
            wy_copy(m, k, j).start()

    def gx_copy(k, j):
        src = piece.at[t, fs_at(k)]
        return rcopy(src, src, gx_s.at[k, j], gx_r.at[k, n_x - j], "tp", chip_at(j) * 2 + core)

    def gx_arrival(k, j):
        src = piece.at[chip_at(j) * 2 + core, fs_at(k)]
        return rcopy(src, src, gx_s.at[k, j], gx_r.at[k, j], "tp", chip_at(j) * 2 + core)

    def gd_copy(k):
        src = piece.at[t, fs_at(k)]
        return rcopy(src, src, gd_s.at[k], gd_r.at[k], "tp", partner)

    def gd_arrival(k):
        src = piece.at[partner, fs_at(k)]
        return rcopy(src, src, gd_s.at[k], gd_r.at[k], "tp", partner)

    def gf_copy(k, j):
        src = piece.at[chip_at(j) * 2 + core, fs_at(k)]
        return rcopy(src, src, gf_s.at[k, j], gf_r.at[k, j], "tp", partner)

    def gf_arrival(k, j):
        src = piece.at[chip_at(j) * 2 + 1 - core, fs_at(k)]
        return rcopy(src, src, gf_s.at[k, j], gf_r.at[k, j], "tp", partner)

    def spread(k):
        for j in range(1, n_x):
            gx_copy(k, j).start()
        gd_copy(k).start()

    own_slots.wait()
    spread(0)

    id_cols = jnp.transpose(id_rows[...])
    ids = [id_cols[:, k : k + 1] for k in range(2)]
    picks, kept = route(ids, 1)
    group_exp = jnp.exp(jnp.transpose(group_logits[...]))
    group_count = group_exp.shape[1]
    low = ints(group_exp.shape, 1) * (experts // group_count)
    member = (ids[0] >= low) & (ids[0] < low + experts // group_count)
    chosen = jnp.sum(jnp.where(member, group_exp, 0.0), axis=1, keepdims=True)
    chosen = chosen / jnp.sum(group_exp, axis=1, keepdims=True)
    pair_exp = jnp.exp(jnp.transpose(pair_logits[...]))
    pair_weight = pair_exp / jnp.sum(pair_exp, axis=1, keepdims=True) * chosen
    mix_weights = [
        jnp.where(kept[k], pair_weight[:, k : k + 1], 0.0) for k in range(2)
    ]

    def blend(k):
        e = fs_at(k)
        slot = ints((tok_rows, padded), 1) + e * padded
        named = (slot == picks[0]) | (slot == picks[1])
        place = jnp.where(named, 1.0, 0.0).astype(BF16)
        weight = jnp.where(ids[0] == e, mix_weights[0], 0.0)
        weight = weight + jnp.where(ids[1] == e, mix_weights[1], 0.0)
        return jnp.dot(place, ret[e], preferred_element_type=F32) * weight

    def spread_arrived(i):
        slot_arrival(nearest(i)).wait_recv()
        spread(nearest(i))

    each(n_fs - 1, spread_arrived)

    def hand_over(k):
        for j in range(1, n_x):
            gx_arrival(k, j).wait_recv()
            gf_copy(k, j).start()

    hand_over(0)

    each(n_fs - 1, lambda i: hand_over(nearest(i)))

    for m in range(3):
        each(n_fs - 1, lambda i: forward(m, nearest(i)))

    def all_in(m):
        own_weights[m].wait()
        for j in range(1, n_grp):
            each(n_fs - 1, lambda i: wy_arrival(m, i + 1, j).wait_recv())

    all_in(0)
    all_in(1)

    def make_hidden(k):
        source = fs_at(k)
        gd_arrival(k).wait_recv()
        for j in range(1, n_x):
            gf_arrival(k, j).wait_recv()
        gate = up = None
        for p in range(n_tp):
            rows = piece[p, source]
            cols = pl.ds(p * width, width)
            gate_part = jnp.dot(rows, gate_out[cols, :], preferred_element_type=F32)
            up_part = jnp.dot(rows, up_out[cols, :], preferred_element_type=F32)
            gate = gate_part if gate is None else gate + gate_part
            up = up_part if up is None else up + up_part
        hidden[k] = (gate / (1.0 + jnp.exp(-gate)) * up).astype(BF16)

    each(n_fs, lambda i: make_hidden(i))
    all_in(2)

    def term(k, j, to_core):
        column = (chip_at(j) * 2 + to_core) * width
        rows = down_out[pl.ds(pl.multiple_of(column, width), width), :]
        return lax.dot_general(hidden[k], rows, (((1,), (1,)), ((), ())), preferred_element_type=F32)

    def pr_copy(k):
        return rcopy(pair_send.at[k], pair_recv.at[k], pr_s.at[k], pr_r.at[k], "tp", partner)

    def stage_pair(k):
        for j in range(n_x):
            pair_send[k, j] = term(k, j, 1 - core).astype(BF16)
        pr_copy(k).start()
        for j in range(n_x):
            own[k, j] = term(k, j, core)

    def xx_copy(k, j):
        return rcopy(x_send.at[k, j], x_recv.at[k, n_x - j], xx_s.at[k, j], xx_r.at[k, n_x - j],
                     "tp", chip_at(j) * 2 + core)

    def xx_arrival(k, j):
        return rcopy(x_send.at[k, j], x_recv.at[k, j], xx_s.at[k, j], xx_r.at[k, j],
                     "tp", chip_at(j) * 2 + core)

    def stage_chip(k):
        pr_copy(k).wait_recv()
        for j in range(1, n_x):
            x_send[k, j] = (own[k, j] + pair_recv[k, j].astype(F32)).astype(BF16)
            xx_copy(k, j).start()
        own[k, 0] = own[k, 0] + pair_recv[k, 0].astype(F32)

    def rt_copy(k):
        return rcopy(result.at[k], ret.at[f], rt_s.at[k], rt_r.at[n_fs - k], "fs", fs_at(k))

    def rt_arrival(k):
        return rcopy(result.at[k], ret.at[fs_at(k)], rt_s.at[k], rt_r.at[k], "fs", fs_at(k))

    def total(k):
        acc = own[k, 0]
        for j in range(1, n_x):
            xx_arrival(k, j).wait_recv()
            acc = acc + x_recv[k, j].astype(F32)
        return acc.astype(BF16)

    def stage_home(k):
        result[k] = total(k)
        rt_copy(k).start()

    def order(i):
        return lax.rem(outward(i) + n_fs, n_fs)

    stage_pair(order(0))

    def pair_and_chip(i):
        stage_pair(order(i + 1))
        stage_chip(order(i))

    each(n_fs - 1, pair_and_chip)
    stage_chip(order(n_fs - 1))
    each(n_fs - 1, lambda i: stage_home(order(i)))
    ret[f] = total(0)
    mix[...] = blend(0)

    def collect(i):
        k = nearest(i)
        rt_arrival(k).wait_recv()
        mix[...] += blend(k)

    each(n_fs - 1, collect)
    mixed[...] = mix[...].astype(BF16)

    def drain_peer(i):
        k = i + 1
        slot_copy(k, f).wait_send()
        rt_copy(k).wait_send()
        for m in range(3):
            wz_copy(m, k).wait_send()
            for j in range(1, n_grp):
                wy_copy(m, k, j).wait_send()

    def drain_chunk(k):
        gd_copy(k).wait_send()
        pr_copy(k).wait_send()
        for j in range(1, n_x):
            gx_copy(k, j).wait_send()
            gf_copy(k, j).wait_send()
            xx_copy(k, j).wait_send()

    each(n_fs - 1, drain_peer)
    each(n_fs, drain_chunk)


def body(
    tokens, norm_gain, gate_weight, up_weight, down_weight, expert_ids, group_logits, pair_logits
):
    n_grp, n_fs, n_tp = (lax.axis_size(a) for a in ("grp", "fs", "tp"))
    n_x = n_tp // 2
    experts, block, hid = gate_weight.shape
    tok_rows, width = tokens.shape
    capacity = 5 * tok_rows * 2 // (4 * experts)
    cap = -(-capacity // 16) * 16
    vmem = pl.BlockSpec(memory_space=pltpu.VMEM)
    hbm = pl.BlockSpec(memory_space=pl.ANY)
    dma = pltpu.SemaphoreType.DMA
    matrix = jax.ShapeDtypeStruct((n_fs * block, hid), BF16)
    chunk = (n_fs, n_x, cap, width)
    sem_shapes = [
        (4,), (3,), (n_fs,), (n_fs,), (3, n_fs), (3, n_fs), (3, n_fs, n_grp), (3, n_fs, n_grp),
        (n_fs, n_x), (n_fs, n_x), (n_fs,), (n_fs,), (n_fs, n_x), (n_fs, n_x),
        (n_fs,), (n_fs,), (n_fs, n_x), (n_fs, n_x), (n_fs,), (n_fs,),
    ]
    mixed, *matrices = pl.pallas_call(
        functools.partial(exchange_kernel, n_grp, n_fs, n_tp, capacity),
        out_shape=(jax.ShapeDtypeStruct((tok_rows, width), BF16), matrix, matrix, matrix),
        in_specs=[vmem] * 5 + [hbm] * 3,
        out_specs=(vmem,) * 4,
        scratch_shapes=[
            pltpu.VMEM((n_fs, cap, width), BF16),
            pltpu.VMEM((3, n_fs, block, hid), F32),
            pltpu.VMEM((3, n_fs, block, hid), BF16),
            pltpu.VMEM((n_fs, cap, width), BF16),
            pltpu.VMEM((tok_rows, width), F32),
            pltpu.VMEM((n_tp, n_fs, cap, width), BF16),
            pltpu.VMEM((n_fs, cap, hid), BF16),
            pltpu.VMEM(chunk, F32),
            pltpu.VMEM(chunk, BF16),
            pltpu.VMEM(chunk, BF16),
            pltpu.VMEM(chunk, BF16),
            pltpu.VMEM(chunk, BF16),
            pltpu.VMEM((n_fs, cap, width), BF16),
        ] + [dma(s) for s in sem_shapes],
        compiler_params=pltpu.CompilerParams(
            collective_id=0, has_side_effects=True, vmem_limit_bytes=48 * 1024 * 1024
        ),
    )(
        tokens, norm_gain[:, None], expert_ids.T, group_logits.T, pair_logits.T,
        gate_weight, up_weight, down_weight,
    )
    return (mixed, *(m[None] for m in matrices))


def pair_kernel(
    n_grp, n_fs, n_tp, capacity, chunk,
    tokens_in, gain_in, ids_in, group_in, pair_in, gate_in, up_in, down_in,
    mixed, gate_out, up_out, down_out,
    tokens, gain, id_rows, group_logits, pair_logits, gain_col,
    raw_own, raw_far, cast, slots, place, back_place, wsend, wrecv, wcol,
    piece, acc, hid, dwn, part_send, part_recv, keep, home_send, back, mix,
    in_sem, raw_sem, send, sl_r, wm_r, wz_r, wy_r, tx_r, td_r, tf_r,
    dw_r, hx_r, hd_r, hf_r, pt_r, hm_r,
):
    g, f, t = lax.axis_index("grp"), lax.axis_index("fs"), lax.axis_index("tp")
    cap, width = piece.shape[2], piece.shape[3]
    block, hidden_units = raw_own.shape[1], raw_own.shape[2]
    share = raw_far.shape[2]
    tok_rows = tokens.shape[0]
    lanes = place.shape[1]
    pair = n_fs // 2

    inner = (f == 1) | (f == 2)

    def flip(i, k):
        return (i, i + 1 - 2 * lax.rem(i, 2), lax.rem(i + 2, 4), 3 - i)[k]

    def fs_at(k):
        if isinstance(k, int):
            return flip(f, k)
        return jnp.where(k == 1, flip(f, 1), jnp.where(k == 2, flip(f, 2), flip(f, 3)))

    def by_role(at_inner, at_outer):
        return jnp.where(inner, at_inner, at_outer)

    def tp_at(j):
        return flip(t, j)

    other_grp = 1 - g

    def rcopy(src, dst, ssem, rsem, axis, peer):
        return pltpu.make_async_remote_copy(
            src_ref=src, dst_ref=dst, send_sem=ssem, recv_sem=rsem,
            device_id={axis: peer}, device_id_type=MESH,
        )

    def all_sent(index, ref):
        rcopy(ref, ref, send.at[index], send.at[index], "fs", fs_at(1)).wait_send()

    def all_here(sem, ref):
        rcopy(ref, ref, sem, sem, "fs", fs_at(1)).wait_recv()

    small = [
        pltpu.make_async_copy(src, dst, in_sem.at[i])
        for i, (src, dst) in enumerate((
            (ids_in, id_rows), (tokens_in, tokens), (gain_in, gain),
            (group_in, group_logits), (pair_in, pair_logits),
        ))
    ]
    w_in = (gate_in, up_in, down_in)
    w_out = (gate_out, up_out, down_out)

    def far_load(m, k):
        return pltpu.make_async_copy(
            w_in[m].at[fs_at(k), pl.ds(g * share, share)], raw_far.at[m, k - 1], raw_sem.at[m, k]
        )

    def own_load(m):
        return pltpu.make_async_copy(w_in[m].at[f], raw_own.at[m], raw_sem.at[m, 0])

    for copy in small:
        copy.start()
    for m in (2, 0, 1):
        for k in (1, 2, 3):
            far_load(m, k).start()
    for m in (2, 0, 1):
        own_load(m).start()

    barrier = pltpu.get_barrier_semaphore()

    def greet(axis, peer):
        pl.semaphore_signal(barrier, inc=1, device_id={axis: peer}, device_id_type=MESH)

    for k in (1, 2, 3):
        greet("fs", fs_at(k))
        greet("tp", tp_at(k))
    greet("grp", other_grp)

    def ints(shape, axis):
        return lax.broadcasted_iota(jnp.int32, shape, axis)

    own_base = (f - lax.rem(f, 2))
    far_base = lax.rem(own_base + 2, 4)
    bases = (own_base, far_base)

    with scope("small_0_wait"):
        small[0].wait()
    first, second = id_rows[0:1, :], id_rows[1:2, :]
    members = [(first >= b) & (first < b + 2) for b in bases]
    square = (tok_rows, tok_rows)
    earlier = (ints(square, 0) < ints(square, 1)).astype(F32).astype(BF16)
    named = jnp.where(ints((8, tok_rows), 0) < 4, members[0].astype(F32), members[1].astype(F32))
    before = jnp.dot(named.astype(BF16), earlier, preferred_element_type=F32)
    ranks = [before[0:1, :], before[4:5, :]]
    kept = [m & (r < capacity) for m, r in zip(members, ranks)]
    seat = [jnp.where(k, r.astype(jnp.int32), -1) for k, r in zip(kept, ranks)]

    with scope("small_1_wait"):
        small[1].wait()

    def fill(i):
        one_hot = jnp.where(ints((lanes, tok_rows), 0) == seat[i], 1.0, 0.0)
        place[i] = one_hot.astype(BF16)
        rows = jnp.dot(place[i, 0:cap, :], tokens[...], preferred_element_type=F32).astype(BF16)
        slots[i] = rows
        return rows

    def slot_copy(k):
        src = slots.at[0] if k == 1 else slots.at[1]
        return rcopy(src, piece.at[t, k], send.at[0], sl_r.at[k], "fs", fs_at(k))

    def relay_copy():
        return rcopy(piece.at[t, 2], piece.at[t, 3], send.at[0], sl_r.at[3], "fs", fs_at(1))

    fill(1)
    with scope("pl_semaphore_wait_barrier_3_3_1"):
        pl.semaphore_wait(barrier, 3 + 3 + 1)
    slot_copy(2).start()
    piece[t, 0] = fill(0)
    slot_copy(1).start()

    def tx_copy(k):
        src = piece.at[t, k]
        return rcopy(src, src, send.at[1], tx_r.at[k], "tp", tp_at(2))

    def td_copy(k):
        src = piece.at[t, k]
        return rcopy(src, src, send.at[2], td_r.at[k // 3], "tp", tp_at(1))

    def tf_copy(k):
        src = piece.at[tp_at(2), k]
        return rcopy(src, src, send.at[3], tf_r.at[k // 3], "tp", tp_at(1))

    def tx_arrival(k):
        src = piece.at[tp_at(2), k]
        return rcopy(src, src, send.at[1], tx_r.at[k], "tp", tp_at(2))

    def td_arrival(k):
        src = piece.at[tp_at(1), k]
        return rcopy(src, src, send.at[2], td_r.at[k // 3], "tp", tp_at(1))

    def tf_arrival(k):
        src = piece.at[tp_at(3), k]
        return rcopy(src, src, send.at[3], tf_r.at[k // 3], "tp", tp_at(1))

    def spread(k):
        tx_copy(k).start()
        td_copy(k).start()

    spread(0)

    half = share // wz_r.shape[2]
    halves = range(wz_r.shape[2])

    def w_rows(source, part, h):
        return pl.ds(source * block + part * share + h * half, half)

    def wz_copy(m, k, h):
        return rcopy(cast.at[m, k - 1, pl.ds(h * half, half)], w_out[m].at[w_rows(f, g, h)],
                     send.at[4], wz_r.at[m, k - 1, h], "fs", fs_at(k))

    def wz_arrival(m, k, h):
        return rcopy(cast.at[m, k - 1, pl.ds(h * half, half)], w_out[m].at[w_rows(fs_at(k), g, h)],
                     send.at[4], wz_r.at[m, k - 1, h], "fs", fs_at(k))

    def wy_sem(m, k):
        return wy_r.at[0] if m == 2 else wy_r.at[k]

    def wy_copy(m, k, h):
        rows = w_out[m].at[w_rows(fs_at(k), g, h)]
        return rcopy(rows, rows, send.at[5], wy_sem(m, k), "grp", other_grp)

    def wy_arrival(m, k, h):
        rows = w_out[m].at[w_rows(fs_at(k), other_grp, h)]
        return rcopy(rows, rows, send.at[5], wy_sem(m, k), "grp", other_grp)

    small[2].wait()
    gain_col[...] = jnp.transpose(jnp.broadcast_to(gain[...], (8, block)))[:, 0:1]
    far_gain = gain_col[pl.ds(g * share, share), :]

    def send_far(m, k):
        with scope("far_load_m_k_wait"):
            far_load(m, k).wait()
        values = raw_far[m, k - 1]
        if m < 2:
            values = far_gain * values
        cast[m, k - 1] = values.astype(BF16)
        for h in halves:
            wz_copy(m, k, h).start()

    def round_own(m):
        with scope("own_load_m_wait"):
            own_load(m).wait()
        values = raw_own[m]
        if m < 2:
            values = gain_col[...] * values
        w_out[m][pl.ds(f * block, block), :] = values.astype(BF16)

    for k in (1, 2, 3):
        send_far(2, k)

    with scope("small_3_wait"):
        small[3].wait()
    with scope("small_4_wait"):
        small[4].wait()
    group_exp = jnp.exp(group_logits[...])
    group_sum = jnp.sum(group_exp, axis=0, keepdims=True)
    pair_exp = jnp.exp(pair_logits[...])
    pair_weight = pair_exp / jnp.sum(pair_exp, axis=0, keepdims=True)
    group_count = group_exp.shape[0]

    def wm_copy(k):
        return rcopy(wsend.at[k // 2], wrecv.at[k], send.at[6], wm_r.at[0], "fs", fs_at(k))

    chosen = jnp.zeros_like(group_sum)
    for i in range(group_count):
        chosen = chosen + jnp.where((first >= 2 * i) & (first < 2 * i + 2), group_exp[i : i + 1, :], 0.0)
    mix_weight = pair_weight * (chosen / group_sum)
    for i in range(2):
        expert = bases[i] + ints((8, tok_rows), 0)
        rest = jnp.where(first == expert, mix_weight[0:1, :], 0.0)
        rest = rest + jnp.where(second == expert, mix_weight[1:2, :], 0.0)
        total = None
        for _ in range(3):
            head = rest.astype(BF16)
            rest = rest - head.astype(F32)
            term = lax.dot_general(head, place[i], (((1,), (1,)), ((), ())), preferred_element_type=F32)
            total = term if total is None else total + term
        wsend[i] = total
    for k in (1, 2, 3):
        wm_copy(k).start()

    def slot_arrival(k):
        return rcopy(slots.at[0], piece.at[t, k], send.at[0], sl_r.at[k], "fs", fs_at(k))

    with scope("cross"):
        slot_arrival(2).wait_recv()
    relay_copy().start()
    spread(2)
    for k in (1, 2, 3):
        for m in (0, 1):
            send_far(m, k)

    def hand_over(k):
        with scope("hand%d" % k):
            tx_arrival(k).wait_recv()
        tf_copy(k).start()

    def forward(m, k):
        for h in halves:
            with scope("forward%d" % m):
                wz_arrival(m, k, h).wait_recv()
            wy_copy(m, k, h).start()

    def arrived(k):
        with scope("arrived"):
            all_here(wy_r.at[k], gate_out.at[pl.ds(0, 2 * share)])

    def land(k):
        with scope("land%d" % k):
            slot_arrival(k).wait_recv()
        spread(k)

    def seat_weights(k, rows):
        cols = jnp.transpose(rows)
        wcol[k] = jnp.where(lax.rem(f, 2) == 0, cols[0:cap, 0:1], cols[0:cap, 1:2])

    hand_over(0)
    round_own(2)
    for i in range(2):
        back_place[i] = jnp.transpose(place[i].astype(F32))[:, 0:cap].astype(BF16)
    seat_weights(0, wsend[0])
    land(1)
    for k in (2, 1, 3):
        forward(2, k)
    hand_over(2)
    hand_over(1)
    for m in (0, 1):
        round_own(m)

    def dw_copy(j):
        src = down_out.at[pl.ds(tp_at(j) * block, block)]
        return rcopy(src, dwn.at[j], send.at[7], dw_r.at[0], "tp", tp_at(j))

    with scope("down_in"):
        all_here(wy_r.at[0], down_out.at[pl.ds(0, 3 * share)])
    for j in (3, 2, 1):
        dw_copy(j).start()
    turns = (by_role(1, 2), by_role(2, 1), 3)
    for m in (0, 1):
        forward(m, turns[0])
    land(3)
    for m in (0, 1):
        forward(m, turns[1])
    with scope("weights_in"):
        all_here(wm_r.at[0], wrecv.at[pl.ds(1, 3)])
        for k in (1, 2, 3):
            seat_weights(k, wrecv[k])
    with scope("rows_in"):
        all_here(td_r.at[0], piece.at[t, pl.ds(0, 3)])
        all_here(tf_r.at[0], piece.at[t, pl.ds(0, 3)])

    def products(k, source):
        rows = piece[source, k]
        cols = pl.ds(source * block, block)
        gate = jnp.dot(rows, gate_out[cols, :], preferred_element_type=F32)
        up = jnp.dot(rows, up_out[cols, :], preferred_element_type=F32)
        return gate, up

    def first_products(k, c):
        gate, up = products(k, f)
        acc[0, k], acc[1, k] = gate, up
        return c

    def more_products(kk):
        def step(k, c):
            gate, up = products(k, fs_at(kk))
            acc[0, k] += gate
            acc[1, k] += up
            return c
        return step

    def multiply(step, blocks):
        with scope("products"):
            lax.fori_loop(*blocks, step, 0)

    first = (0, n_fs - 1)
    multiply(first_products, first)
    arrived(turns[0])
    multiply(more_products(turns[0]), first)
    for m in (0, 1):
        forward(m, turns[2])
    hand_over(3)
    with scope("rows_in"):
        all_here(td_r.at[1], piece.at[t, 3])
        all_here(tf_r.at[1], piece.at[t, 3])
    first_products(3, 0)
    more_products(turns[0])(3, 0)
    arrived(turns[1])
    multiply(more_products(turns[1]), (0, n_fs))
    arrived(turns[2])

    spans = [pl.ds(at, min(chunk, cap - at)) for at in range(0, cap, chunk)]
    parts = range(len(spans))

    def h_copy(j, k, c, ssem, rsem, source):
        src, dst = hid.at[source, k, spans[c]], hid.at[source ^ j, k, spans[c]]
        return rcopy(src, dst, ssem, rsem, "tp", tp_at(j))

    def hx_copy(k, c):
        return h_copy(2, k, c, send.at[8], hx_r.at[k, c], 0)

    def hd_copy(k, c):
        return h_copy(1, k, c, send.at[9], hd_r.at[k], 0)

    def hf_copy(k, c):
        return h_copy(1, k, c, send.at[10], hf_r.at[k, c], 2)

    last = fs_at(turns[2])
    blocks = (by_role(2, 3), by_role(3, 2), 1, 0)
    for k in blocks:
        with scope("hidden"):
            gate, up = products(k, last)
            gate = acc[0, k] + gate
            up = acc[1, k] + up
            hid[0, k] = (gate / (1.0 + jnp.exp(-gate)) * up * wcol[k]).astype(BF16)
            for c in parts:
                hx_copy(k, c).start()
                hd_copy(k, c).start()

    with scope("drain"):
        all_here(dw_r.at[0], dwn.at[pl.ds(1, 3)])
        all_sent(0, piece.at[t, pl.ds(0, 3)])
        for i in (1, 2, 3):
            all_sent(i, piece.at[t])
        all_sent(4, cast)
        all_sent(5, cast)
        all_sent(6, wrecv.at[pl.ds(1, 3)])
        all_sent(7, dwn.at[pl.ds(1, 3)])

    queue = [(k, c) for k in blocks for c in parts]

    def pass_on(n):
        if n < len(queue):
            with scope("hx"):
                hx_copy(*queue[n]).wait_recv()
            hf_copy(*queue[n]).start()

    def result(n):
        k, c = queue[n]

        def term(j):
            rows = down_out[pl.ds(t * block, block), :] if j == 0 else dwn[j]
            return lax.dot_general(
                hid[j, k, spans[c], :], rows, (((1,), (1,)), ((), ())), preferred_element_type=F32)

        if c == 0:
            with scope("hd"):
                all_here(hd_r.at[k], hid.at[1, k])
        total = term(0) + term(1)
        if n == 0:
            pass_on(0)
        total = total + term(2)
        if n > 0:
            pass_on(n + 1)
        with scope("hf"):
            hf_copy(k, c).wait_recv()
        total = total + term(3)
        if n == 0:
            pass_on(1)
        return total

    def part_copy(i, c):
        return rcopy(part_send.at[i, spans[c]], part_recv.at[i, spans[c]],
                     send.at[11 + i // 2], pt_r.at[i, c], "fs", fs_at(1))

    def home_copy(i, c):
        return rcopy(home_send.at[i, spans[c]], back.at[1, spans[c]],
                     send.at[13], hm_r.at[0], "fs", fs_at(2 + i))

    def home_step(n):
        if n < 0 or n >= 2 * len(parts):
            return
        i, c = divmod(n, len(parts))

        @pl.when(inner)
        def _():
            with scope("part%d" % i):
                part_copy(i, c).wait_recv()
            both = keep[i, spans[c], :] + part_recv[i, spans[c], :].astype(F32)
            home_send[i, spans[c], :] = both.astype(BF16)
            home_copy(i, c).start()

    for n in range(len(queue)):
        i, c = divmod(n, len(parts))
        if i == 2:
            part_send[2, spans[c], :] = result(n).astype(BF16)
            part_copy(2, c).start()
        else:
            keep[min(i, 2), spans[c], :] = result(n)
        if i < 2:
            @pl.when(jnp.logical_not(inner))
            def _():
                part_send[i, spans[c], :] = keep[i, spans[c], :].astype(BF16)
                part_copy(i, c).start()
        home_step(n - 2)

    def finish_own():
        for c in parts:
            with scope("part2"):
                part_copy(2, c).wait_recv()
            both = keep[2, spans[c], :] + part_recv[2, spans[c], :].astype(F32)
            back[0, spans[c], :] = both.astype(BF16)

    def finish_far():
        with scope("home"):
            all_here(hm_r.at[0], back.at[1])

    pl.when(inner)(finish_own)
    pl.when(jnp.logical_not(inner))(finish_far)
    sooner, later = by_role(0, 1), by_role(1, 0)
    mix[...] = jnp.dot(back_place[sooner], back[sooner], preferred_element_type=F32)
    pl.when(inner)(finish_far)
    pl.when(jnp.logical_not(inner))(finish_own)
    with scope("last_dot"):
        more = jnp.dot(back_place[later], back[later], preferred_element_type=F32)
        mixed[...] = (mix[...] + more).astype(BF16)

    for i in (8, 9, 10):
        all_sent(i, hid.at[0])
    all_sent(12, part_send.at[2])

    @pl.when(inner)
    def _():
        all_sent(13, home_send)

    @pl.when(jnp.logical_not(inner))
    def _():
        all_sent(11, part_send.at[pl.ds(0, 2)])


def pair_body(
    tokens, norm_gain, gate_weight, up_weight, down_weight, expert_ids, group_logits, pair_logits
):
    n_grp, n_fs, n_tp = (lax.axis_size(a) for a in ("grp", "fs", "tp"))
    experts, block, hid = gate_weight.shape
    tok_rows, width = tokens.shape
    share = block // n_grp
    capacity = 5 * tok_rows * 2 // (4 * experts)
    cap = -(-capacity // 16) * 16
    lanes = -(-cap // 128) * 128
    vmem = pl.BlockSpec(memory_space=pltpu.VMEM)
    hbm = pl.BlockSpec(memory_space=pltpu.HBM)
    dma = pltpu.SemaphoreType.DMA
    matrix = jax.ShapeDtypeStruct((n_fs * block, hid), BF16)
    rows = (cap, width)
    chunk = -(-cap // 32) * 16
    spans = -(-cap // chunk)
    sem_shapes = [
        (5,), (3, n_fs), (14,), (n_fs,), (1,), (3, n_fs - 1, 2), (n_fs,), (n_fs,), (2,), (2,),
        (1,), (n_fs, spans), (n_fs,), (n_fs, spans), (3, spans), (1,),
    ]
    mixed, *matrices = pl.pallas_call(
        functools.partial(pair_kernel, n_grp, n_fs, n_tp, capacity, chunk),
        out_shape=(jax.ShapeDtypeStruct((tok_rows, width), BF16), matrix, matrix, matrix),
        in_specs=[hbm] * 8,
        out_specs=(vmem,) * 4,
        scratch_shapes=[
            pltpu.VMEM((tok_rows, width), BF16),
            pltpu.VMEM((1, block), F32),
            pltpu.VMEM((2, tok_rows), jnp.int32),
            pltpu.VMEM((group_logits.shape[1], tok_rows), F32),
            pltpu.VMEM((2, tok_rows), F32),
            pltpu.VMEM((block, 1), F32),
            pltpu.VMEM((3, block, hid), F32),
            pltpu.VMEM((3, n_fs - 1, share, hid), F32),
            pltpu.VMEM((3, n_fs - 1, share, hid), BF16),
            pltpu.VMEM((2, *rows), BF16),
            pltpu.VMEM((2, lanes, tok_rows), BF16),
            pltpu.VMEM((2, tok_rows, cap), BF16),
            pltpu.VMEM((2, 8, lanes), F32),
            pltpu.VMEM((n_fs, 8, lanes), F32),
            pltpu.VMEM((n_fs, cap, 1), F32),
            pltpu.VMEM((n_tp, n_fs, *rows), BF16),
            pltpu.VMEM((2, n_fs, cap, hid), F32),
            pltpu.VMEM((n_tp, n_fs, cap, hid), BF16),
            pltpu.VMEM((n_tp, block, hid), BF16),
            pltpu.VMEM((3, *rows), BF16),
            pltpu.VMEM((3, *rows), BF16),
            pltpu.VMEM((3, *rows), F32),
            pltpu.VMEM((2, *rows), BF16),
            pltpu.VMEM((2, *rows), BF16),
            pltpu.VMEM((tok_rows, width), F32),
        ] + [dma(s) for s in sem_shapes],
        compiler_params=pltpu.CompilerParams(
            collective_id=0, has_side_effects=True, vmem_limit_bytes=40 * 1024 * 1024
        ),
    )(*(pltpu.with_memory_space_constraint(x, pltpu.HBM) for x in (
        tokens, norm_gain[None, :], expert_ids.T, group_logits.T, pair_logits.T,
        gate_weight, up_weight, down_weight,
    )))
    return write_out(mixed, *matrices)


def write_kernel(mixed, gate, up, down, *rest):
    outs, sem = rest[:4], rest[4]
    copies = [
        pltpu.make_async_copy(src, dst, sem.at[i])
        for i, (src, dst) in enumerate(zip(
            (gate, up, down, mixed), (outs[1].at[0], outs[2].at[0], outs[3].at[0], outs[0])
        ))
    ]
    for copy in copies:
        copy.start()
    for copy in copies:
        copy.wait()


def write_out(mixed, *matrices):
    return pl.pallas_call(
        write_kernel,
        out_shape=(
            jax.ShapeDtypeStruct(mixed.shape, BF16),
            *(jax.ShapeDtypeStruct((1, *m.shape), BF16) for m in matrices),
        ),
        in_specs=[pl.BlockSpec(memory_space=pltpu.VMEM)] * 4,
        out_specs=(pl.BlockSpec(memory_space=pltpu.HBM),) * 4,
        scratch_shapes=[pltpu.SemaphoreType.DMA((4,))],
        compiler_params=pltpu.CompilerParams(vmem_limit_bytes=1024 * 1024),
    )(mixed, *matrices)


def paired(mesh, tokens, gate_weight, expert_ids, group_logits):
    n_grp, n_fs, n_tp = (mesh.shape[a] for a in ("grp", "fs", "tp"))
    experts, features, _ = gate_weight.shape
    return (
        experts // group_logits.shape[1] == expert_ids.shape[1] == 2
        and n_fs == n_tp == experts == 4
        and n_grp == 2
    )


def solution(mesh):
    placed = (
        P(("grp", "fs"), "tp"),
        P("fs"),
        P(None, "fs", "tp"),
        P(None, "fs", "tp"),
        P(None, "fs", "tp"),
        P(("grp", "fs"), None),
        P(("grp", "fs"), None),
        P(("grp", "fs"), None),
    )

    def run(tokens, norm_gain, gate_weight, up_weight, down_weight, expert_ids, group_logits, pair_logits):
        args = (tokens, norm_gain, gate_weight, up_weight, down_weight, expert_ids, group_logits, pair_logits)
        special = paired(mesh, tokens, gate_weight, expert_ids, group_logits)
        return jax.shard_map(
            pair_body if special else body,
            mesh=mesh,
            in_specs=placed,
            out_specs=(
                P(("grp", "fs"), "tp"),
                P(("grp", "fs"), None, "tp"),
                P(("grp", "fs"), None, "tp"),
                P(("grp", "fs"), None, "tp"),
            ),
            check_vma=False,
        )(*args)

    return run
```

```python
import functools

import jax
import jax.numpy as jnp
from jax import lax
from jax.experimental import pallas as pl
from jax.experimental.pallas import tpu as pltpu
from jax.sharding import PartitionSpec as P

MESH = pl.DeviceIdType.MESH
BF16 = jnp.bfloat16
F32 = jnp.float32
scope = jax.named_scope


def each(count, step):
    if count <= 4:
        for i in range(count):
            step(i)
    else:
        lax.fori_loop(0, count, lambda i, c: (step(i), c)[1], 0)


def exchange_kernel(
    n_grp, n_fs, n_tp, capacity,
    tokens, gain, id_rows, group_logits, pair_logits, gate_in, up_in, down_in,
    mixed, gate_out, up_out, down_out,
    out_ref, raw, cast, ret, mix, piece, hidden, own, pair_send, pair_recv, x_send, x_recv, result,
    local_sem, raw_sem, slot_s, slot_r, wz_s, wz_r, wy_s, wy_r,
    gx_s, gx_r, gd_s, gd_r, gf_s, gf_r, pr_s, pr_r, xx_s, xx_r, rt_s, rt_r,
):
    g, f, t = lax.axis_index("grp"), lax.axis_index("fs"), lax.axis_index("tp")
    n_x = n_tp // 2
    chip, core = t // 2, lax.rem(t, 2)
    partner = chip * 2 + 1 - core
    width = piece.shape[3]
    block = cast.shape[2]
    tok_rows, padded = tokens.shape[0], out_ref.shape[1]
    experts = n_fs
    share = block // n_grp

    def fs_at(k):
        return lax.rem(f + k, n_fs)

    def outward(i):
        return jnp.where(f < n_fs // 2, i + 1, n_fs - 1 - i)

    def nearest(i):
        if n_fs != 4:
            return outward(i)
        first = jnp.where(f % 2 == 0, 1, 3)
        last = jnp.where(f == 0, 3, jnp.where(f == 3, 1, 2))
        return (first, 6 - first - last, last)[i]

    def grp_at(k):
        return lax.rem(g + k, n_grp)

    def chip_at(k):
        return lax.rem(chip + k, n_x)

    def rcopy(src, dst, ssem, rsem, axis, peer):
        return pltpu.make_async_remote_copy(
            src_ref=src, dst_ref=dst, send_sem=ssem, recv_sem=rsem,
            device_id={axis: peer}, device_id_type=MESH,
        )

    raw_copies = [
        pltpu.make_async_copy(w, raw.at[m], raw_sem.at[m])
        for m, w in enumerate((gate_in, up_in, down_in))
    ]
    for copy in raw_copies:
        copy.start()

    barrier = pltpu.get_barrier_semaphore()

    def greet(axis, peer):
        pl.semaphore_signal(barrier, inc=1, device_id={axis: peer}, device_id_type=MESH)

    each(n_fs - 1, lambda i: greet("fs", fs_at(i + 1)))
    each(n_grp - 1, lambda i: greet("grp", grp_at(i + 1)))
    each(n_x - 1, lambda i: greet("tp", chip_at(i + 1) * 2 + core))
    greet("tp", partner)

    def ints(shape, axis):
        return lax.broadcasted_iota(jnp.int32, shape, axis)

    def route(ids, axis):
        shape = (experts, tok_rows) if axis == 0 else (tok_rows, experts)
        named = [(ints(shape, axis) == i).astype(F32) for i in ids]
        square = (tok_rows, tok_rows)
        earlier = (ints(square, axis) < ints(square, 1 - axis)).astype(F32).astype(BF16)
        both = (named[0] + named[1]).astype(BF16)
        pair = (both, earlier) if axis == 0 else (earlier, both)
        before = jnp.dot(*pair, preferred_element_type=F32)
        picks, kept = [], []
        for i, name in zip(ids, named):
            rank = jnp.sum(before * name, axis=axis, keepdims=True)
            kept.append(rank < capacity)
            slot = i * padded + rank.astype(jnp.int32)
            picks.append(jnp.where(rank < capacity, slot, -1))
        return picks, kept

    row_picks, _ = route([id_rows[0:1, :], id_rows[1:2, :]], 0)

    def fill(k):
        e = fs_at(k)
        slot = ints((padded, tok_rows), 0) + e * padded
        named = (slot == row_picks[0]) | (slot == row_picks[1])
        place = jnp.where(named, 1.0, 0.0).astype(BF16)
        out_ref[e] = jnp.dot(place, tokens[...], preferred_element_type=F32).astype(BF16)

    each(n_fs - 1, lambda i: fill(i + 1))
    pl.semaphore_wait(barrier, n_fs - 1 + n_grp - 1 + n_x - 1 + 1)

    weights = (
        (cast.at[0], gate_out), (cast.at[1], up_out), (cast.at[2], down_out)
    )

    def slot_copy(k, source):
        return rcopy(out_ref.at[fs_at(k)], piece.at[t, source], slot_s.at[k],
                     slot_r.at[n_fs - k], "fs", fs_at(k))

    def slot_arrival(k):
        return rcopy(out_ref.at[f], piece.at[t, fs_at(k)], slot_s.at[k], slot_r.at[k], "fs", fs_at(k))

    each(n_fs - 1, lambda i: slot_copy(outward(i), f).start())
    fill(0)
    own_slots = pltpu.make_async_copy(out_ref.at[f], piece.at[t, f], local_sem.at[3])
    own_slots.start()

    def w_rows(source, part):
        return pl.ds(source * block + part * share, share)

    def wz_copy(m, k):
        w_in, w_out = weights[m]
        return rcopy(w_in.at[fs_at(k), pl.ds(g * share, share)], w_out.at[w_rows(f, g)],
                     wz_s.at[m, k], wz_r.at[m, n_fs - k], "fs", fs_at(k))

    def wz_arrival(m, k):
        w_in, w_out = weights[m]
        return rcopy(w_in.at[fs_at(k), pl.ds(g * share, share)], w_out.at[w_rows(fs_at(k), g)],
                     wz_s.at[m, k], wz_r.at[m, k], "fs", fs_at(k))

    def wy_copy(m, k, j):
        w_out = weights[m][1]
        rows = w_rows(fs_at(k), g)
        return rcopy(w_out.at[rows], w_out.at[rows], wy_s.at[m, k, j],
                     wy_r.at[m, k, n_grp - j], "grp", grp_at(j))

    def wy_arrival(m, k, j):
        w_out = weights[m][1]
        rows = w_rows(fs_at(k), grp_at(j))
        return rcopy(w_out.at[rows], w_out.at[rows], wy_s.at[m, k, j],
                     wy_r.at[m, k, j], "grp", grp_at(j))

    own_weights = []
    for m in range(3):
        w_in, w_out = weights[m]
        raw_copies[m].wait()

        def round_block(e):
            if m < 2:
                cast[m, e] = (gain[...] * raw[m, e]).astype(BF16)
            else:
                cast[m, e] = raw[m, e].astype(BF16)

        each(n_fs, round_block)
        copy = pltpu.make_async_copy(w_in.at[f], w_out.at[pl.ds(f * block, block)], local_sem.at[m])
        copy.start()
        own_weights.append(copy)

    for m in range(3):
        each(n_fs - 1, lambda i: wz_copy(m, outward(i)).start())

    def forward(m, k):
        wz_arrival(m, k).wait_recv()
        for j in range(1, n_grp):
            wy_copy(m, k, j).start()

    def gx_copy(k, j):
        src = piece.at[t, fs_at(k)]
        return rcopy(src, src, gx_s.at[k, j], gx_r.at[k, n_x - j], "tp", chip_at(j) * 2 + core)

    def gx_arrival(k, j):
        src = piece.at[chip_at(j) * 2 + core, fs_at(k)]
        return rcopy(src, src, gx_s.at[k, j], gx_r.at[k, j], "tp", chip_at(j) * 2 + core)

    def gd_copy(k):
        src = piece.at[t, fs_at(k)]
        return rcopy(src, src, gd_s.at[k], gd_r.at[k], "tp", partner)

    def gd_arrival(k):
        src = piece.at[partner, fs_at(k)]
        return rcopy(src, src, gd_s.at[k], gd_r.at[k], "tp", partner)

    def gf_copy(k, j):
        src = piece.at[chip_at(j) * 2 + core, fs_at(k)]
        return rcopy(src, src, gf_s.at[k, j], gf_r.at[k, j], "tp", partner)

    def gf_arrival(k, j):
        src = piece.at[chip_at(j) * 2 + 1 - core, fs_at(k)]
        return rcopy(src, src, gf_s.at[k, j], gf_r.at[k, j], "tp", partner)

    def spread(k):
        for j in range(1, n_x):
            gx_copy(k, j).start()
        gd_copy(k).start()

    own_slots.wait()
    spread(0)

    id_cols = jnp.transpose(id_rows[...])
    ids = [id_cols[:, k : k + 1] for k in range(2)]
    picks, kept = route(ids, 1)
    group_exp = jnp.exp(jnp.transpose(group_logits[...]))
    group_count = group_exp.shape[1]
    low = ints(group_exp.shape, 1) * (experts // group_count)
    member = (ids[0] >= low) & (ids[0] < low + experts // group_count)
    chosen = jnp.sum(jnp.where(member, group_exp, 0.0), axis=1, keepdims=True)
    chosen = chosen / jnp.sum(group_exp, axis=1, keepdims=True)
    pair_exp = jnp.exp(jnp.transpose(pair_logits[...]))
    pair_weight = pair_exp / jnp.sum(pair_exp, axis=1, keepdims=True) * chosen
    mix_weights = [
        jnp.where(kept[k], pair_weight[:, k : k + 1], 0.0) for k in range(2)
    ]

    def blend(k):
        e = fs_at(k)
        slot = ints((tok_rows, padded), 1) + e * padded
        named = (slot == picks[0]) | (slot == picks[1])
        place = jnp.where(named, 1.0, 0.0).astype(BF16)
        weight = jnp.where(ids[0] == e, mix_weights[0], 0.0)
        weight = weight + jnp.where(ids[1] == e, mix_weights[1], 0.0)
        return jnp.dot(place, ret[e], preferred_element_type=F32) * weight

    def spread_arrived(i):
        slot_arrival(nearest(i)).wait_recv()
        spread(nearest(i))

    each(n_fs - 1, spread_arrived)

    def hand_over(k):
        for j in range(1, n_x):
            gx_arrival(k, j).wait_recv()
            gf_copy(k, j).start()

    hand_over(0)

    each(n_fs - 1, lambda i: hand_over(nearest(i)))

    for m in range(3):
        each(n_fs - 1, lambda i: forward(m, nearest(i)))

    def all_in(m):
        own_weights[m].wait()
        for j in range(1, n_grp):
            each(n_fs - 1, lambda i: wy_arrival(m, i + 1, j).wait_recv())

    all_in(0)
    all_in(1)

    def make_hidden(k):
        source = fs_at(k)
        gd_arrival(k).wait_recv()
        for j in range(1, n_x):
            gf_arrival(k, j).wait_recv()
        gate = up = None
        for p in range(n_tp):
            rows = piece[p, source]
            cols = pl.ds(p * width, width)
            gate_part = jnp.dot(rows, gate_out[cols, :], preferred_element_type=F32)
            up_part = jnp.dot(rows, up_out[cols, :], preferred_element_type=F32)
            gate = gate_part if gate is None else gate + gate_part
            up = up_part if up is None else up + up_part
        hidden[k] = (gate / (1.0 + jnp.exp(-gate)) * up).astype(BF16)

    each(n_fs, lambda i: make_hidden(i))
    all_in(2)

    def term(k, j, to_core):
        column = (chip_at(j) * 2 + to_core) * width
        rows = down_out[pl.ds(pl.multiple_of(column, width), width), :]
        return lax.dot_general(hidden[k], rows, (((1,), (1,)), ((), ())), preferred_element_type=F32)

    def pr_copy(k):
        return rcopy(pair_send.at[k], pair_recv.at[k], pr_s.at[k], pr_r.at[k], "tp", partner)

    def stage_pair(k):
        for j in range(n_x):
            pair_send[k, j] = term(k, j, 1 - core).astype(BF16)
        pr_copy(k).start()
        for j in range(n_x):
            own[k, j] = term(k, j, core)

    def xx_copy(k, j):
        return rcopy(x_send.at[k, j], x_recv.at[k, n_x - j], xx_s.at[k, j], xx_r.at[k, n_x - j],
                     "tp", chip_at(j) * 2 + core)

    def xx_arrival(k, j):
        return rcopy(x_send.at[k, j], x_recv.at[k, j], xx_s.at[k, j], xx_r.at[k, j],
                     "tp", chip_at(j) * 2 + core)

    def stage_chip(k):
        pr_copy(k).wait_recv()
        for j in range(1, n_x):
            x_send[k, j] = (own[k, j] + pair_recv[k, j].astype(F32)).astype(BF16)
            xx_copy(k, j).start()
        own[k, 0] = own[k, 0] + pair_recv[k, 0].astype(F32)

    def rt_copy(k):
        return rcopy(result.at[k], ret.at[f], rt_s.at[k], rt_r.at[n_fs - k], "fs", fs_at(k))

    def rt_arrival(k):
        return rcopy(result.at[k], ret.at[fs_at(k)], rt_s.at[k], rt_r.at[k], "fs", fs_at(k))

    def total(k):
        acc = own[k, 0]
        for j in range(1, n_x):
            xx_arrival(k, j).wait_recv()
            acc = acc + x_recv[k, j].astype(F32)
        return acc.astype(BF16)

    def stage_home(k):
        result[k] = total(k)
        rt_copy(k).start()

    def order(i):
        return lax.rem(outward(i) + n_fs, n_fs)

    stage_pair(order(0))

    def pair_and_chip(i):
        stage_pair(order(i + 1))
        stage_chip(order(i))

    each(n_fs - 1, pair_and_chip)
    stage_chip(order(n_fs - 1))
    each(n_fs - 1, lambda i: stage_home(order(i)))
    ret[f] = total(0)
    mix[...] = blend(0)

    def collect(i):
        k = nearest(i)
        rt_arrival(k).wait_recv()
        mix[...] += blend(k)

    each(n_fs - 1, collect)
    mixed[...] = mix[...].astype(BF16)

    def drain_peer(i):
        k = i + 1
        slot_copy(k, f).wait_send()
        rt_copy(k).wait_send()
        for m in range(3):
            wz_copy(m, k).wait_send()
            for j in range(1, n_grp):
                wy_copy(m, k, j).wait_send()

    def drain_chunk(k):
        gd_copy(k).wait_send()
        pr_copy(k).wait_send()
        for j in range(1, n_x):
            gx_copy(k, j).wait_send()
            gf_copy(k, j).wait_send()
            xx_copy(k, j).wait_send()

    each(n_fs - 1, drain_peer)
    each(n_fs, drain_chunk)


def body(
    tokens, norm_gain, gate_weight, up_weight, down_weight, expert_ids, group_logits, pair_logits
):
    n_grp, n_fs, n_tp = (lax.axis_size(a) for a in ("grp", "fs", "tp"))
    n_x = n_tp // 2
    experts, block, hid = gate_weight.shape
    tok_rows, width = tokens.shape
    capacity = 5 * tok_rows * 2 // (4 * experts)
    cap = -(-capacity // 16) * 16
    vmem = pl.BlockSpec(memory_space=pltpu.VMEM)
    hbm = pl.BlockSpec(memory_space=pl.ANY)
    dma = pltpu.SemaphoreType.DMA
    matrix = jax.ShapeDtypeStruct((n_fs * block, hid), BF16)
    chunk = (n_fs, n_x, cap, width)
    sem_shapes = [
        (4,), (3,), (n_fs,), (n_fs,), (3, n_fs), (3, n_fs), (3, n_fs, n_grp), (3, n_fs, n_grp),
        (n_fs, n_x), (n_fs, n_x), (n_fs,), (n_fs,), (n_fs, n_x), (n_fs, n_x),
        (n_fs,), (n_fs,), (n_fs, n_x), (n_fs, n_x), (n_fs,), (n_fs,),
    ]
    mixed, *matrices = pl.pallas_call(
        functools.partial(exchange_kernel, n_grp, n_fs, n_tp, capacity),
        out_shape=(jax.ShapeDtypeStruct((tok_rows, width), BF16), matrix, matrix, matrix),
        in_specs=[vmem] * 5 + [hbm] * 3,
        out_specs=(vmem,) * 4,
        scratch_shapes=[
            pltpu.VMEM((n_fs, cap, width), BF16),
            pltpu.VMEM((3, n_fs, block, hid), F32),
            pltpu.VMEM((3, n_fs, block, hid), BF16),
            pltpu.VMEM((n_fs, cap, width), BF16),
            pltpu.VMEM((tok_rows, width), F32),
            pltpu.VMEM((n_tp, n_fs, cap, width), BF16),
            pltpu.VMEM((n_fs, cap, hid), BF16),
            pltpu.VMEM(chunk, F32),
            pltpu.VMEM(chunk, BF16),
            pltpu.VMEM(chunk, BF16),
            pltpu.VMEM(chunk, BF16),
            pltpu.VMEM(chunk, BF16),
            pltpu.VMEM((n_fs, cap, width), BF16),
        ] + [dma(s) for s in sem_shapes],
        compiler_params=pltpu.CompilerParams(
            collective_id=0, has_side_effects=True, vmem_limit_bytes=48 * 1024 * 1024
        ),
    )(
        tokens, norm_gain[:, None], expert_ids.T, group_logits.T, pair_logits.T,
        gate_weight, up_weight, down_weight,
    )
    return (mixed, *(m[None] for m in matrices))


def pair_kernel(
    n_grp, n_fs, n_tp, capacity, chunk,
    tokens_in, gain_in, ids_in, group_in, pair_in, gate_in, up_in, down_in,
    mixed, gate_out, up_out, down_out,
    tokens, gain, id_rows, group_logits, pair_logits, gain_col,
    raw_own, raw_far, cast, slots, place, back_place, wsend, wrecv, wcol,
    piece, acc, hid, dwn, part_send, part_recv, keep, home_send, back, mix,
    in_sem, raw_sem, send, sl_r, wm_r, wd_r, wz_r, wy_r, tx_r, td_r, tf_r,
    dw_r, hx_r, hd_r, hf_r, pt_r, hm_r,
):
    g, f, t = lax.axis_index("grp"), lax.axis_index("fs"), lax.axis_index("tp")
    cap, width = piece.shape[2], piece.shape[3]
    block, hidden_units = raw_own.shape[1], raw_own.shape[2]
    share = raw_far.shape[2]
    tok_rows = tokens.shape[0]
    lanes = place.shape[1]
    pair = n_fs // 2

    inner = (f == 1) | (f == 2)

    def flip(i, k):
        return (i, i + 1 - 2 * lax.rem(i, 2), lax.rem(i + 2, 4), 3 - i)[k]

    def fs_at(k):
        if isinstance(k, int):
            return flip(f, k)
        return jnp.where(k == 1, flip(f, 1), jnp.where(k == 2, flip(f, 2), flip(f, 3)))

    def by_role(at_inner, at_outer):
        return jnp.where(inner, at_inner, at_outer)

    def tp_at(j):
        return flip(t, j)

    other_grp = 1 - g

    def rcopy(src, dst, ssem, rsem, axis, peer):
        return pltpu.make_async_remote_copy(
            src_ref=src, dst_ref=dst, send_sem=ssem, recv_sem=rsem,
            device_id={axis: peer}, device_id_type=MESH,
        )

    def all_sent(index, ref):
        rcopy(ref, ref, send.at[index], send.at[index], "fs", fs_at(1)).wait_send()

    def all_here(sem, ref):
        rcopy(ref, ref, sem, sem, "fs", fs_at(1)).wait_recv()

    small = [
        pltpu.make_async_copy(src, dst, in_sem.at[i])
        for i, (src, dst) in enumerate((
            (ids_in, id_rows), (tokens_in, tokens), (gain_in, gain),
            (group_in, group_logits), (pair_in, pair_logits),
        ))
    ]
    w_in = (gate_in, up_in, down_in)
    w_out = (gate_out, up_out, down_out)

    def far_load(m, k):
        return pltpu.make_async_copy(
            w_in[m].at[fs_at(k), pl.ds(g * share, share)], raw_far.at[m, k - 1], raw_sem.at[m, 1]
        )

    def far_loaded(m):
        whole = w_in[m].at[pl.ds(0, 3), pl.ds(0, share)]
        pltpu.make_async_copy(whole, raw_far.at[m], raw_sem.at[m, 1]).wait()

    def own_load(m):
        return pltpu.make_async_copy(w_in[m].at[f], raw_own.at[m], raw_sem.at[m, 0])

    for copy in small:
        copy.start()
    for m in (2, 0, 1):
        for k in (1, 2, 3):
            far_load(m, k).start()
    for m in (2, 0, 1):
        own_load(m).start()

    barrier = pltpu.get_barrier_semaphore()

    def greet(axis, peer):
        pl.semaphore_signal(barrier, inc=1, device_id={axis: peer}, device_id_type=MESH)

    for k in (1, 2, 3):
        greet("fs", fs_at(k))
        greet("tp", tp_at(k))
    greet("grp", other_grp)

    cuts = wz_r.shape[2]

    def cuts_of(m):
        return range(1 if m == 2 else cuts)

    def piece_rows(m):
        return share if m == 2 else share // cuts

    def w_rows(source, part, m, h):
        return pl.ds(source * block + part * share + h * piece_rows(m), piece_rows(m))

    def far_rows(m, k, h):
        return cast.at[m, k - 1, pl.ds(h * piece_rows(m), piece_rows(m))]

    def wz_sem(m, k, h):
        return wd_r.at[k - 1] if m == 2 else wz_r.at[m, k - 1, h]

    def wz_copy(m, k, h):
        return rcopy(far_rows(m, k, h), w_out[m].at[w_rows(f, g, m, h)],
                     send.at[2], wz_sem(m, k, h), "fs", fs_at(k))

    def wz_arrival(m, k, h):
        return rcopy(far_rows(m, k, h), w_out[m].at[w_rows(fs_at(k), g, m, h)],
                     send.at[2], wz_sem(m, k, h), "fs", fs_at(k))

    def wy_sem(m, k):
        return wy_r.at[0] if m == 2 else wy_r.at[k]

    def wy_copy(m, k, h):
        rows = w_out[m].at[w_rows(fs_at(k), g, m, h)]
        return rcopy(rows, rows, send.at[2], wy_sem(m, k), "grp", other_grp)

    def wy_arrival(m, k, h):
        rows = w_out[m].at[w_rows(fs_at(k), other_grp, m, h)]
        return rcopy(rows, rows, send.at[2], wy_sem(m, k), "grp", other_grp)

    def ints(shape, axis):
        return lax.broadcasted_iota(jnp.int32, shape, axis)

    own_base = (f - lax.rem(f, 2))
    far_base = lax.rem(own_base + 2, 4)
    bases = (own_base, far_base)

    with scope("small_0_wait"):
        small[0].wait()
    first, second = id_rows[0:1, :], id_rows[1:2, :]
    members = [(first >= b) & (first < b + 2) for b in bases]
    square = (tok_rows, tok_rows)
    earlier = (ints(square, 0) < ints(square, 1)).astype(F32).astype(BF16)
    named = jnp.where(ints((8, tok_rows), 0) < 4, members[0].astype(F32), members[1].astype(F32))
    before = jnp.dot(named.astype(BF16), earlier, preferred_element_type=F32)
    ranks = [before[0:1, :], before[4:5, :]]
    kept = [m & (r < capacity) for m, r in zip(members, ranks)]
    seat = [jnp.where(k, r.astype(jnp.int32), -1) for k, r in zip(kept, ranks)]

    with scope("small_1_wait"):
        small[1].wait()

    def fill(i):
        one_hot = jnp.where(ints((lanes, tok_rows), 0) == seat[i], 1.0, 0.0)
        place[i] = one_hot.astype(BF16)
        rows = jnp.dot(place[i, 0:cap, :], tokens[...], preferred_element_type=F32).astype(BF16)
        slots[i] = rows
        return rows

    def slot_copy(k):
        src = slots.at[0] if k == 1 else slots.at[1]
        return rcopy(src, piece.at[t, k], send.at[0], sl_r.at[k], "fs", fs_at(k))

    def relay_copy():
        return rcopy(piece.at[t, 2], piece.at[t, 3], send.at[0], sl_r.at[3], "fs", fs_at(1))

    fill(1)
    with scope("barrier"):
        pl.semaphore_wait(barrier, 3 + 3 + 1)
    slot_copy(2).start()
    piece[t, 0] = fill(0)
    slot_copy(1).start()

    def tx_copy(k):
        src = piece.at[t, k]
        return rcopy(src, src, send.at[1], tx_r.at[k], "tp", tp_at(2))

    def td_copy(k):
        src = piece.at[t, k]
        return rcopy(src, src, send.at[1], td_r.at[k // 3], "tp", tp_at(1))

    def tf_copy(k):
        src = piece.at[tp_at(2), k]
        return rcopy(src, src, send.at[1], tf_r.at[k // 3], "tp", tp_at(1))

    def tx_arrival(k):
        src = piece.at[tp_at(2), k]
        return rcopy(src, src, send.at[1], tx_r.at[k], "tp", tp_at(2))

    def td_arrival(k):
        src = piece.at[tp_at(1), k]
        return rcopy(src, src, send.at[1], td_r.at[k // 3], "tp", tp_at(1))

    def tf_arrival(k):
        src = piece.at[tp_at(3), k]
        return rcopy(src, src, send.at[1], tf_r.at[k // 3], "tp", tp_at(1))

    def spread(k):
        tx_copy(k).start()
        td_copy(k).start()

    spread(0)

    small[2].wait()
    gain_col[...] = jnp.transpose(jnp.broadcast_to(gain[...], (8, block)))[:, 0:1]
    far_gain = gain_col[pl.ds(g * share, share), :]

    def send_far(m, k):
        with scope("far_load_m_k_wait"):
            cast[m, k - 1] = (far_gain * raw_far[m, k - 1]).astype(BF16)
        for h in cuts_of(m):
            wz_copy(m, k, h).start()

    def round_own(m):
        with scope("own_load_m_wait"):
            own_load(m).wait()
        values = raw_own[m]
        if m < 2:
            values = gain_col[...] * values
        w_out[m][pl.ds(f * block, block), :] = values.astype(BF16)

    far_loaded(2)
    for k in (1, 2, 3):
        cast[2, k - 1] = raw_far[2, k - 1].astype(BF16)
        wz_copy(2, k, 0).start()
    far_loaded(0)
    far_loaded(1)

    with scope("small_3_wait"):
        small[3].wait()
    with scope("small_4_wait"):
        small[4].wait()
    group_exp = jnp.exp(group_logits[...])
    group_sum = jnp.sum(group_exp, axis=0, keepdims=True)
    pair_exp = jnp.exp(pair_logits[...])
    pair_weight = pair_exp / jnp.sum(pair_exp, axis=0, keepdims=True)
    group_count = group_exp.shape[0]

    def wm_copy(k):
        return rcopy(wsend.at[k // 2], wrecv.at[k], send.at[3], wm_r.at[0], "fs", fs_at(k))

    chosen = jnp.zeros_like(group_sum)
    for i in range(group_count):
        chosen = chosen + jnp.where((first >= 2 * i) & (first < 2 * i + 2), group_exp[i : i + 1, :], 0.0)
    mix_weight = pair_weight * (chosen / group_sum)
    for i in range(2):
        expert = bases[i] + ints((8, tok_rows), 0)
        rest = jnp.where(first == expert, mix_weight[0:1, :], 0.0)
        rest = rest + jnp.where(second == expert, mix_weight[1:2, :], 0.0)
        total = None
        for _ in range(3):
            head = rest.astype(BF16)
            rest = rest - head.astype(F32)
            term = lax.dot_general(head, place[i], (((1,), (1,)), ((), ())), preferred_element_type=F32)
            total = term if total is None else total + term
        wsend[i] = total
    for k in (1, 2, 3):
        wm_copy(k).start()

    def slot_arrival(k):
        return rcopy(slots.at[0], piece.at[t, k], send.at[0], sl_r.at[k], "fs", fs_at(k))

    with scope("cross"):
        slot_arrival(2).wait_recv()
    relay_copy().start()
    spread(2)
    for k in (1, 2, 3):
        for m in (0, 1):
            send_far(m, k)

    def hand_over(k):
        with scope("hand%d" % k):
            tx_arrival(k).wait_recv()
        tf_copy(k).start()

    def forward(m, k, h):
        with scope("forward%d%d%d" % (m, k, h)):
            wz_arrival(m, k, h).wait_recv()
        wy_copy(m, k, h).start()

    def forward_all(steps, more):
        @pl.when(inner)
        def _():
            for step in steps:
                forward(*step)

        @pl.when(jnp.logical_not(inner))
        def _():
            for step in more:
                forward(*step)

    def arrived(k):
        with scope("arrived"):
            all_here(wy_r.at[k], gate_out.at[pl.ds(0, 2 * share)])

    def land(k):
        with scope("land%d" % k):
            slot_arrival(k).wait_recv()
        spread(k)

    def seat_weights(k, rows):
        cols = jnp.transpose(rows)
        wcol[k] = jnp.where(lax.rem(f, 2) == 0, cols[0:cap, 0:1], cols[0:cap, 1:2])

    hand_over(0)
    round_own(2)
    for i in range(2):
        back_place[i] = jnp.transpose(place[i].astype(F32))[:, 0:cap].astype(BF16)
    seat_weights(0, wsend[0])
    land(1)
    for k in (2, 1, 3):
        forward(2, k, 0)
    hand_over(2)
    hand_over(1)
    for m in (0, 1):
        round_own(m)

    def dw_copy(j):
        src = down_out.at[pl.ds(tp_at(j) * block, block)]
        return rcopy(src, dwn.at[j], send.at[4], dw_r.at[0], "tp", tp_at(j))

    with scope("down_in"):
        all_here(wy_r.at[0], down_out.at[pl.ds(0, 3 * share)])
    for j in (3, 2, 1):
        dw_copy(j).start()
    def steps(*turns):
        return [(m, k, h) for k in turns for m in (0, 1) for h in cuts_of(m)]

    turns = (by_role(1, 2), by_role(2, 1), 3)
    forward_all(steps(1), steps(2))
    land(3)
    forward_all(steps(2), steps(1))
    with scope("weights_in"):
        all_here(wm_r.at[0], wrecv.at[pl.ds(1, 3)])
        for k in (1, 2, 3):
            seat_weights(k, wrecv[k])
    with scope("rows_in"):
        all_here(td_r.at[0], piece.at[t, pl.ds(0, 3)])
        all_here(tf_r.at[0], piece.at[t, pl.ds(0, 3)])

    def products(k, source):
        rows = piece[source, k]
        cols = pl.ds(source * block, block)
        gate = jnp.dot(rows, gate_out[cols, :], preferred_element_type=F32)
        up = jnp.dot(rows, up_out[cols, :], preferred_element_type=F32)
        return gate, up

    def first_products(k, c):
        gate, up = products(k, f)
        acc[0, k], acc[1, k] = gate, up
        return c

    def more_products(kk):
        def step(k, c):
            gate, up = products(k, fs_at(kk))
            acc[0, k] += gate
            acc[1, k] += up
            return c
        return step

    def multiply(step, blocks):
        with scope("products"):
            lax.fori_loop(*blocks, step, 0)

    first = (0, n_fs - 1)
    multiply(first_products, first)
    arrived(turns[0])
    multiply(more_products(turns[0]), first)
    forward_all(steps(3), steps(3))
    hand_over(3)
    with scope("rows_in"):
        all_here(td_r.at[1], piece.at[t, 3])
        all_here(tf_r.at[1], piece.at[t, 3])
    first_products(3, 0)
    more_products(turns[0])(3, 0)
    arrived(turns[1])
    multiply(more_products(turns[1]), (0, n_fs))
    arrived(turns[2])

    spans = [pl.ds(at, min(chunk, cap - at)) for at in range(0, cap, chunk)]
    parts = range(len(spans))

    def h_copy(j, k, c, ssem, rsem, source):
        src, dst = hid.at[source, k, spans[c]], hid.at[source ^ j, k, spans[c]]
        return rcopy(src, dst, ssem, rsem, "tp", tp_at(j))

    def hx_copy(k, c):
        return h_copy(2, k, c, send.at[5], hx_r.at[k, c], 0)

    def hd_copy(k, c):
        return h_copy(1, k, c, send.at[5], hd_r.at[k], 0)

    def hf_copy(k, c):
        return h_copy(1, k, c, send.at[5], hf_r.at[k, c], 2)

    last = fs_at(turns[2])
    blocks = (by_role(1, 3), 2, by_role(3, 1), 0)
    for k in blocks:
        with scope("hidden"):
            gate, up = products(k, last)
            gate = acc[0, k] + gate
            up = acc[1, k] + up
            hid[0, k] = (gate / (1.0 + jnp.exp(-gate)) * up * wcol[k]).astype(BF16)
            for c in parts:
                hx_copy(k, c).start()
                hd_copy(k, c).start()

    with scope("drain"):
        all_here(dw_r.at[0], dwn.at[pl.ds(1, 3)])
        all_sent(0, piece.at[t, pl.ds(0, 3)])
        all_sent(1, piece.at[pl.ds(0, 3)])
        all_sent(2, raw_far)
        all_sent(3, wrecv.at[pl.ds(1, 3)])
        all_sent(4, dwn.at[pl.ds(1, 3)])

    queue = [(k, c) for k in blocks for c in parts]

    def pass_on(n):
        if n < len(queue):
            with scope("hx"):
                hx_copy(*queue[n]).wait_recv()
            hf_copy(*queue[n]).start()

    def result(n):
        k, c = queue[n]

        def term(j):
            rows = down_out[pl.ds(t * block, block), :] if j == 0 else dwn[j]
            return lax.dot_general(
                hid[j, k, spans[c], :], rows, (((1,), (1,)), ((), ())), preferred_element_type=F32)

        if c == 0:
            with scope("hd"):
                all_here(hd_r.at[k], hid.at[1, k])
        total = term(0) + term(1)
        if n == 0:
            pass_on(0)
        total = total + term(2)
        if n > 0:
            pass_on(n + 1)
        with scope("hf"):
            hf_copy(k, c).wait_recv()
        total = total + term(3)
        if n == 0:
            pass_on(1)
        return total

    def part_copy(i, c):
        return rcopy(part_send.at[i, spans[c]], part_recv.at[i, spans[c]],
                     send.at[6 + i // 2], pt_r.at[i, c], "fs", fs_at(1))

    def home_copy(i, c):
        return rcopy(home_send.at[i, spans[c]], back.at[1, spans[c]],
                     send.at[8], hm_r.at[0], "fs", fs_at(2 + i))

    def home_step(n):
        if n < 0 or n >= 2 * len(parts):
            return
        i, c = divmod(n, len(parts))

        @pl.when(inner)
        def _():
            with scope("part%d" % i):
                part_copy(i, c).wait_recv()
            both = keep[i + 1, spans[c], :] + part_recv[i, spans[c], :].astype(F32)
            home_send[i, spans[c], :] = both.astype(BF16)
            home_copy(i, c).start()

    for n in range(len(queue)):
        i, c = divmod(n, len(parts))
        keep[i, spans[c], :] = result(n)

        def send_part(to):
            part_send[to, spans[c], :] = keep[i, spans[c], :].astype(BF16)
            part_copy(to, c).start()

        if i < 3:
            pl.when(jnp.logical_not(inner))(functools.partial(send_part, i))
        if i == 0:
            pl.when(inner)(functools.partial(send_part, 2))
        home_step(n - len(parts) - 1)

    def finish_own():
        for c in parts:
            with scope("part2"):
                part_copy(2, c).wait_recv()
            both = keep[3, spans[c], :] + part_recv[2, spans[c], :].astype(F32)
            back[0, spans[c], :] = both.astype(BF16)

    def finish_far():
        with scope("home"):
            all_here(hm_r.at[0], back.at[1])

    pl.when(inner)(finish_own)
    pl.when(jnp.logical_not(inner))(finish_far)
    sooner, later = by_role(0, 1), by_role(1, 0)
    mix[...] = jnp.dot(back_place[sooner], back[sooner], preferred_element_type=F32)
    pl.when(inner)(finish_far)
    pl.when(jnp.logical_not(inner))(finish_own)
    with scope("last_dot"):
        more = jnp.dot(back_place[later], back[later], preferred_element_type=F32)
        mixed[...] = (mix[...] + more).astype(BF16)

    all_sent(5, hid.at[pl.ds(0, 3)])
    all_sent(7, part_send.at[2])

    @pl.when(inner)
    def _():
        all_sent(8, home_send)

    @pl.when(jnp.logical_not(inner))
    def _():
        all_sent(6, part_send.at[pl.ds(0, 2)])


def pair_body(
    tokens, norm_gain, gate_weight, up_weight, down_weight, expert_ids, group_logits, pair_logits
):
    n_grp, n_fs, n_tp = (lax.axis_size(a) for a in ("grp", "fs", "tp"))
    experts, block, hid = gate_weight.shape
    tok_rows, width = tokens.shape
    share = block // n_grp
    capacity = 5 * tok_rows * 2 // (4 * experts)
    cap = -(-capacity // 16) * 16
    lanes = -(-cap // 128) * 128
    vmem = pl.BlockSpec(memory_space=pltpu.VMEM)
    hbm = pl.BlockSpec(memory_space=pltpu.HBM)
    dma = pltpu.SemaphoreType.DMA
    matrix = jax.ShapeDtypeStruct((n_fs * block, hid), BF16)
    rows = (cap, width)
    chunk = -(-cap // 48) * 16
    spans = -(-cap // chunk)
    sem_shapes = [
        (5,), (3, 2), (9,), (n_fs,), (1,), (n_fs - 1,), (2, n_fs - 1, 4), (n_fs,), (n_fs,), (2,), (2,),
        (1,), (n_fs, spans), (n_fs,), (n_fs, spans), (3, spans), (1,),
    ]
    mixed, *matrices = pl.pallas_call(
        functools.partial(pair_kernel, n_grp, n_fs, n_tp, capacity, chunk),
        out_shape=(jax.ShapeDtypeStruct((tok_rows, width), BF16), matrix, matrix, matrix),
        in_specs=[hbm] * 8,
        out_specs=(vmem,) * 4,
        scratch_shapes=[
            pltpu.VMEM((tok_rows, width), BF16),
            pltpu.VMEM((1, block), F32),
            pltpu.VMEM((2, tok_rows), jnp.int32),
            pltpu.VMEM((group_logits.shape[1], tok_rows), F32),
            pltpu.VMEM((2, tok_rows), F32),
            pltpu.VMEM((block, 1), F32),
            pltpu.VMEM((3, block, hid), F32),
            pltpu.VMEM((3, n_fs - 1, share, hid), F32),
            pltpu.VMEM((3, n_fs - 1, share, hid), BF16),
            pltpu.VMEM((2, *rows), BF16),
            pltpu.VMEM((2, lanes, tok_rows), BF16),
            pltpu.VMEM((2, tok_rows, cap), BF16),
            pltpu.VMEM((2, 8, lanes), F32),
            pltpu.VMEM((n_fs, 8, lanes), F32),
            pltpu.VMEM((n_fs, cap, 1), F32),
            pltpu.VMEM((n_tp, n_fs, *rows), BF16),
            pltpu.VMEM((2, n_fs, cap, hid), F32),
            pltpu.VMEM((n_tp, n_fs, cap, hid), BF16),
            pltpu.VMEM((n_tp, block, hid), BF16),
            pltpu.VMEM((3, *rows), BF16),
            pltpu.VMEM((3, *rows), BF16),
            pltpu.VMEM((n_fs, *rows), F32),
            pltpu.VMEM((2, *rows), BF16),
            pltpu.VMEM((2, *rows), BF16),
            pltpu.VMEM((tok_rows, width), F32),
        ] + [dma(s) for s in sem_shapes],
        compiler_params=pltpu.CompilerParams(
            collective_id=0, has_side_effects=True, vmem_limit_bytes=40 * 1024 * 1024
        ),
    )(*(pltpu.with_memory_space_constraint(x, pltpu.HBM) for x in (
        tokens, norm_gain[None, :], expert_ids.T, group_logits.T, pair_logits.T,
        gate_weight, up_weight, down_weight,
    )))
    return write_out(mixed, *matrices)


def write_kernel(mixed, gate, up, down, *rest):
    outs, sem = rest[:4], rest[4]
    pairs = (
        (gate, outs[1].at[0]), (up, outs[2].at[0]), (down, outs[3].at[0]), (mixed, outs[0])
    )
    for i, (src, dst) in enumerate(pairs):
        rows = src.shape[0] // 4
        for c in range(4):
            at = pl.ds(c * rows, rows)
            pltpu.make_async_copy(src.at[at], dst.at[at], sem.at[i]).start()
    for i, (src, dst) in enumerate(pairs):
        pltpu.make_async_copy(src, dst, sem.at[i]).wait()


def write_out(mixed, *matrices):
    return pl.pallas_call(
        write_kernel,
        out_shape=(
            jax.ShapeDtypeStruct(mixed.shape, BF16),
            *(jax.ShapeDtypeStruct((1, *m.shape), BF16) for m in matrices),
        ),
        in_specs=[pl.BlockSpec(memory_space=pltpu.VMEM)] * 4,
        out_specs=(pl.BlockSpec(memory_space=pltpu.HBM),) * 4,
        scratch_shapes=[pltpu.SemaphoreType.DMA((4,))],
        compiler_params=pltpu.CompilerParams(vmem_limit_bytes=1024 * 1024),
    )(mixed, *matrices)


def paired(mesh, tokens, gate_weight, expert_ids, group_logits):
    n_grp, n_fs, n_tp = (mesh.shape[a] for a in ("grp", "fs", "tp"))
    experts, features, _ = gate_weight.shape
    return (
        experts // group_logits.shape[1] == expert_ids.shape[1] == 2
        and n_fs == n_tp == experts == 4
        and n_grp == 2
    )


def solution(mesh):
    placed = (
        P(("grp", "fs"), "tp"),
        P("fs"),
        P(None, "fs", "tp"),
        P(None, "fs", "tp"),
        P(None, "fs", "tp"),
        P(("grp", "fs"), None),
        P(("grp", "fs"), None),
        P(("grp", "fs"), None),
    )

    def run(tokens, norm_gain, gate_weight, up_weight, down_weight, expert_ids, group_logits, pair_logits):
        args = (tokens, norm_gain, gate_weight, up_weight, down_weight, expert_ids, group_logits, pair_logits)
        special = paired(mesh, tokens, gate_weight, expert_ids, group_logits)
        return jax.shard_map(
            pair_body if special else body,
            mesh=mesh,
            in_specs=placed,
            out_specs=(
                P(("grp", "fs"), "tp"),
                P(("grp", "fs"), None, "tp"),
                P(("grp", "fs"), None, "tp"),
                P(("grp", "fs"), None, "tp"),
            ),
            check_vma=False,
        )(*args)

    return run
```

```python
import functools

import jax
import jax.numpy as jnp
from jax import lax
from jax.experimental import pallas as pl
from jax.experimental.pallas import tpu as pltpu
from jax.sharding import PartitionSpec as P

MESH = pl.DeviceIdType.MESH
BF16 = jnp.bfloat16
F32 = jnp.float32
scope = jax.named_scope


def each(count, step):
    if count <= 4:
        for i in range(count):
            step(i)
    else:
        lax.fori_loop(0, count, lambda i, c: (step(i), c)[1], 0)


def exchange_kernel(
    n_grp, n_fs, n_tp, capacity,
    tokens, gain, id_rows, group_logits, pair_logits, gate_in, up_in, down_in,
    mixed, gate_out, up_out, down_out,
    out_ref, raw, cast, ret, mix, piece, hidden, own, pair_send, pair_recv, x_send, x_recv, result,
    local_sem, raw_sem, slot_s, slot_r, wz_s, wz_r, wy_s, wy_r,
    gx_s, gx_r, gd_s, gd_r, gf_s, gf_r, pr_s, pr_r, xx_s, xx_r, rt_s, rt_r,
):
    g, f, t = lax.axis_index("grp"), lax.axis_index("fs"), lax.axis_index("tp")
    n_x = n_tp // 2
    chip, core = t // 2, lax.rem(t, 2)
    partner = chip * 2 + 1 - core
    width = piece.shape[3]
    block = cast.shape[2]
    tok_rows, padded = tokens.shape[0], out_ref.shape[1]
    experts = n_fs
    share = block // n_grp

    def fs_at(k):
        return lax.rem(f + k, n_fs)

    def outward(i):
        return jnp.where(f < n_fs // 2, i + 1, n_fs - 1 - i)

    def nearest(i):
        if n_fs != 4:
            return outward(i)
        first = jnp.where(f % 2 == 0, 1, 3)
        last = jnp.where(f == 0, 3, jnp.where(f == 3, 1, 2))
        return (first, 6 - first - last, last)[i]

    def grp_at(k):
        return lax.rem(g + k, n_grp)

    def chip_at(k):
        return lax.rem(chip + k, n_x)

    def rcopy(src, dst, ssem, rsem, axis, peer):
        return pltpu.make_async_remote_copy(
            src_ref=src, dst_ref=dst, send_sem=ssem, recv_sem=rsem,
            device_id={axis: peer}, device_id_type=MESH,
        )

    raw_copies = [
        pltpu.make_async_copy(w, raw.at[m], raw_sem.at[m])
        for m, w in enumerate((gate_in, up_in, down_in))
    ]
    for copy in raw_copies:
        copy.start()

    barrier = pltpu.get_barrier_semaphore()

    def greet(axis, peer):
        pl.semaphore_signal(barrier, inc=1, device_id={axis: peer}, device_id_type=MESH)

    each(n_fs - 1, lambda i: greet("fs", fs_at(i + 1)))
    each(n_grp - 1, lambda i: greet("grp", grp_at(i + 1)))
    each(n_x - 1, lambda i: greet("tp", chip_at(i + 1) * 2 + core))
    greet("tp", partner)

    def ints(shape, axis):
        return lax.broadcasted_iota(jnp.int32, shape, axis)

    def route(ids, axis):
        shape = (experts, tok_rows) if axis == 0 else (tok_rows, experts)
        named = [(ints(shape, axis) == i).astype(F32) for i in ids]
        square = (tok_rows, tok_rows)
        earlier = (ints(square, axis) < ints(square, 1 - axis)).astype(F32).astype(BF16)
        both = (named[0] + named[1]).astype(BF16)
        pair = (both, earlier) if axis == 0 else (earlier, both)
        before = jnp.dot(*pair, preferred_element_type=F32)
        picks, kept = [], []
        for i, name in zip(ids, named):
            rank = jnp.sum(before * name, axis=axis, keepdims=True)
            kept.append(rank < capacity)
            slot = i * padded + rank.astype(jnp.int32)
            picks.append(jnp.where(rank < capacity, slot, -1))
        return picks, kept

    row_picks, _ = route([id_rows[0:1, :], id_rows[1:2, :]], 0)

    def fill(k):
        e = fs_at(k)
        slot = ints((padded, tok_rows), 0) + e * padded
        named = (slot == row_picks[0]) | (slot == row_picks[1])
        place = jnp.where(named, 1.0, 0.0).astype(BF16)
        out_ref[e] = jnp.dot(place, tokens[...], preferred_element_type=F32).astype(BF16)

    each(n_fs - 1, lambda i: fill(i + 1))
    pl.semaphore_wait(barrier, n_fs - 1 + n_grp - 1 + n_x - 1 + 1)

    weights = (
        (cast.at[0], gate_out), (cast.at[1], up_out), (cast.at[2], down_out)
    )

    def slot_copy(k, source):
        return rcopy(out_ref.at[fs_at(k)], piece.at[t, source], slot_s.at[k],
                     slot_r.at[n_fs - k], "fs", fs_at(k))

    def slot_arrival(k):
        return rcopy(out_ref.at[f], piece.at[t, fs_at(k)], slot_s.at[k], slot_r.at[k], "fs", fs_at(k))

    each(n_fs - 1, lambda i: slot_copy(outward(i), f).start())
    fill(0)
    own_slots = pltpu.make_async_copy(out_ref.at[f], piece.at[t, f], local_sem.at[3])
    own_slots.start()

    def w_rows(source, part):
        return pl.ds(source * block + part * share, share)

    def wz_copy(m, k):
        w_in, w_out = weights[m]
        return rcopy(w_in.at[fs_at(k), pl.ds(g * share, share)], w_out.at[w_rows(f, g)],
                     wz_s.at[m, k], wz_r.at[m, n_fs - k], "fs", fs_at(k))

    def wz_arrival(m, k):
        w_in, w_out = weights[m]
        return rcopy(w_in.at[fs_at(k), pl.ds(g * share, share)], w_out.at[w_rows(fs_at(k), g)],
                     wz_s.at[m, k], wz_r.at[m, k], "fs", fs_at(k))

    def wy_copy(m, k, j):
        w_out = weights[m][1]
        rows = w_rows(fs_at(k), g)
        return rcopy(w_out.at[rows], w_out.at[rows], wy_s.at[m, k, j],
                     wy_r.at[m, k, n_grp - j], "grp", grp_at(j))

    def wy_arrival(m, k, j):
        w_out = weights[m][1]
        rows = w_rows(fs_at(k), grp_at(j))
        return rcopy(w_out.at[rows], w_out.at[rows], wy_s.at[m, k, j],
                     wy_r.at[m, k, j], "grp", grp_at(j))

    own_weights = []
    for m in range(3):
        w_in, w_out = weights[m]
        raw_copies[m].wait()

        def round_block(e):
            if m < 2:
                cast[m, e] = (gain[...] * raw[m, e]).astype(BF16)
            else:
                cast[m, e] = raw[m, e].astype(BF16)

        each(n_fs, round_block)
        copy = pltpu.make_async_copy(w_in.at[f], w_out.at[pl.ds(f * block, block)], local_sem.at[m])
        copy.start()
        own_weights.append(copy)

    for m in range(3):
        each(n_fs - 1, lambda i: wz_copy(m, outward(i)).start())

    def forward(m, k):
        wz_arrival(m, k).wait_recv()
        for j in range(1, n_grp):
            wy_copy(m, k, j).start()

    def gx_copy(k, j):
        src = piece.at[t, fs_at(k)]
        return rcopy(src, src, gx_s.at[k, j], gx_r.at[k, n_x - j], "tp", chip_at(j) * 2 + core)

    def gx_arrival(k, j):
        src = piece.at[chip_at(j) * 2 + core, fs_at(k)]
        return rcopy(src, src, gx_s.at[k, j], gx_r.at[k, j], "tp", chip_at(j) * 2 + core)

    def gd_copy(k):
        src = piece.at[t, fs_at(k)]
        return rcopy(src, src, gd_s.at[k], gd_r.at[k], "tp", partner)

    def gd_arrival(k):
        src = piece.at[partner, fs_at(k)]
        return rcopy(src, src, gd_s.at[k], gd_r.at[k], "tp", partner)

    def gf_copy(k, j):
        src = piece.at[chip_at(j) * 2 + core, fs_at(k)]
        return rcopy(src, src, gf_s.at[k, j], gf_r.at[k, j], "tp", partner)

    def gf_arrival(k, j):
        src = piece.at[chip_at(j) * 2 + 1 - core, fs_at(k)]
        return rcopy(src, src, gf_s.at[k, j], gf_r.at[k, j], "tp", partner)

    def spread(k):
        for j in range(1, n_x):
            gx_copy(k, j).start()
        gd_copy(k).start()

    own_slots.wait()
    spread(0)

    id_cols = jnp.transpose(id_rows[...])
    ids = [id_cols[:, k : k + 1] for k in range(2)]
    picks, kept = route(ids, 1)
    group_exp = jnp.exp(jnp.transpose(group_logits[...]))
    group_count = group_exp.shape[1]
    low = ints(group_exp.shape, 1) * (experts // group_count)
    member = (ids[0] >= low) & (ids[0] < low + experts // group_count)
    chosen = jnp.sum(jnp.where(member, group_exp, 0.0), axis=1, keepdims=True)
    chosen = chosen / jnp.sum(group_exp, axis=1, keepdims=True)
    pair_exp = jnp.exp(jnp.transpose(pair_logits[...]))
    pair_weight = pair_exp / jnp.sum(pair_exp, axis=1, keepdims=True) * chosen
    mix_weights = [
        jnp.where(kept[k], pair_weight[:, k : k + 1], 0.0) for k in range(2)
    ]

    def blend(k):
        e = fs_at(k)
        slot = ints((tok_rows, padded), 1) + e * padded
        named = (slot == picks[0]) | (slot == picks[1])
        place = jnp.where(named, 1.0, 0.0).astype(BF16)
        weight = jnp.where(ids[0] == e, mix_weights[0], 0.0)
        weight = weight + jnp.where(ids[1] == e, mix_weights[1], 0.0)
        return jnp.dot(place, ret[e], preferred_element_type=F32) * weight

    def spread_arrived(i):
        slot_arrival(nearest(i)).wait_recv()
        spread(nearest(i))

    each(n_fs - 1, spread_arrived)

    def hand_over(k):
        for j in range(1, n_x):
            gx_arrival(k, j).wait_recv()
            gf_copy(k, j).start()

    hand_over(0)

    each(n_fs - 1, lambda i: hand_over(nearest(i)))

    for m in range(3):
        each(n_fs - 1, lambda i: forward(m, nearest(i)))

    def all_in(m):
        own_weights[m].wait()
        for j in range(1, n_grp):
            each(n_fs - 1, lambda i: wy_arrival(m, i + 1, j).wait_recv())

    all_in(0)
    all_in(1)

    def make_hidden(k):
        source = fs_at(k)
        gd_arrival(k).wait_recv()
        for j in range(1, n_x):
            gf_arrival(k, j).wait_recv()
        gate = up = None
        for p in range(n_tp):
            rows = piece[p, source]
            cols = pl.ds(p * width, width)
            gate_part = jnp.dot(rows, gate_out[cols, :], preferred_element_type=F32)
            up_part = jnp.dot(rows, up_out[cols, :], preferred_element_type=F32)
            gate = gate_part if gate is None else gate + gate_part
            up = up_part if up is None else up + up_part
        hidden[k] = (gate / (1.0 + jnp.exp(-gate)) * up).astype(BF16)

    each(n_fs, lambda i: make_hidden(i))
    all_in(2)

    def term(k, j, to_core):
        column = (chip_at(j) * 2 + to_core) * width
        rows = down_out[pl.ds(pl.multiple_of(column, width), width), :]
        return lax.dot_general(hidden[k], rows, (((1,), (1,)), ((), ())), preferred_element_type=F32)

    def pr_copy(k):
        return rcopy(pair_send.at[k], pair_recv.at[k], pr_s.at[k], pr_r.at[k], "tp", partner)

    def stage_pair(k):
        for j in range(n_x):
            pair_send[k, j] = term(k, j, 1 - core).astype(BF16)
        pr_copy(k).start()
        for j in range(n_x):
            own[k, j] = term(k, j, core)

    def xx_copy(k, j):
        return rcopy(x_send.at[k, j], x_recv.at[k, n_x - j], xx_s.at[k, j], xx_r.at[k, n_x - j],
                     "tp", chip_at(j) * 2 + core)

    def xx_arrival(k, j):
        return rcopy(x_send.at[k, j], x_recv.at[k, j], xx_s.at[k, j], xx_r.at[k, j],
                     "tp", chip_at(j) * 2 + core)

    def stage_chip(k):
        pr_copy(k).wait_recv()
        for j in range(1, n_x):
            x_send[k, j] = (own[k, j] + pair_recv[k, j].astype(F32)).astype(BF16)
            xx_copy(k, j).start()
        own[k, 0] = own[k, 0] + pair_recv[k, 0].astype(F32)

    def rt_copy(k):
        return rcopy(result.at[k], ret.at[f], rt_s.at[k], rt_r.at[n_fs - k], "fs", fs_at(k))

    def rt_arrival(k):
        return rcopy(result.at[k], ret.at[fs_at(k)], rt_s.at[k], rt_r.at[k], "fs", fs_at(k))

    def total(k):
        acc = own[k, 0]
        for j in range(1, n_x):
            xx_arrival(k, j).wait_recv()
            acc = acc + x_recv[k, j].astype(F32)
        return acc.astype(BF16)

    def stage_home(k):
        result[k] = total(k)
        rt_copy(k).start()

    def order(i):
        return lax.rem(outward(i) + n_fs, n_fs)

    stage_pair(order(0))

    def pair_and_chip(i):
        stage_pair(order(i + 1))
        stage_chip(order(i))

    each(n_fs - 1, pair_and_chip)
    stage_chip(order(n_fs - 1))
    each(n_fs - 1, lambda i: stage_home(order(i)))
    ret[f] = total(0)
    mix[...] = blend(0)

    def collect(i):
        k = nearest(i)
        rt_arrival(k).wait_recv()
        mix[...] += blend(k)

    each(n_fs - 1, collect)
    mixed[...] = mix[...].astype(BF16)

    def drain_peer(i):
        k = i + 1
        slot_copy(k, f).wait_send()
        rt_copy(k).wait_send()
        for m in range(3):
            wz_copy(m, k).wait_send()
            for j in range(1, n_grp):
                wy_copy(m, k, j).wait_send()

    def drain_chunk(k):
        gd_copy(k).wait_send()
        pr_copy(k).wait_send()
        for j in range(1, n_x):
            gx_copy(k, j).wait_send()
            gf_copy(k, j).wait_send()
            xx_copy(k, j).wait_send()

    each(n_fs - 1, drain_peer)
    each(n_fs, drain_chunk)


def body(
    tokens, norm_gain, gate_weight, up_weight, down_weight, expert_ids, group_logits, pair_logits
):
    n_grp, n_fs, n_tp = (lax.axis_size(a) for a in ("grp", "fs", "tp"))
    n_x = n_tp // 2
    experts, block, hid = gate_weight.shape
    tok_rows, width = tokens.shape
    capacity = 5 * tok_rows * 2 // (4 * experts)
    cap = -(-capacity // 16) * 16
    vmem = pl.BlockSpec(memory_space=pltpu.VMEM)
    hbm = pl.BlockSpec(memory_space=pl.ANY)
    dma = pltpu.SemaphoreType.DMA
    matrix = jax.ShapeDtypeStruct((n_fs * block, hid), BF16)
    chunk = (n_fs, n_x, cap, width)
    sem_shapes = [
        (4,), (3,), (n_fs,), (n_fs,), (3, n_fs), (3, n_fs), (3, n_fs, n_grp), (3, n_fs, n_grp),
        (n_fs, n_x), (n_fs, n_x), (n_fs,), (n_fs,), (n_fs, n_x), (n_fs, n_x),
        (n_fs,), (n_fs,), (n_fs, n_x), (n_fs, n_x), (n_fs,), (n_fs,),
    ]
    mixed, *matrices = pl.pallas_call(
        functools.partial(exchange_kernel, n_grp, n_fs, n_tp, capacity),
        out_shape=(jax.ShapeDtypeStruct((tok_rows, width), BF16), matrix, matrix, matrix),
        in_specs=[vmem] * 5 + [hbm] * 3,
        out_specs=(vmem,) * 4,
        scratch_shapes=[
            pltpu.VMEM((n_fs, cap, width), BF16),
            pltpu.VMEM((3, n_fs, block, hid), F32),
            pltpu.VMEM((3, n_fs, block, hid), BF16),
            pltpu.VMEM((n_fs, cap, width), BF16),
            pltpu.VMEM((tok_rows, width), F32),
            pltpu.VMEM((n_tp, n_fs, cap, width), BF16),
            pltpu.VMEM((n_fs, cap, hid), BF16),
            pltpu.VMEM(chunk, F32),
            pltpu.VMEM(chunk, BF16),
            pltpu.VMEM(chunk, BF16),
            pltpu.VMEM(chunk, BF16),
            pltpu.VMEM(chunk, BF16),
            pltpu.VMEM((n_fs, cap, width), BF16),
        ] + [dma(s) for s in sem_shapes],
        compiler_params=pltpu.CompilerParams(
            collective_id=0, has_side_effects=True, vmem_limit_bytes=48 * 1024 * 1024
        ),
    )(
        tokens, norm_gain[:, None], expert_ids.T, group_logits.T, pair_logits.T,
        gate_weight, up_weight, down_weight,
    )
    return (mixed, *(m[None] for m in matrices))


def pair_kernel(
    n_grp, n_fs, n_tp, capacity, chunk,
    tokens_in, gain_in, ids_in, group_in, pair_in, gate_in, up_in, down_in,
    mixed, gate_out, up_out, down_out,
    tokens, gain, id_rows, group_logits, pair_logits, gain_col,
    raw_own, raw_far, cast, slots, place, back_place, wsend, wrecv, wcol,
    piece, acc, hid, dwn, part_send, part_recv, keep, home_send, back, mix,
    in_sem, raw_sem, send, sl_r, wm_r, wd_r, wz_r, wy_r, tx_r, td_r, tf_r,
    dw_r, hx_r, hd_r, hf_r, pt_r, hm_r,
):
    g, f, t = lax.axis_index("grp"), lax.axis_index("fs"), lax.axis_index("tp")
    cap, width = piece.shape[2], piece.shape[3]
    block, hidden_units = raw_own.shape[1], raw_own.shape[2]
    share = raw_far.shape[2]
    tok_rows = tokens.shape[0]
    lanes = place.shape[1]
    pair = n_fs // 2

    inner = (f == 1) | (f == 2)

    def flip(i, k):
        return (i, i + 1 - 2 * lax.rem(i, 2), lax.rem(i + 2, 4), 3 - i)[k]

    def fs_at(k):
        if isinstance(k, int):
            return flip(f, k)
        return jnp.where(k == 1, flip(f, 1), jnp.where(k == 2, flip(f, 2), flip(f, 3)))

    def by_role(at_inner, at_outer):
        return jnp.where(inner, at_inner, at_outer)

    def tp_at(j):
        return flip(t, j)

    other_grp = 1 - g

    def rcopy(src, dst, ssem, rsem, axis, peer):
        return pltpu.make_async_remote_copy(
            src_ref=src, dst_ref=dst, send_sem=ssem, recv_sem=rsem,
            device_id={axis: peer}, device_id_type=MESH,
        )

    def all_sent(index, ref):
        rcopy(ref, ref, send.at[index], send.at[index], "fs", fs_at(1)).wait_send()

    def all_here(sem, ref):
        rcopy(ref, ref, sem, sem, "fs", fs_at(1)).wait_recv()

    small = [
        pltpu.make_async_copy(src, dst, in_sem.at[i])
        for i, (src, dst) in enumerate((
            (ids_in, id_rows), (tokens_in, tokens), (gain_in, gain),
            (group_in, group_logits), (pair_in, pair_logits),
        ))
    ]
    w_in = (gate_in, up_in, down_in)
    w_out = (gate_out, up_out, down_out)

    def far_load(m, k):
        return pltpu.make_async_copy(
            w_in[m].at[fs_at(k), pl.ds(g * share, share)], raw_far.at[m, k - 1], raw_sem.at[m, 1]
        )

    def far_loaded(m):
        whole = w_in[m].at[pl.ds(0, 3), pl.ds(0, share)]
        pltpu.make_async_copy(whole, raw_far.at[m], raw_sem.at[m, 1]).wait()

    def own_load(m):
        return pltpu.make_async_copy(w_in[m].at[f], raw_own.at[m], raw_sem.at[m, 0])

    for copy in small:
        copy.start()
    for m in (2, 0, 1):
        for k in (1, 2, 3):
            far_load(m, k).start()
    for m in (2, 0, 1):
        own_load(m).start()

    barrier = pltpu.get_barrier_semaphore()

    def greet(axis, peer):
        pl.semaphore_signal(barrier, inc=1, device_id={axis: peer}, device_id_type=MESH)

    for k in (1, 2, 3):
        greet("fs", fs_at(k))
        greet("tp", tp_at(k))
    greet("grp", other_grp)

    cuts = wz_r.shape[2]

    def cuts_of(m):
        return range(1 if m == 2 else cuts)

    def piece_rows(m):
        return share if m == 2 else share // cuts

    def w_rows(source, part, m, h):
        return pl.ds(source * block + part * share + h * piece_rows(m), piece_rows(m))

    def far_rows(m, k, h):
        return cast.at[m, k - 1, pl.ds(h * piece_rows(m), piece_rows(m))]

    def wz_sem(m, k, h):
        return wd_r.at[k - 1] if m == 2 else wz_r.at[m, k - 1, h]

    def wz_copy(m, k, h):
        return rcopy(far_rows(m, k, h), w_out[m].at[w_rows(f, g, m, h)],
                     send.at[2], wz_sem(m, k, h), "fs", fs_at(k))

    def wz_arrival(m, k, h):
        return rcopy(far_rows(m, k, h), w_out[m].at[w_rows(fs_at(k), g, m, h)],
                     send.at[2], wz_sem(m, k, h), "fs", fs_at(k))

    def wy_sem(m, k):
        return wy_r.at[0] if m == 2 else wy_r.at[k]

    def wy_copy(m, k, h):
        rows = w_out[m].at[w_rows(fs_at(k), g, m, h)]
        return rcopy(rows, rows, send.at[2], wy_sem(m, k), "grp", other_grp)

    def wy_arrival(m, k, h):
        rows = w_out[m].at[w_rows(fs_at(k), other_grp, m, h)]
        return rcopy(rows, rows, send.at[2], wy_sem(m, k), "grp", other_grp)

    def ints(shape, axis):
        return lax.broadcasted_iota(jnp.int32, shape, axis)

    own_base = (f - lax.rem(f, 2))
    far_base = lax.rem(own_base + 2, 4)
    bases = (own_base, far_base)

    with scope("small_0_wait"):
        small[0].wait()
    first, second = id_rows[0:1, :], id_rows[1:2, :]
    members = [(first >= b) & (first < b + 2) for b in bases]
    square = (tok_rows, tok_rows)
    earlier = (ints(square, 0) < ints(square, 1)).astype(F32).astype(BF16)
    named = jnp.where(ints((8, tok_rows), 0) < 4, members[0].astype(F32), members[1].astype(F32))
    before = jnp.dot(named.astype(BF16), earlier, preferred_element_type=F32)
    ranks = [before[0:1, :], before[4:5, :]]
    kept = [m & (r < capacity) for m, r in zip(members, ranks)]
    seat = [jnp.where(k, r.astype(jnp.int32), -1) for k, r in zip(kept, ranks)]

    with scope("small_1_wait"):
        small[1].wait()

    def fill(i):
        one_hot = jnp.where(ints((lanes, tok_rows), 0) == seat[i], 1.0, 0.0)
        place[i] = one_hot.astype(BF16)
        rows = jnp.dot(place[i, 0:cap, :], tokens[...], preferred_element_type=F32).astype(BF16)
        slots[i] = rows
        return rows

    def slot_copy(k):
        src = slots.at[0] if k == 1 else slots.at[1]
        return rcopy(src, piece.at[t, k], send.at[0], sl_r.at[k], "fs", fs_at(k))

    def relay_copy():
        return rcopy(piece.at[t, 2], piece.at[t, 3], send.at[0], sl_r.at[3], "fs", fs_at(1))

    fill(1)
    with scope("barrier"):
        pl.semaphore_wait(barrier, 3 + 3 + 1)
    slot_copy(2).start()
    piece[t, 0] = fill(0)
    slot_copy(1).start()

    def tx_copy(k):
        src = piece.at[t, k]
        return rcopy(src, src, send.at[1], tx_r.at[k], "tp", tp_at(2))

    def td_copy(k):
        src = piece.at[t, k]
        return rcopy(src, src, send.at[1], td_r.at[k // 3], "tp", tp_at(1))

    def tf_copy(k):
        src = piece.at[tp_at(2), k]
        return rcopy(src, src, send.at[1], tf_r.at[k // 3], "tp", tp_at(1))

    def tx_arrival(k):
        src = piece.at[tp_at(2), k]
        return rcopy(src, src, send.at[1], tx_r.at[k], "tp", tp_at(2))

    def td_arrival(k):
        src = piece.at[tp_at(1), k]
        return rcopy(src, src, send.at[1], td_r.at[k // 3], "tp", tp_at(1))

    def tf_arrival(k):
        src = piece.at[tp_at(3), k]
        return rcopy(src, src, send.at[1], tf_r.at[k // 3], "tp", tp_at(1))

    def spread(k):
        tx_copy(k).start()
        td_copy(k).start()

    spread(0)

    small[2].wait()
    gain_col[...] = jnp.transpose(jnp.broadcast_to(gain[...], (8, block)))[:, 0:1]
    far_gain = gain_col[pl.ds(g * share, share), :]

    def send_far(m, k):
        with scope("far_load_m_k_wait"):
            cast[m, k - 1] = (far_gain * raw_far[m, k - 1]).astype(BF16)
        for h in cuts_of(m):
            wz_copy(m, k, h).start()

    def round_own(m):
        with scope("own_load_m_wait"):
            own_load(m).wait()
        values = raw_own[m]
        if m < 2:
            values = gain_col[...] * values
        w_out[m][pl.ds(f * block, block), :] = values.astype(BF16)

    far_loaded(2)
    for k in (1, 2, 3):
        cast[2, k - 1] = raw_far[2, k - 1].astype(BF16)
        wz_copy(2, k, 0).start()
    far_loaded(0)
    far_loaded(1)

    with scope("small_3_wait"):
        small[3].wait()
    with scope("small_4_wait"):
        small[4].wait()
    group_exp = jnp.exp(group_logits[...])
    group_sum = jnp.sum(group_exp, axis=0, keepdims=True)
    pair_exp = jnp.exp(pair_logits[...])
    pair_weight = pair_exp / jnp.sum(pair_exp, axis=0, keepdims=True)
    group_count = group_exp.shape[0]

    def wm_copy(k):
        return rcopy(wsend.at[k // 2], wrecv.at[k], send.at[3], wm_r.at[0], "fs", fs_at(k))

    chosen = jnp.zeros_like(group_sum)
    for i in range(group_count):
        chosen = chosen + jnp.where((first >= 2 * i) & (first < 2 * i + 2), group_exp[i : i + 1, :], 0.0)
    mix_weight = pair_weight * (chosen / group_sum)
    for i in range(2):
        expert = bases[i] + ints((8, tok_rows), 0)
        rest = jnp.where(first == expert, mix_weight[0:1, :], 0.0)
        rest = rest + jnp.where(second == expert, mix_weight[1:2, :], 0.0)
        total = None
        for _ in range(3):
            head = rest.astype(BF16)
            rest = rest - head.astype(F32)
            term = lax.dot_general(head, place[i], (((1,), (1,)), ((), ())), preferred_element_type=F32)
            total = term if total is None else total + term
        wsend[i] = total
    for k in (1, 2, 3):
        wm_copy(k).start()

    def slot_arrival(k):
        return rcopy(slots.at[0], piece.at[t, k], send.at[0], sl_r.at[k], "fs", fs_at(k))

    with scope("cross"):
        slot_arrival(2).wait_recv()
    relay_copy().start()
    spread(2)
    for k in (1, 2, 3):
        for m in (0, 1):
            send_far(m, k)

    def hand_over(k):
        with scope("hand%d" % k):
            tx_arrival(k).wait_recv()
        tf_copy(k).start()

    def forward(m, k, h):
        with scope("forward%d%d%d" % (m, k, h)):
            wz_arrival(m, k, h).wait_recv()
        wy_copy(m, k, h).start()

    def forward_all(steps, more):
        @pl.when(inner)
        def _():
            for step in steps:
                forward(*step)

        @pl.when(jnp.logical_not(inner))
        def _():
            for step in more:
                forward(*step)

    def arrived(k):
        with scope("arrived"):
            all_here(wy_r.at[k], gate_out.at[pl.ds(0, 2 * share)])

    def land(k):
        with scope("land%d" % k):
            slot_arrival(k).wait_recv()
        spread(k)

    def seat_weights(k, rows):
        cols = jnp.transpose(rows)
        wcol[k] = jnp.where(lax.rem(f, 2) == 0, cols[0:cap, 0:1], cols[0:cap, 1:2])

    hand_over(0)
    round_own(2)
    for i in range(2):
        back_place[i] = jnp.transpose(place[i].astype(F32))[:, 0:cap].astype(BF16)
    seat_weights(0, wsend[0])
    land(1)
    for k in (2, 1, 3):
        forward(2, k, 0)
    hand_over(2)
    hand_over(1)
    for m in (0, 1):
        round_own(m)

    def dw_copy(j):
        src = down_out.at[pl.ds(tp_at(j) * block, block)]
        return rcopy(src, dwn.at[j], send.at[4], dw_r.at[0], "tp", tp_at(j))

    with scope("down_in"):
        all_here(wy_r.at[0], down_out.at[pl.ds(0, 3 * share)])
    for j in (3, 2, 1):
        dw_copy(j).start()
    def steps(*turns):
        return [(m, k, h) for k in turns for m in (0, 1) for h in cuts_of(m)]

    turns = (by_role(1, 2), by_role(2, 1), 3)
    forward_all(steps(1), steps(2))
    land(3)
    forward_all(steps(2), steps(1))
    with scope("weights_in"):
        all_here(wm_r.at[0], wrecv.at[pl.ds(1, 3)])
        for k in (1, 2, 3):
            seat_weights(k, wrecv[k])
    with scope("rows_in"):
        all_here(td_r.at[0], piece.at[t, pl.ds(0, 3)])
        all_here(tf_r.at[0], piece.at[t, pl.ds(0, 3)])

    def products(k, source):
        rows = piece[source, k]
        cols = pl.ds(source * block, block)
        gate = jnp.dot(rows, gate_out[cols, :], preferred_element_type=F32)
        up = jnp.dot(rows, up_out[cols, :], preferred_element_type=F32)
        return gate, up

    def first_products(k, c):
        gate, up = products(k, f)
        acc[0, k], acc[1, k] = gate, up
        return c

    def more_products(kk):
        def step(k, c):
            gate, up = products(k, fs_at(kk))
            acc[0, k] += gate
            acc[1, k] += up
            return c
        return step

    def multiply(step, blocks):
        with scope("products"):
            lax.fori_loop(*blocks, step, 0)

    first = (0, n_fs - 1)
    multiply(first_products, first)
    arrived(turns[0])
    multiply(more_products(turns[0]), first)
    forward_all(steps(3), steps(3))
    hand_over(3)
    arrived(turns[1])
    multiply(more_products(turns[1]), first)
    with scope("rows_in"):
        all_here(td_r.at[1], piece.at[t, 3])
        all_here(tf_r.at[1], piece.at[t, 3])
    first_products(3, 0)
    more_products(turns[0])(3, 0)
    more_products(turns[1])(3, 0)
    arrived(turns[2])

    edges = (0, *chunk, cap)
    spans = [pl.ds(a, b - a) for a, b in zip(edges, edges[1:])]
    parts = range(len(spans))

    def h_copy(j, k, c, ssem, rsem, source):
        src, dst = hid.at[source, k, spans[c]], hid.at[source ^ j, k, spans[c]]
        return rcopy(src, dst, ssem, rsem, "tp", tp_at(j))

    def hx_copy(k, c):
        return h_copy(2, k, c, send.at[5], hx_r.at[k, c], 0)

    def hd_copy(k, c):
        return h_copy(1, k, c, send.at[5], hd_r.at[k], 0)

    def hf_copy(k, c):
        return h_copy(1, k, c, send.at[5], hf_r.at[k, c], 2)

    last = fs_at(turns[2])
    blocks = (by_role(1, 3), 2, by_role(3, 1), 0)
    for k in blocks:
        with scope("hidden"):
            gate, up = products(k, last)
            gate = acc[0, k] + gate
            up = acc[1, k] + up
            hid[0, k] = (gate / (1.0 + jnp.exp(-gate)) * up * wcol[k]).astype(BF16)
            for c in parts:
                hx_copy(k, c).start()
                hd_copy(k, c).start()

    with scope("drain"):
        all_here(dw_r.at[0], dwn.at[pl.ds(1, 3)])
        all_sent(0, piece.at[t, pl.ds(0, 3)])
        all_sent(1, piece.at[pl.ds(0, 3)])
        all_sent(2, raw_far)
        all_sent(3, wrecv.at[pl.ds(1, 3)])
        all_sent(4, dwn.at[pl.ds(1, 3)])

    queue = [(k, c) for k in blocks for c in parts]

    def pass_on(n):
        if n < len(queue):
            with scope("hx"):
                hx_copy(*queue[n]).wait_recv()
            hf_copy(*queue[n]).start()

    def result(n):
        k, c = queue[n]

        def term(j):
            rows = down_out[pl.ds(t * block, block), :] if j == 0 else dwn[j]
            return lax.dot_general(
                hid[j, k, spans[c], :], rows, (((1,), (1,)), ((), ())), preferred_element_type=F32)

        if c == 0:
            with scope("hd"):
                all_here(hd_r.at[k], hid.at[1, k])
        total = term(0) + term(1)
        if n == 0:
            pass_on(0)
        total = total + term(2)
        if n > 0:
            pass_on(n + 1)
        with scope("hf"):
            hf_copy(k, c).wait_recv()
        total = total + term(3)
        if n == 0:
            pass_on(1)
        return total

    def part_copy(i, c):
        return rcopy(part_send.at[i, spans[c]], part_recv.at[i, spans[c]],
                     send.at[6 + i // 2], pt_r.at[i, c], "fs", fs_at(1))

    def home_copy(i, c):
        return rcopy(home_send.at[i, spans[c]], back.at[1, spans[c]],
                     send.at[8], hm_r.at[0], "fs", fs_at(2 + i))

    def home_step(n):
        if n < 0 or n >= 2 * len(parts):
            return
        i, c = divmod(n, len(parts))

        @pl.when(inner)
        def _():
            with scope("part%d" % i):
                part_copy(i, c).wait_recv()
            both = keep[i + 1, spans[c], :] + part_recv[i, spans[c], :].astype(F32)
            home_send[i, spans[c], :] = both.astype(BF16)
            home_copy(i, c).start()

    for n in range(len(queue)):
        i, c = divmod(n, len(parts))
        keep[i, spans[c], :] = result(n)

        def send_part(to):
            part_send[to, spans[c], :] = keep[i, spans[c], :].astype(BF16)
            part_copy(to, c).start()

        if i < 3:
            pl.when(jnp.logical_not(inner))(functools.partial(send_part, i))
        if i == 0:
            pl.when(inner)(functools.partial(send_part, 2))
        home_step(n - len(parts) - 1)

    def finish_own():
        for c in parts:
            with scope("part2"):
                part_copy(2, c).wait_recv()
            both = keep[3, spans[c], :] + part_recv[2, spans[c], :].astype(F32)
            back[0, spans[c], :] = both.astype(BF16)

    def finish_far():
        with scope("home"):
            all_here(hm_r.at[0], back.at[1])

    pl.when(inner)(finish_own)
    pl.when(jnp.logical_not(inner))(finish_far)
    sooner, later = by_role(0, 1), by_role(1, 0)
    mix[...] = jnp.dot(back_place[sooner], back[sooner], preferred_element_type=F32)
    pl.when(inner)(finish_far)
    pl.when(jnp.logical_not(inner))(finish_own)
    with scope("last_dot"):
        more = jnp.dot(back_place[later], back[later], preferred_element_type=F32)
        mixed[...] = (mix[...] + more).astype(BF16)

    all_sent(5, hid.at[pl.ds(0, 3)])
    all_sent(7, part_send.at[2])

    @pl.when(inner)
    def _():
        all_sent(8, home_send)

    @pl.when(jnp.logical_not(inner))
    def _():
        all_sent(6, part_send.at[pl.ds(0, 2)])


def pair_body(
    tokens, norm_gain, gate_weight, up_weight, down_weight, expert_ids, group_logits, pair_logits
):
    n_grp, n_fs, n_tp = (lax.axis_size(a) for a in ("grp", "fs", "tp"))
    experts, block, hid = gate_weight.shape
    tok_rows, width = tokens.shape
    share = block // n_grp
    capacity = 5 * tok_rows * 2 // (4 * experts)
    cap = -(-capacity // 16) * 16
    lanes = -(-cap // 128) * 128
    vmem = pl.BlockSpec(memory_space=pltpu.VMEM)
    hbm = pl.BlockSpec(memory_space=pltpu.HBM)
    dma = pltpu.SemaphoreType.DMA
    matrix = jax.ShapeDtypeStruct((n_fs * block, hid), BF16)
    rows = (cap, width)
    chunk = (cap // 80 * 16, cap // 80 * 16 * 2, cap // 80 * 16 * 3)
    spans = len(chunk) + 1
    sem_shapes = [
        (5,), (3, 2), (9,), (n_fs,), (1,), (n_fs - 1,), (2, n_fs - 1, 4), (n_fs,), (n_fs,), (2,), (2,),
        (1,), (n_fs, spans), (n_fs,), (n_fs, spans), (3, spans), (1,),
    ]
    mixed, *matrices = pl.pallas_call(
        functools.partial(pair_kernel, n_grp, n_fs, n_tp, capacity, chunk),
        out_shape=(jax.ShapeDtypeStruct((tok_rows, width), BF16), matrix, matrix, matrix),
        in_specs=[hbm] * 8,
        out_specs=(vmem,) * 4,
        scratch_shapes=[
            pltpu.VMEM((tok_rows, width), BF16),
            pltpu.VMEM((1, block), F32),
            pltpu.VMEM((2, tok_rows), jnp.int32),
            pltpu.VMEM((group_logits.shape[1], tok_rows), F32),
            pltpu.VMEM((2, tok_rows), F32),
            pltpu.VMEM((block, 1), F32),
            pltpu.VMEM((3, block, hid), F32),
            pltpu.VMEM((3, n_fs - 1, share, hid), F32),
            pltpu.VMEM((3, n_fs - 1, share, hid), BF16),
            pltpu.VMEM((2, *rows), BF16),
            pltpu.VMEM((2, lanes, tok_rows), BF16),
            pltpu.VMEM((2, tok_rows, cap), BF16),
            pltpu.VMEM((2, 8, lanes), F32),
            pltpu.VMEM((n_fs, 8, lanes), F32),
            pltpu.VMEM((n_fs, cap, 1), F32),
            pltpu.VMEM((n_tp, n_fs, *rows), BF16),
            pltpu.VMEM((2, n_fs, cap, hid), F32),
            pltpu.VMEM((n_tp, n_fs, cap, hid), BF16),
            pltpu.VMEM((n_tp, block, hid), BF16),
            pltpu.VMEM((3, *rows), BF16),
            pltpu.VMEM((3, *rows), BF16),
            pltpu.VMEM((n_fs, *rows), F32),
            pltpu.VMEM((2, *rows), BF16),
            pltpu.VMEM((2, *rows), BF16),
            pltpu.VMEM((tok_rows, width), F32),
        ] + [dma(s) for s in sem_shapes],
        compiler_params=pltpu.CompilerParams(
            collective_id=0, has_side_effects=True, vmem_limit_bytes=40 * 1024 * 1024
        ),
    )(*(pltpu.with_memory_space_constraint(x, pltpu.HBM) for x in (
        tokens, norm_gain[None, :], expert_ids.T, group_logits.T, pair_logits.T,
        gate_weight, up_weight, down_weight,
    )))
    return write_out(mixed, *matrices)


def write_kernel(mixed, gate, up, down, *rest):
    outs, sem = rest[:4], rest[4]
    pairs = (
        (gate, outs[1].at[0]), (up, outs[2].at[0]), (down, outs[3].at[0]), (mixed, outs[0])
    )
    for i, (src, dst) in enumerate(pairs):
        rows = src.shape[0] // 4
        for c in range(4):
            at = pl.ds(c * rows, rows)
            pltpu.make_async_copy(src.at[at], dst.at[at], sem.at[i]).start()
    for i, (src, dst) in enumerate(pairs):
        pltpu.make_async_copy(src, dst, sem.at[i]).wait()


def write_out(mixed, *matrices):
    return pl.pallas_call(
        write_kernel,
        out_shape=(
            jax.ShapeDtypeStruct(mixed.shape, BF16),
            *(jax.ShapeDtypeStruct((1, *m.shape), BF16) for m in matrices),
        ),
        in_specs=[pl.BlockSpec(memory_space=pltpu.VMEM)] * 4,
        out_specs=(pl.BlockSpec(memory_space=pltpu.HBM),) * 4,
        scratch_shapes=[pltpu.SemaphoreType.DMA((4,))],
        compiler_params=pltpu.CompilerParams(vmem_limit_bytes=1024 * 1024),
    )(mixed, *matrices)


def paired(mesh, tokens, gate_weight, expert_ids, group_logits):
    n_grp, n_fs, n_tp = (mesh.shape[a] for a in ("grp", "fs", "tp"))
    experts, features, _ = gate_weight.shape
    return (
        experts // group_logits.shape[1] == expert_ids.shape[1] == 2
        and n_fs == n_tp == experts == 4
        and n_grp == 2
    )


def solution(mesh):
    placed = (
        P(("grp", "fs"), "tp"),
        P("fs"),
        P(None, "fs", "tp"),
        P(None, "fs", "tp"),
        P(None, "fs", "tp"),
        P(("grp", "fs"), None),
        P(("grp", "fs"), None),
        P(("grp", "fs"), None),
    )

    def run(tokens, norm_gain, gate_weight, up_weight, down_weight, expert_ids, group_logits, pair_logits):
        args = (tokens, norm_gain, gate_weight, up_weight, down_weight, expert_ids, group_logits, pair_logits)
        special = paired(mesh, tokens, gate_weight, expert_ids, group_logits)
        return jax.shard_map(
            pair_body if special else body,
            mesh=mesh,
            in_specs=placed,
            out_specs=(
                P(("grp", "fs"), "tp"),
                P(("grp", "fs"), None, "tp"),
                P(("grp", "fs"), None, "tp"),
                P(("grp", "fs"), None, "tp"),
            ),
            check_vma=False,
        )(*args)

    return run
```

```python
import functools

import jax
import jax.numpy as jnp
from jax import lax
from jax.experimental import pallas as pl
from jax.experimental.pallas import tpu as pltpu
from jax.sharding import PartitionSpec as P

MESH = pl.DeviceIdType.MESH
BF16 = jnp.bfloat16
F32 = jnp.float32
scope = jax.named_scope


def each(count, step):
    if count <= 4:
        for i in range(count):
            step(i)
    else:
        lax.fori_loop(0, count, lambda i, c: (step(i), c)[1], 0)


def exchange_kernel(
    n_grp, n_fs, n_tp, capacity,
    tokens, gain, id_rows, group_logits, pair_logits, gate_in, up_in, down_in,
    mixed, gate_out, up_out, down_out,
    out_ref, raw, cast, ret, mix, piece, hidden, own, pair_send, pair_recv, x_send, x_recv, result,
    local_sem, raw_sem, slot_s, slot_r, wz_s, wz_r, wy_s, wy_r,
    gx_s, gx_r, gd_s, gd_r, gf_s, gf_r, pr_s, pr_r, xx_s, xx_r, rt_s, rt_r,
):
    g, f, t = lax.axis_index("grp"), lax.axis_index("fs"), lax.axis_index("tp")
    n_x = n_tp // 2
    chip, core = t // 2, lax.rem(t, 2)
    partner = chip * 2 + 1 - core
    width = piece.shape[3]
    block = cast.shape[2]
    tok_rows, padded = tokens.shape[0], out_ref.shape[1]
    experts = n_fs
    share = block // n_grp

    def fs_at(k):
        return lax.rem(f + k, n_fs)

    def outward(i):
        return jnp.where(f < n_fs // 2, i + 1, n_fs - 1 - i)

    def nearest(i):
        if n_fs != 4:
            return outward(i)
        first = jnp.where(f % 2 == 0, 1, 3)
        last = jnp.where(f == 0, 3, jnp.where(f == 3, 1, 2))
        return (first, 6 - first - last, last)[i]

    def grp_at(k):
        return lax.rem(g + k, n_grp)

    def chip_at(k):
        return lax.rem(chip + k, n_x)

    def rcopy(src, dst, ssem, rsem, axis, peer):
        return pltpu.make_async_remote_copy(
            src_ref=src, dst_ref=dst, send_sem=ssem, recv_sem=rsem,
            device_id={axis: peer}, device_id_type=MESH,
        )

    raw_copies = [
        pltpu.make_async_copy(w, raw.at[m], raw_sem.at[m])
        for m, w in enumerate((gate_in, up_in, down_in))
    ]
    for copy in raw_copies:
        copy.start()

    barrier = pltpu.get_barrier_semaphore()

    def greet(axis, peer):
        pl.semaphore_signal(barrier, inc=1, device_id={axis: peer}, device_id_type=MESH)

    each(n_fs - 1, lambda i: greet("fs", fs_at(i + 1)))
    each(n_grp - 1, lambda i: greet("grp", grp_at(i + 1)))
    each(n_x - 1, lambda i: greet("tp", chip_at(i + 1) * 2 + core))
    greet("tp", partner)

    def ints(shape, axis):
        return lax.broadcasted_iota(jnp.int32, shape, axis)

    def route(ids, axis):
        shape = (experts, tok_rows) if axis == 0 else (tok_rows, experts)
        named = [(ints(shape, axis) == i).astype(F32) for i in ids]
        square = (tok_rows, tok_rows)
        earlier = (ints(square, axis) < ints(square, 1 - axis)).astype(F32).astype(BF16)
        both = (named[0] + named[1]).astype(BF16)
        pair = (both, earlier) if axis == 0 else (earlier, both)
        before = jnp.dot(*pair, preferred_element_type=F32)
        picks, kept = [], []
        for i, name in zip(ids, named):
            rank = jnp.sum(before * name, axis=axis, keepdims=True)
            kept.append(rank < capacity)
            slot = i * padded + rank.astype(jnp.int32)
            picks.append(jnp.where(rank < capacity, slot, -1))
        return picks, kept

    row_picks, _ = route([id_rows[0:1, :], id_rows[1:2, :]], 0)

    def fill(k):
        e = fs_at(k)
        slot = ints((padded, tok_rows), 0) + e * padded
        named = (slot == row_picks[0]) | (slot == row_picks[1])
        place = jnp.where(named, 1.0, 0.0).astype(BF16)
        out_ref[e] = jnp.dot(place, tokens[...], preferred_element_type=F32).astype(BF16)

    each(n_fs - 1, lambda i: fill(i + 1))
    pl.semaphore_wait(barrier, n_fs - 1 + n_grp - 1 + n_x - 1 + 1)

    weights = (
        (cast.at[0], gate_out), (cast.at[1], up_out), (cast.at[2], down_out)
    )

    def slot_copy(k, source):
        return rcopy(out_ref.at[fs_at(k)], piece.at[t, source], slot_s.at[k],
                     slot_r.at[n_fs - k], "fs", fs_at(k))

    def slot_arrival(k):
        return rcopy(out_ref.at[f], piece.at[t, fs_at(k)], slot_s.at[k], slot_r.at[k], "fs", fs_at(k))

    each(n_fs - 1, lambda i: slot_copy(outward(i), f).start())
    fill(0)
    own_slots = pltpu.make_async_copy(out_ref.at[f], piece.at[t, f], local_sem.at[3])
    own_slots.start()

    def w_rows(source, part):
        return pl.ds(source * block + part * share, share)

    def wz_copy(m, k):
        w_in, w_out = weights[m]
        return rcopy(w_in.at[fs_at(k), pl.ds(g * share, share)], w_out.at[w_rows(f, g)],
                     wz_s.at[m, k], wz_r.at[m, n_fs - k], "fs", fs_at(k))

    def wz_arrival(m, k):
        w_in, w_out = weights[m]
        return rcopy(w_in.at[fs_at(k), pl.ds(g * share, share)], w_out.at[w_rows(fs_at(k), g)],
                     wz_s.at[m, k], wz_r.at[m, k], "fs", fs_at(k))

    def wy_copy(m, k, j):
        w_out = weights[m][1]
        rows = w_rows(fs_at(k), g)
        return rcopy(w_out.at[rows], w_out.at[rows], wy_s.at[m, k, j],
                     wy_r.at[m, k, n_grp - j], "grp", grp_at(j))

    def wy_arrival(m, k, j):
        w_out = weights[m][1]
        rows = w_rows(fs_at(k), grp_at(j))
        return rcopy(w_out.at[rows], w_out.at[rows], wy_s.at[m, k, j],
                     wy_r.at[m, k, j], "grp", grp_at(j))

    own_weights = []
    for m in range(3):
        w_in, w_out = weights[m]
        raw_copies[m].wait()

        def round_block(e):
            if m < 2:
                cast[m, e] = (gain[...] * raw[m, e]).astype(BF16)
            else:
                cast[m, e] = raw[m, e].astype(BF16)

        each(n_fs, round_block)
        copy = pltpu.make_async_copy(w_in.at[f], w_out.at[pl.ds(f * block, block)], local_sem.at[m])
        copy.start()
        own_weights.append(copy)

    for m in range(3):
        each(n_fs - 1, lambda i: wz_copy(m, outward(i)).start())

    def forward(m, k):
        wz_arrival(m, k).wait_recv()
        for j in range(1, n_grp):
            wy_copy(m, k, j).start()

    def gx_copy(k, j):
        src = piece.at[t, fs_at(k)]
        return rcopy(src, src, gx_s.at[k, j], gx_r.at[k, n_x - j], "tp", chip_at(j) * 2 + core)

    def gx_arrival(k, j):
        src = piece.at[chip_at(j) * 2 + core, fs_at(k)]
        return rcopy(src, src, gx_s.at[k, j], gx_r.at[k, j], "tp", chip_at(j) * 2 + core)

    def gd_copy(k):
        src = piece.at[t, fs_at(k)]
        return rcopy(src, src, gd_s.at[k], gd_r.at[k], "tp", partner)

    def gd_arrival(k):
        src = piece.at[partner, fs_at(k)]
        return rcopy(src, src, gd_s.at[k], gd_r.at[k], "tp", partner)

    def gf_copy(k, j):
        src = piece.at[chip_at(j) * 2 + core, fs_at(k)]
        return rcopy(src, src, gf_s.at[k, j], gf_r.at[k, j], "tp", partner)

    def gf_arrival(k, j):
        src = piece.at[chip_at(j) * 2 + 1 - core, fs_at(k)]
        return rcopy(src, src, gf_s.at[k, j], gf_r.at[k, j], "tp", partner)

    def spread(k):
        for j in range(1, n_x):
            gx_copy(k, j).start()
        gd_copy(k).start()

    own_slots.wait()
    spread(0)

    id_cols = jnp.transpose(id_rows[...])
    ids = [id_cols[:, k : k + 1] for k in range(2)]
    picks, kept = route(ids, 1)
    group_exp = jnp.exp(jnp.transpose(group_logits[...]))
    group_count = group_exp.shape[1]
    low = ints(group_exp.shape, 1) * (experts // group_count)
    member = (ids[0] >= low) & (ids[0] < low + experts // group_count)
    chosen = jnp.sum(jnp.where(member, group_exp, 0.0), axis=1, keepdims=True)
    chosen = chosen / jnp.sum(group_exp, axis=1, keepdims=True)
    pair_exp = jnp.exp(jnp.transpose(pair_logits[...]))
    pair_weight = pair_exp / jnp.sum(pair_exp, axis=1, keepdims=True) * chosen
    mix_weights = [
        jnp.where(kept[k], pair_weight[:, k : k + 1], 0.0) for k in range(2)
    ]

    def blend(k):
        e = fs_at(k)
        slot = ints((tok_rows, padded), 1) + e * padded
        named = (slot == picks[0]) | (slot == picks[1])
        place = jnp.where(named, 1.0, 0.0).astype(BF16)
        weight = jnp.where(ids[0] == e, mix_weights[0], 0.0)
        weight = weight + jnp.where(ids[1] == e, mix_weights[1], 0.0)
        return jnp.dot(place, ret[e], preferred_element_type=F32) * weight

    def spread_arrived(i):
        slot_arrival(nearest(i)).wait_recv()
        spread(nearest(i))

    each(n_fs - 1, spread_arrived)

    def hand_over(k):
        for j in range(1, n_x):
            gx_arrival(k, j).wait_recv()
            gf_copy(k, j).start()

    hand_over(0)

    each(n_fs - 1, lambda i: hand_over(nearest(i)))

    for m in range(3):
        each(n_fs - 1, lambda i: forward(m, nearest(i)))

    def all_in(m):
        own_weights[m].wait()
        for j in range(1, n_grp):
            each(n_fs - 1, lambda i: wy_arrival(m, i + 1, j).wait_recv())

    all_in(0)
    all_in(1)

    def make_hidden(k):
        source = fs_at(k)
        gd_arrival(k).wait_recv()
        for j in range(1, n_x):
            gf_arrival(k, j).wait_recv()
        gate = up = None
        for p in range(n_tp):
            rows = piece[p, source]
            cols = pl.ds(p * width, width)
            gate_part = jnp.dot(rows, gate_out[cols, :], preferred_element_type=F32)
            up_part = jnp.dot(rows, up_out[cols, :], preferred_element_type=F32)
            gate = gate_part if gate is None else gate + gate_part
            up = up_part if up is None else up + up_part
        hidden[k] = (gate / (1.0 + jnp.exp(-gate)) * up).astype(BF16)

    each(n_fs, lambda i: make_hidden(i))
    all_in(2)

    def term(k, j, to_core):
        column = (chip_at(j) * 2 + to_core) * width
        rows = down_out[pl.ds(pl.multiple_of(column, width), width), :]
        return lax.dot_general(hidden[k], rows, (((1,), (1,)), ((), ())), preferred_element_type=F32)

    def pr_copy(k):
        return rcopy(pair_send.at[k], pair_recv.at[k], pr_s.at[k], pr_r.at[k], "tp", partner)

    def stage_pair(k):
        for j in range(n_x):
            pair_send[k, j] = term(k, j, 1 - core).astype(BF16)
        pr_copy(k).start()
        for j in range(n_x):
            own[k, j] = term(k, j, core)

    def xx_copy(k, j):
        return rcopy(x_send.at[k, j], x_recv.at[k, n_x - j], xx_s.at[k, j], xx_r.at[k, n_x - j],
                     "tp", chip_at(j) * 2 + core)

    def xx_arrival(k, j):
        return rcopy(x_send.at[k, j], x_recv.at[k, j], xx_s.at[k, j], xx_r.at[k, j],
                     "tp", chip_at(j) * 2 + core)

    def stage_chip(k):
        pr_copy(k).wait_recv()
        for j in range(1, n_x):
            x_send[k, j] = (own[k, j] + pair_recv[k, j].astype(F32)).astype(BF16)
            xx_copy(k, j).start()
        own[k, 0] = own[k, 0] + pair_recv[k, 0].astype(F32)

    def rt_copy(k):
        return rcopy(result.at[k], ret.at[f], rt_s.at[k], rt_r.at[n_fs - k], "fs", fs_at(k))

    def rt_arrival(k):
        return rcopy(result.at[k], ret.at[fs_at(k)], rt_s.at[k], rt_r.at[k], "fs", fs_at(k))

    def total(k):
        acc = own[k, 0]
        for j in range(1, n_x):
            xx_arrival(k, j).wait_recv()
            acc = acc + x_recv[k, j].astype(F32)
        return acc.astype(BF16)

    def stage_home(k):
        result[k] = total(k)
        rt_copy(k).start()

    def order(i):
        return lax.rem(outward(i) + n_fs, n_fs)

    stage_pair(order(0))

    def pair_and_chip(i):
        stage_pair(order(i + 1))
        stage_chip(order(i))

    each(n_fs - 1, pair_and_chip)
    stage_chip(order(n_fs - 1))
    each(n_fs - 1, lambda i: stage_home(order(i)))
    ret[f] = total(0)
    mix[...] = blend(0)

    def collect(i):
        k = nearest(i)
        rt_arrival(k).wait_recv()
        mix[...] += blend(k)

    each(n_fs - 1, collect)
    mixed[...] = mix[...].astype(BF16)

    def drain_peer(i):
        k = i + 1
        slot_copy(k, f).wait_send()
        rt_copy(k).wait_send()
        for m in range(3):
            wz_copy(m, k).wait_send()
            for j in range(1, n_grp):
                wy_copy(m, k, j).wait_send()

    def drain_chunk(k):
        gd_copy(k).wait_send()
        pr_copy(k).wait_send()
        for j in range(1, n_x):
            gx_copy(k, j).wait_send()
            gf_copy(k, j).wait_send()
            xx_copy(k, j).wait_send()

    each(n_fs - 1, drain_peer)
    each(n_fs, drain_chunk)


def body(
    tokens, norm_gain, gate_weight, up_weight, down_weight, expert_ids, group_logits, pair_logits
):
    n_grp, n_fs, n_tp = (lax.axis_size(a) for a in ("grp", "fs", "tp"))
    n_x = n_tp // 2
    experts, block, hid = gate_weight.shape
    tok_rows, width = tokens.shape
    capacity = 5 * tok_rows * 2 // (4 * experts)
    cap = -(-capacity // 16) * 16
    vmem = pl.BlockSpec(memory_space=pltpu.VMEM)
    hbm = pl.BlockSpec(memory_space=pl.ANY)
    dma = pltpu.SemaphoreType.DMA
    matrix = jax.ShapeDtypeStruct((n_fs * block, hid), BF16)
    chunk = (n_fs, n_x, cap, width)
    sem_shapes = [
        (4,), (3,), (n_fs,), (n_fs,), (3, n_fs), (3, n_fs), (3, n_fs, n_grp), (3, n_fs, n_grp),
        (n_fs, n_x), (n_fs, n_x), (n_fs,), (n_fs,), (n_fs, n_x), (n_fs, n_x),
        (n_fs,), (n_fs,), (n_fs, n_x), (n_fs, n_x), (n_fs,), (n_fs,),
    ]
    mixed, *matrices = pl.pallas_call(
        functools.partial(exchange_kernel, n_grp, n_fs, n_tp, capacity),
        out_shape=(jax.ShapeDtypeStruct((tok_rows, width), BF16), matrix, matrix, matrix),
        in_specs=[vmem] * 5 + [hbm] * 3,
        out_specs=(vmem,) * 4,
        scratch_shapes=[
            pltpu.VMEM((n_fs, cap, width), BF16),
            pltpu.VMEM((3, n_fs, block, hid), F32),
            pltpu.VMEM((3, n_fs, block, hid), BF16),
            pltpu.VMEM((n_fs, cap, width), BF16),
            pltpu.VMEM((tok_rows, width), F32),
            pltpu.VMEM((n_tp, n_fs, cap, width), BF16),
            pltpu.VMEM((n_fs, cap, hid), BF16),
            pltpu.VMEM(chunk, F32),
            pltpu.VMEM(chunk, BF16),
            pltpu.VMEM(chunk, BF16),
            pltpu.VMEM(chunk, BF16),
            pltpu.VMEM(chunk, BF16),
            pltpu.VMEM((n_fs, cap, width), BF16),
        ] + [dma(s) for s in sem_shapes],
        compiler_params=pltpu.CompilerParams(
            collective_id=0, has_side_effects=True, vmem_limit_bytes=48 * 1024 * 1024
        ),
    )(
        tokens, norm_gain[:, None], expert_ids.T, group_logits.T, pair_logits.T,
        gate_weight, up_weight, down_weight,
    )
    return (mixed, *(m[None] for m in matrices))


def pair_kernel(
    n_grp, n_fs, n_tp, capacity, chunk,
    tokens_in, gain_in, ids_in, group_in, pair_in, gate_in, up_in, down_in,
    mixed, gate_out, up_out, down_out,
    tokens, gain, id_rows, group_logits, pair_logits, gain_col,
    raw_own, raw_far, cast, slots, place, back_place, wsend, wrecv, wcol,
    piece, acc, hid, dwn, part_send, part_recv, keep, home_send, back, mix,
    in_sem, raw_sem, send, sl_r, wm_r, wd_r, wz_r, wy_r, tx_r, td_r, tf_r,
    dw_r, hx_r, hd_r, hf_r, pt_r, hm_r,
):
    g, f, t = lax.axis_index("grp"), lax.axis_index("fs"), lax.axis_index("tp")
    cap, width = piece.shape[2], piece.shape[3]
    block, hidden_units = raw_own.shape[1], raw_own.shape[2]
    share = raw_far.shape[2]
    tok_rows = tokens.shape[0]
    lanes = place.shape[1]
    pair = n_fs // 2

    inner = (f == 1) | (f == 2)

    def flip(i, k):
        return (i, i + 1 - 2 * lax.rem(i, 2), lax.rem(i + 2, 4), 3 - i)[k]

    def fs_at(k):
        if isinstance(k, int):
            return flip(f, k)
        return jnp.where(k == 1, flip(f, 1), jnp.where(k == 2, flip(f, 2), flip(f, 3)))

    def by_role(at_inner, at_outer):
        return jnp.where(inner, at_inner, at_outer)

    def tp_at(j):
        return flip(t, j)

    other_grp = 1 - g

    def rcopy(src, dst, ssem, rsem, axis, peer):
        return pltpu.make_async_remote_copy(
            src_ref=src, dst_ref=dst, send_sem=ssem, recv_sem=rsem,
            device_id={axis: peer}, device_id_type=MESH,
        )

    def all_sent(index, ref):
        rcopy(ref, ref, send.at[index], send.at[index], "fs", fs_at(1)).wait_send()

    def all_here(sem, ref):
        rcopy(ref, ref, sem, sem, "fs", fs_at(1)).wait_recv()

    small = [
        pltpu.make_async_copy(src, dst, in_sem.at[i])
        for i, (src, dst) in enumerate((
            (ids_in, id_rows), (tokens_in, tokens), (gain_in, gain),
            (group_in, group_logits), (pair_in, pair_logits),
        ))
    ]
    w_in = (gate_in, up_in, down_in)
    w_out = (gate_out, up_out, down_out)

    def far_load(m, k):
        return pltpu.make_async_copy(
            w_in[m].at[fs_at(k), pl.ds(g * share, share)], raw_far.at[m, k - 1], raw_sem.at[m, 1]
        )

    def far_loaded(m):
        whole = w_in[m].at[pl.ds(0, 3), pl.ds(0, share)]
        pltpu.make_async_copy(whole, raw_far.at[m], raw_sem.at[m, 1]).wait()

    def own_load(m):
        return pltpu.make_async_copy(w_in[m].at[f], raw_own.at[m], raw_sem.at[m, 0])

    for copy in small:
        copy.start()
    for m in (2, 0, 1):
        for k in (1, 2, 3):
            far_load(m, k).start()
    for m in (2, 0, 1):
        own_load(m).start()

    barrier = pltpu.get_barrier_semaphore()

    def greet(axis, peer):
        pl.semaphore_signal(barrier, inc=1, device_id={axis: peer}, device_id_type=MESH)

    for k in (1, 2, 3):
        greet("fs", fs_at(k))
        greet("tp", tp_at(k))
    greet("grp", other_grp)

    cuts = wz_r.shape[2]

    def cuts_of(m):
        return range(1 if m == 2 else cuts)

    def piece_rows(m):
        return share if m == 2 else share // cuts

    def w_rows(source, part, m, h):
        return pl.ds(source * block + part * share + h * piece_rows(m), piece_rows(m))

    def far_rows(m, k, h):
        return cast.at[m, k - 1, pl.ds(h * piece_rows(m), piece_rows(m))]

    def wz_sem(m, k, h):
        return wd_r.at[k - 1] if m == 2 else wz_r.at[m, k - 1, h]

    def wz_copy(m, k, h):
        return rcopy(far_rows(m, k, h), w_out[m].at[w_rows(f, g, m, h)],
                     send.at[2], wz_sem(m, k, h), "fs", fs_at(k))

    def wz_arrival(m, k, h):
        return rcopy(far_rows(m, k, h), w_out[m].at[w_rows(fs_at(k), g, m, h)],
                     send.at[2], wz_sem(m, k, h), "fs", fs_at(k))

    def wy_sem(m, k):
        return wy_r.at[0] if m == 2 else wy_r.at[k]

    def wy_copy(m, k, h):
        rows = w_out[m].at[w_rows(fs_at(k), g, m, h)]
        return rcopy(rows, rows, send.at[2], wy_sem(m, k), "grp", other_grp)

    def wy_arrival(m, k, h):
        rows = w_out[m].at[w_rows(fs_at(k), other_grp, m, h)]
        return rcopy(rows, rows, send.at[2], wy_sem(m, k), "grp", other_grp)

    def ints(shape, axis):
        return lax.broadcasted_iota(jnp.int32, shape, axis)

    own_base = (f - lax.rem(f, 2))
    far_base = lax.rem(own_base + 2, 4)
    bases = (own_base, far_base)

    with scope("small_0_wait"):
        small[0].wait()
    first, second = id_rows[0:1, :], id_rows[1:2, :]
    members = [(first >= b) & (first < b + 2) for b in bases]
    square = (tok_rows, tok_rows)
    earlier = (ints(square, 0) < ints(square, 1)).astype(F32).astype(BF16)
    named = jnp.where(ints((8, tok_rows), 0) < 4, members[0].astype(F32), members[1].astype(F32))
    before = jnp.dot(named.astype(BF16), earlier, preferred_element_type=F32)
    ranks = [before[0:1, :], before[4:5, :]]
    kept = [m & (r < capacity) for m, r in zip(members, ranks)]
    seat = [jnp.where(k, r.astype(jnp.int32), -1) for k, r in zip(kept, ranks)]

    with scope("small_1_wait"):
        small[1].wait()

    def fill(i):
        one_hot = jnp.where(ints((lanes, tok_rows), 0) == seat[i], 1.0, 0.0)
        place[i] = one_hot.astype(BF16)
        rows = jnp.dot(place[i, 0:cap, :], tokens[...], preferred_element_type=F32).astype(BF16)
        slots[i] = rows
        return rows

    def slot_copy(k):
        src = slots.at[0] if k == 1 else slots.at[1]
        return rcopy(src, piece.at[t, k], send.at[0], sl_r.at[k], "fs", fs_at(k))

    def relay_copy():
        return rcopy(piece.at[t, 2], piece.at[t, 3], send.at[0], sl_r.at[3], "fs", fs_at(1))

    fill(1)
    with scope("barrier"):
        pl.semaphore_wait(barrier, 3 + 3 + 1)
    slot_copy(2).start()
    piece[t, 0] = fill(0)
    slot_copy(1).start()

    def tx_copy(k):
        src = piece.at[t, k]
        return rcopy(src, src, send.at[1], tx_r.at[k], "tp", tp_at(2))

    def td_copy(k):
        src = piece.at[t, k]
        return rcopy(src, src, send.at[1], td_r.at[k // 3], "tp", tp_at(1))

    def tf_copy(k):
        src = piece.at[tp_at(2), k]
        return rcopy(src, src, send.at[1], tf_r.at[k // 3], "tp", tp_at(1))

    def tx_arrival(k):
        src = piece.at[tp_at(2), k]
        return rcopy(src, src, send.at[1], tx_r.at[k], "tp", tp_at(2))

    def td_arrival(k):
        src = piece.at[tp_at(1), k]
        return rcopy(src, src, send.at[1], td_r.at[k // 3], "tp", tp_at(1))

    def tf_arrival(k):
        src = piece.at[tp_at(3), k]
        return rcopy(src, src, send.at[1], tf_r.at[k // 3], "tp", tp_at(1))

    def spread(k):
        tx_copy(k).start()
        td_copy(k).start()

    spread(0)

    small[2].wait()
    gain_col[...] = jnp.transpose(jnp.broadcast_to(gain[...], (8, block)))[:, 0:1]
    far_gain = gain_col[pl.ds(g * share, share), :]

    def send_far(m, k):
        with scope("far_load_m_k_wait"):
            cast[m, k - 1] = (far_gain * raw_far[m, k - 1]).astype(BF16)
        for h in cuts_of(m):
            wz_copy(m, k, h).start()

    def round_own(m):
        with scope("own_load_m_wait"):
            own_load(m).wait()
        values = raw_own[m]
        if m < 2:
            values = gain_col[...] * values
        w_out[m][pl.ds(f * block, block), :] = values.astype(BF16)

    far_loaded(2)
    for k in (1, 2, 3):
        cast[2, k - 1] = raw_far[2, k - 1].astype(BF16)
        wz_copy(2, k, 0).start()
    far_loaded(0)
    far_loaded(1)

    with scope("small_3_wait"):
        small[3].wait()
    with scope("small_4_wait"):
        small[4].wait()
    group_exp = jnp.exp(group_logits[...])
    group_sum = jnp.sum(group_exp, axis=0, keepdims=True)
    pair_exp = jnp.exp(pair_logits[...])
    pair_weight = pair_exp / jnp.sum(pair_exp, axis=0, keepdims=True)
    group_count = group_exp.shape[0]

    def wm_copy(k):
        return rcopy(wsend.at[k // 2], wrecv.at[k], send.at[3], wm_r.at[0], "fs", fs_at(k))

    chosen = jnp.zeros_like(group_sum)
    for i in range(group_count):
        chosen = chosen + jnp.where((first >= 2 * i) & (first < 2 * i + 2), group_exp[i : i + 1, :], 0.0)
    mix_weight = pair_weight * (chosen / group_sum)
    for i in range(2):
        expert = bases[i] + ints((8, tok_rows), 0)
        rest = jnp.where(first == expert, mix_weight[0:1, :], 0.0)
        rest = rest + jnp.where(second == expert, mix_weight[1:2, :], 0.0)
        total = None
        for _ in range(3):
            head = rest.astype(BF16)
            rest = rest - head.astype(F32)
            term = lax.dot_general(head, place[i], (((1,), (1,)), ((), ())), preferred_element_type=F32)
            total = term if total is None else total + term
        wsend[i] = total
    for k in (1, 2, 3):
        wm_copy(k).start()

    def slot_arrival(k):
        return rcopy(slots.at[0], piece.at[t, k], send.at[0], sl_r.at[k], "fs", fs_at(k))

    with scope("cross"):
        slot_arrival(2).wait_recv()
    relay_copy().start()
    spread(2)
    for k in (1, 2, 3):
        for m in (0, 1):
            send_far(m, k)

    def hand_over(k):
        with scope("hand%d" % k):
            tx_arrival(k).wait_recv()
        tf_copy(k).start()

    def forward(m, k, h):
        with scope("forward%d%d%d" % (m, k, h)):
            wz_arrival(m, k, h).wait_recv()
        wy_copy(m, k, h).start()

    def forward_all(steps, more):
        @pl.when(inner)
        def _():
            for step in steps:
                forward(*step)

        @pl.when(jnp.logical_not(inner))
        def _():
            for step in more:
                forward(*step)

    def arrived(k):
        with scope("arrived"):
            all_here(wy_r.at[k], gate_out.at[pl.ds(0, 2 * share)])

    def land(k):
        with scope("land%d" % k):
            slot_arrival(k).wait_recv()
        spread(k)

    def seat_weights(k, rows):
        cols = jnp.transpose(rows)
        wcol[k] = jnp.where(lax.rem(f, 2) == 0, cols[0:cap, 0:1], cols[0:cap, 1:2])

    hand_over(0)
    round_own(2)
    for i in range(2):
        back_place[i] = jnp.transpose(place[i].astype(F32))[:, 0:cap].astype(BF16)
    seat_weights(0, wsend[0])
    land(1)
    for k in (2, 1, 3):
        forward(2, k, 0)
    hand_over(2)
    hand_over(1)
    for m in (0, 1):
        round_own(m)

    def dw_copy(j):
        src = down_out.at[pl.ds(tp_at(j) * block, block)]
        return rcopy(src, dwn.at[j], send.at[4], dw_r.at[0], "tp", tp_at(j))

    with scope("down_in"):
        all_here(wy_r.at[0], down_out.at[pl.ds(0, 3 * share)])
    for j in (3, 2, 1):
        dw_copy(j).start()
    def steps(*turns):
        return [(m, k, h) for k in turns for m in (0, 1) for h in cuts_of(m)]

    turns = (by_role(1, 2), by_role(2, 1), 3)
    forward_all(steps(1), steps(2))
    land(3)
    forward_all(steps(2), steps(1))
    with scope("weights_in"):
        all_here(wm_r.at[0], wrecv.at[pl.ds(1, 3)])
        for k in (1, 2, 3):
            seat_weights(k, wrecv[k])
    with scope("rows_in"):
        all_here(td_r.at[0], piece.at[t, pl.ds(0, 3)])
        all_here(tf_r.at[0], piece.at[t, pl.ds(0, 3)])

    def products(k, source):
        rows = piece[source, k]
        cols = pl.ds(source * block, block)
        gate = jnp.dot(rows, gate_out[cols, :], preferred_element_type=F32)
        up = jnp.dot(rows, up_out[cols, :], preferred_element_type=F32)
        return gate, up

    def first_products(k, c):
        gate, up = products(k, f)
        acc[0, k], acc[1, k] = gate, up
        return c

    def more_products(kk):
        def step(k, c):
            gate, up = products(k, fs_at(kk))
            acc[0, k] += gate
            acc[1, k] += up
            return c
        return step

    def multiply(step, blocks):
        with scope("products"):
            lax.fori_loop(*blocks, step, 0)

    first = (0, n_fs - 1)
    multiply(first_products, first)
    arrived(turns[0])
    multiply(more_products(turns[0]), first)
    forward_all(steps(3), steps(3))
    hand_over(3)
    arrived(turns[1])
    multiply(more_products(turns[1]), first)
    with scope("rows_in"):
        all_here(td_r.at[1], piece.at[t, 3])
        all_here(tf_r.at[1], piece.at[t, 3])
    first_products(3, 0)
    more_products(turns[0])(3, 0)
    more_products(turns[1])(3, 0)
    arrived(turns[2])

    edges = (0, *chunk, cap)
    spans = [pl.ds(a, b - a) for a, b in zip(edges, edges[1:])]
    parts = range(len(spans))

    def h_copy(j, k, c, ssem, rsem, source):
        src, dst = hid.at[source, k, spans[c]], hid.at[source ^ j, k, spans[c]]
        return rcopy(src, dst, ssem, rsem, "tp", tp_at(j))

    def hx_copy(k, c):
        return h_copy(2, k, c, send.at[5], hx_r.at[k, c], 0)

    def hd_copy(k, c):
        return h_copy(1, k, c, send.at[5], hd_r.at[k], 0)

    def hf_copy(k, c):
        return h_copy(1, k, c, send.at[5], hf_r.at[k, c], 2)

    last = fs_at(turns[2])
    blocks = (by_role(1, 3), 2, by_role(3, 1), 0)
    def diagonal_copy(k, c):
        src, dst = hid.at[0, k, spans[c]], hid.at[3, k, spans[c]]
        return rcopy(src, dst, send.at[5], hf_r.at[k, c], "tp", tp_at(3))

    direct = 1

    def launch(i):
        for c in parts:
            if i == 0 and c < direct:
                diagonal_copy(blocks[i], c).start()
            hx_copy(blocks[i], c).start()

    for k in blocks:
        with scope("hidden"):
            gate, up = products(k, last)
            gate = acc[0, k] + gate
            up = acc[1, k] + up
            hid[0, k] = (gate / (1.0 + jnp.exp(-gate)) * up * wcol[k]).astype(BF16)
            if k is blocks[0]:
                launch(0)
            for c in parts:
                hd_copy(k, c).start()

    with scope("drain"):
        all_here(dw_r.at[0], dwn.at[pl.ds(1, 3)])
        all_sent(0, piece.at[t, pl.ds(0, 3)])
        all_sent(1, piece.at[pl.ds(0, 3)])
        all_sent(2, raw_far)
        all_sent(3, wrecv.at[pl.ds(1, 3)])
        all_sent(4, dwn.at[pl.ds(1, 3)])

    queue = [(k, c) for k in blocks for c in parts]

    def pass_on(n):
        if n < len(queue):
            with scope("hx"):
                hx_copy(*queue[n]).wait_recv()
            if n >= direct:
                hf_copy(*queue[n]).start()

    def result(n):
        k, c = queue[n]

        def term(j):
            rows = down_out[pl.ds(t * block, block), :] if j == 0 else dwn[j]
            return lax.dot_general(
                hid[j, k, spans[c], :], rows, (((1,), (1,)), ((), ())), preferred_element_type=F32)

        if c == 0:
            with scope("hd"):
                all_here(hd_r.at[k], hid.at[1, k])
        total = term(0) + term(1)
        if n == 0:
            pass_on(0)
            launch(1)
        total = total + term(2)
        if n > 0:
            pass_on(n + 1)
        with scope("hf"):
            hf_copy(k, c).wait_recv()
        total = total + term(3)
        if n == 0:
            pass_on(1)
        return total

    def part_copy(i, c):
        return rcopy(part_send.at[i, spans[c]], part_recv.at[i, spans[c]],
                     send.at[6 + i // 2], pt_r.at[i, c], "fs", fs_at(1))

    def home_copy(i, c):
        return rcopy(home_send.at[i, spans[c]], back.at[1, spans[c]],
                     send.at[8], hm_r.at[0], "fs", fs_at(2 + i))

    def home_step(n):
        if n < 0 or n >= 2 * len(parts):
            return
        i, c = divmod(n, len(parts))

        @pl.when(inner)
        def _():
            with scope("part%d" % i):
                part_copy(i, c).wait_recv()
            both = keep[i + 1, spans[c], :] + part_recv[i, spans[c], :].astype(F32)
            home_send[i, spans[c], :] = both.astype(BF16)
            home_copy(i, c).start()

    for n in range(len(queue)):
        i, c = divmod(n, len(parts))
        if c == 0 and i in (1, 2):
            launch(i + 1)
        keep[i, spans[c], :] = result(n)

        def send_part(to):
            part_send[to, spans[c], :] = keep[i, spans[c], :].astype(BF16)
            part_copy(to, c).start()

        if i < 3:
            pl.when(jnp.logical_not(inner))(functools.partial(send_part, i))
        if i == 0:
            pl.when(inner)(functools.partial(send_part, 2))
        home_step(n - len(parts) - 1)

    def finish_own():
        for c in parts:
            with scope("part2"):
                part_copy(2, c).wait_recv()
            both = keep[3, spans[c], :] + part_recv[2, spans[c], :].astype(F32)
            back[0, spans[c], :] = both.astype(BF16)

    def finish_far():
        with scope("home"):
            all_here(hm_r.at[0], back.at[1])

    pl.when(inner)(finish_own)
    pl.when(jnp.logical_not(inner))(finish_far)
    sooner, later = by_role(0, 1), by_role(1, 0)
    mix[...] = jnp.dot(back_place[sooner], back[sooner], preferred_element_type=F32)
    pl.when(inner)(finish_far)
    pl.when(jnp.logical_not(inner))(finish_own)
    with scope("last_dot"):
        more = jnp.dot(back_place[later], back[later], preferred_element_type=F32)
        mixed[...] = (mix[...] + more).astype(BF16)

    all_sent(5, hid.at[pl.ds(0, 3)])
    all_sent(7, part_send.at[2])

    @pl.when(inner)
    def _():
        all_sent(8, home_send)

    @pl.when(jnp.logical_not(inner))
    def _():
        all_sent(6, part_send.at[pl.ds(0, 2)])


def pair_body(
    tokens, norm_gain, gate_weight, up_weight, down_weight, expert_ids, group_logits, pair_logits
):
    n_grp, n_fs, n_tp = (lax.axis_size(a) for a in ("grp", "fs", "tp"))
    experts, block, hid = gate_weight.shape
    tok_rows, width = tokens.shape
    share = block // n_grp
    capacity = 5 * tok_rows * 2 // (4 * experts)
    cap = -(-capacity // 16) * 16
    lanes = -(-cap // 128) * 128
    vmem = pl.BlockSpec(memory_space=pltpu.VMEM)
    hbm = pl.BlockSpec(memory_space=pltpu.HBM)
    dma = pltpu.SemaphoreType.DMA
    matrix = jax.ShapeDtypeStruct((n_fs * block, hid), BF16)
    rows = (cap, width)
    chunk = (cap // 80 * 16, cap // 80 * 16 * 2, cap // 80 * 16 * 3)
    spans = len(chunk) + 1
    sem_shapes = [
        (5,), (3, 2), (9,), (n_fs,), (1,), (n_fs - 1,), (2, n_fs - 1, 4), (n_fs,), (n_fs,), (2,), (2,),
        (1,), (n_fs, spans), (n_fs,), (n_fs, spans), (3, spans), (1,),
    ]
    mixed, *matrices = pl.pallas_call(
        functools.partial(pair_kernel, n_grp, n_fs, n_tp, capacity, chunk),
        out_shape=(jax.ShapeDtypeStruct((tok_rows, width), BF16), matrix, matrix, matrix),
        in_specs=[hbm] * 8,
        out_specs=(vmem,) * 4,
        scratch_shapes=[
            pltpu.VMEM((tok_rows, width), BF16),
            pltpu.VMEM((1, block), F32),
            pltpu.VMEM((2, tok_rows), jnp.int32),
            pltpu.VMEM((group_logits.shape[1], tok_rows), F32),
            pltpu.VMEM((2, tok_rows), F32),
            pltpu.VMEM((block, 1), F32),
            pltpu.VMEM((3, block, hid), F32),
            pltpu.VMEM((3, n_fs - 1, share, hid), F32),
            pltpu.VMEM((3, n_fs - 1, share, hid), BF16),
            pltpu.VMEM((2, *rows), BF16),
            pltpu.VMEM((2, lanes, tok_rows), BF16),
            pltpu.VMEM((2, tok_rows, cap), BF16),
            pltpu.VMEM((2, 8, lanes), F32),
            pltpu.VMEM((n_fs, 8, lanes), F32),
            pltpu.VMEM((n_fs, cap, 1), F32),
            pltpu.VMEM((n_tp, n_fs, *rows), BF16),
            pltpu.VMEM((2, n_fs, cap, hid), F32),
            pltpu.VMEM((n_tp, n_fs, cap, hid), BF16),
            pltpu.VMEM((n_tp, block, hid), BF16),
            pltpu.VMEM((3, *rows), BF16),
            pltpu.VMEM((3, *rows), BF16),
            pltpu.VMEM((n_fs, *rows), F32),
            pltpu.VMEM((2, *rows), BF16),
            pltpu.VMEM((2, *rows), BF16),
            pltpu.VMEM((tok_rows, width), F32),
        ] + [dma(s) for s in sem_shapes],
        compiler_params=pltpu.CompilerParams(
            collective_id=0, has_side_effects=True, vmem_limit_bytes=40 * 1024 * 1024
        ),
    )(*(pltpu.with_memory_space_constraint(x, pltpu.HBM) for x in (
        tokens, norm_gain[None, :], expert_ids.T, group_logits.T, pair_logits.T,
        gate_weight, up_weight, down_weight,
    )))
    return write_out(mixed, *matrices)


def write_kernel(mixed, gate, up, down, *rest):
    outs, sem = rest[:4], rest[4]
    pairs = (
        (gate, outs[1].at[0]), (up, outs[2].at[0]), (down, outs[3].at[0]), (mixed, outs[0])
    )
    for i, (src, dst) in enumerate(pairs):
        rows = src.shape[0] // 4
        for c in range(4):
            at = pl.ds(c * rows, rows)
            pltpu.make_async_copy(src.at[at], dst.at[at], sem.at[i]).start()
    for i, (src, dst) in enumerate(pairs):
        pltpu.make_async_copy(src, dst, sem.at[i]).wait()


def write_out(mixed, *matrices):
    return pl.pallas_call(
        write_kernel,
        out_shape=(
            jax.ShapeDtypeStruct(mixed.shape, BF16),
            *(jax.ShapeDtypeStruct((1, *m.shape), BF16) for m in matrices),
        ),
        in_specs=[pl.BlockSpec(memory_space=pltpu.VMEM)] * 4,
        out_specs=(pl.BlockSpec(memory_space=pltpu.HBM),) * 4,
        scratch_shapes=[pltpu.SemaphoreType.DMA((4,))],
        compiler_params=pltpu.CompilerParams(vmem_limit_bytes=1024 * 1024),
    )(mixed, *matrices)


def paired(mesh, tokens, gate_weight, expert_ids, group_logits):
    n_grp, n_fs, n_tp = (mesh.shape[a] for a in ("grp", "fs", "tp"))
    experts, features, _ = gate_weight.shape
    return (
        experts // group_logits.shape[1] == expert_ids.shape[1] == 2
        and n_fs == n_tp == experts == 4
        and n_grp == 2
    )


def solution(mesh):
    placed = (
        P(("grp", "fs"), "tp"),
        P("fs"),
        P(None, "fs", "tp"),
        P(None, "fs", "tp"),
        P(None, "fs", "tp"),
        P(("grp", "fs"), None),
        P(("grp", "fs"), None),
        P(("grp", "fs"), None),
    )

    def run(tokens, norm_gain, gate_weight, up_weight, down_weight, expert_ids, group_logits, pair_logits):
        args = (tokens, norm_gain, gate_weight, up_weight, down_weight, expert_ids, group_logits, pair_logits)
        special = paired(mesh, tokens, gate_weight, expert_ids, group_logits)
        return jax.shard_map(
            pair_body if special else body,
            mesh=mesh,
            in_specs=placed,
            out_specs=(
                P(("grp", "fs"), "tp"),
                P(("grp", "fs"), None, "tp"),
                P(("grp", "fs"), None, "tp"),
                P(("grp", "fs"), None, "tp"),
            ),
            check_vma=False,
        )(*args)

    return run
```

```python
import functools

import jax
import jax.numpy as jnp
from jax import lax
from jax.experimental import pallas as pl
from jax.experimental.pallas import tpu as pltpu
from jax.sharding import PartitionSpec as P

MESH = pl.DeviceIdType.MESH
BF16 = jnp.bfloat16
F32 = jnp.float32
scope = jax.named_scope


def each(count, step):
    if count <= 4:
        for i in range(count):
            step(i)
    else:
        lax.fori_loop(0, count, lambda i, c: (step(i), c)[1], 0)


def exchange_kernel(
    n_grp, n_fs, n_tp, capacity,
    tokens, gain, id_rows, group_logits, pair_logits, gate_in, up_in, down_in,
    mixed, gate_out, up_out, down_out,
    out_ref, raw, cast, ret, mix, piece, hidden, own, pair_send, pair_recv, x_send, x_recv, result,
    local_sem, raw_sem, slot_s, slot_r, wz_s, wz_r, wy_s, wy_r,
    gx_s, gx_r, gd_s, gd_r, gf_s, gf_r, pr_s, pr_r, xx_s, xx_r, rt_s, rt_r,
):
    g, f, t = lax.axis_index("grp"), lax.axis_index("fs"), lax.axis_index("tp")
    n_x = n_tp // 2
    chip, core = t // 2, lax.rem(t, 2)
    partner = chip * 2 + 1 - core
    width = piece.shape[3]
    block = cast.shape[2]
    tok_rows, padded = tokens.shape[0], out_ref.shape[1]
    experts = n_fs
    share = block // n_grp

    def fs_at(k):
        return lax.rem(f + k, n_fs)

    def outward(i):
        return jnp.where(f < n_fs // 2, i + 1, n_fs - 1 - i)

    def nearest(i):
        if n_fs != 4:
            return outward(i)
        first = jnp.where(f % 2 == 0, 1, 3)
        last = jnp.where(f == 0, 3, jnp.where(f == 3, 1, 2))
        return (first, 6 - first - last, last)[i]

    def grp_at(k):
        return lax.rem(g + k, n_grp)

    def chip_at(k):
        return lax.rem(chip + k, n_x)

    def rcopy(src, dst, ssem, rsem, axis, peer):
        return pltpu.make_async_remote_copy(
            src_ref=src, dst_ref=dst, send_sem=ssem, recv_sem=rsem,
            device_id={axis: peer}, device_id_type=MESH,
        )

    raw_copies = [
        pltpu.make_async_copy(w, raw.at[m], raw_sem.at[m])
        for m, w in enumerate((gate_in, up_in, down_in))
    ]
    for copy in raw_copies:
        copy.start()

    barrier = pltpu.get_barrier_semaphore()

    def greet(axis, peer):
        pl.semaphore_signal(barrier, inc=1, device_id={axis: peer}, device_id_type=MESH)

    each(n_fs - 1, lambda i: greet("fs", fs_at(i + 1)))
    each(n_grp - 1, lambda i: greet("grp", grp_at(i + 1)))
    each(n_x - 1, lambda i: greet("tp", chip_at(i + 1) * 2 + core))
    greet("tp", partner)

    def ints(shape, axis):
        return lax.broadcasted_iota(jnp.int32, shape, axis)

    def route(ids, axis):
        shape = (experts, tok_rows) if axis == 0 else (tok_rows, experts)
        named = [(ints(shape, axis) == i).astype(F32) for i in ids]
        square = (tok_rows, tok_rows)
        earlier = (ints(square, axis) < ints(square, 1 - axis)).astype(F32).astype(BF16)
        both = (named[0] + named[1]).astype(BF16)
        pair = (both, earlier) if axis == 0 else (earlier, both)
        before = jnp.dot(*pair, preferred_element_type=F32)
        picks, kept = [], []
        for i, name in zip(ids, named):
            rank = jnp.sum(before * name, axis=axis, keepdims=True)
            kept.append(rank < capacity)
            slot = i * padded + rank.astype(jnp.int32)
            picks.append(jnp.where(rank < capacity, slot, -1))
        return picks, kept

    row_picks, _ = route([id_rows[0:1, :], id_rows[1:2, :]], 0)

    def fill(k):
        e = fs_at(k)
        slot = ints((padded, tok_rows), 0) + e * padded
        named = (slot == row_picks[0]) | (slot == row_picks[1])
        place = jnp.where(named, 1.0, 0.0).astype(BF16)
        out_ref[e] = jnp.dot(place, tokens[...], preferred_element_type=F32).astype(BF16)

    each(n_fs - 1, lambda i: fill(i + 1))
    pl.semaphore_wait(barrier, n_fs - 1 + n_grp - 1 + n_x - 1 + 1)

    weights = (
        (cast.at[0], gate_out), (cast.at[1], up_out), (cast.at[2], down_out)
    )

    def slot_copy(k, source):
        return rcopy(out_ref.at[fs_at(k)], piece.at[t, source], slot_s.at[k],
                     slot_r.at[n_fs - k], "fs", fs_at(k))

    def slot_arrival(k):
        return rcopy(out_ref.at[f], piece.at[t, fs_at(k)], slot_s.at[k], slot_r.at[k], "fs", fs_at(k))

    each(n_fs - 1, lambda i: slot_copy(outward(i), f).start())
    fill(0)
    own_slots = pltpu.make_async_copy(out_ref.at[f], piece.at[t, f], local_sem.at[3])
    own_slots.start()

    def w_rows(source, part):
        return pl.ds(source * block + part * share, share)

    def wz_copy(m, k):
        w_in, w_out = weights[m]
        return rcopy(w_in.at[fs_at(k), pl.ds(g * share, share)], w_out.at[w_rows(f, g)],
                     wz_s.at[m, k], wz_r.at[m, n_fs - k], "fs", fs_at(k))

    def wz_arrival(m, k):
        w_in, w_out = weights[m]
        return rcopy(w_in.at[fs_at(k), pl.ds(g * share, share)], w_out.at[w_rows(fs_at(k), g)],
                     wz_s.at[m, k], wz_r.at[m, k], "fs", fs_at(k))

    def wy_copy(m, k, j):
        w_out = weights[m][1]
        rows = w_rows(fs_at(k), g)
        return rcopy(w_out.at[rows], w_out.at[rows], wy_s.at[m, k, j],
                     wy_r.at[m, k, n_grp - j], "grp", grp_at(j))

    def wy_arrival(m, k, j):
        w_out = weights[m][1]
        rows = w_rows(fs_at(k), grp_at(j))
        return rcopy(w_out.at[rows], w_out.at[rows], wy_s.at[m, k, j],
                     wy_r.at[m, k, j], "grp", grp_at(j))

    own_weights = []
    for m in range(3):
        w_in, w_out = weights[m]
        raw_copies[m].wait()

        def round_block(e):
            if m < 2:
                cast[m, e] = (gain[...] * raw[m, e]).astype(BF16)
            else:
                cast[m, e] = raw[m, e].astype(BF16)

        each(n_fs, round_block)
        copy = pltpu.make_async_copy(w_in.at[f], w_out.at[pl.ds(f * block, block)], local_sem.at[m])
        copy.start()
        own_weights.append(copy)

    for m in range(3):
        each(n_fs - 1, lambda i: wz_copy(m, outward(i)).start())

    def forward(m, k):
        wz_arrival(m, k).wait_recv()
        for j in range(1, n_grp):
            wy_copy(m, k, j).start()

    def gx_copy(k, j):
        src = piece.at[t, fs_at(k)]
        return rcopy(src, src, gx_s.at[k, j], gx_r.at[k, n_x - j], "tp", chip_at(j) * 2 + core)

    def gx_arrival(k, j):
        src = piece.at[chip_at(j) * 2 + core, fs_at(k)]
        return rcopy(src, src, gx_s.at[k, j], gx_r.at[k, j], "tp", chip_at(j) * 2 + core)

    def gd_copy(k):
        src = piece.at[t, fs_at(k)]
        return rcopy(src, src, gd_s.at[k], gd_r.at[k], "tp", partner)

    def gd_arrival(k):
        src = piece.at[partner, fs_at(k)]
        return rcopy(src, src, gd_s.at[k], gd_r.at[k], "tp", partner)

    def gf_copy(k, j):
        src = piece.at[chip_at(j) * 2 + core, fs_at(k)]
        return rcopy(src, src, gf_s.at[k, j], gf_r.at[k, j], "tp", partner)

    def gf_arrival(k, j):
        src = piece.at[chip_at(j) * 2 + 1 - core, fs_at(k)]
        return rcopy(src, src, gf_s.at[k, j], gf_r.at[k, j], "tp", partner)

    def spread(k):
        for j in range(1, n_x):
            gx_copy(k, j).start()
        gd_copy(k).start()

    own_slots.wait()
    spread(0)

    id_cols = jnp.transpose(id_rows[...])
    ids = [id_cols[:, k : k + 1] for k in range(2)]
    picks, kept = route(ids, 1)
    group_exp = jnp.exp(jnp.transpose(group_logits[...]))
    group_count = group_exp.shape[1]
    low = ints(group_exp.shape, 1) * (experts // group_count)
    member = (ids[0] >= low) & (ids[0] < low + experts // group_count)
    chosen = jnp.sum(jnp.where(member, group_exp, 0.0), axis=1, keepdims=True)
    chosen = chosen / jnp.sum(group_exp, axis=1, keepdims=True)
    pair_exp = jnp.exp(jnp.transpose(pair_logits[...]))
    pair_weight = pair_exp / jnp.sum(pair_exp, axis=1, keepdims=True) * chosen
    mix_weights = [
        jnp.where(kept[k], pair_weight[:, k : k + 1], 0.0) for k in range(2)
    ]

    def blend(k):
        e = fs_at(k)
        slot = ints((tok_rows, padded), 1) + e * padded
        named = (slot == picks[0]) | (slot == picks[1])
        place = jnp.where(named, 1.0, 0.0).astype(BF16)
        weight = jnp.where(ids[0] == e, mix_weights[0], 0.0)
        weight = weight + jnp.where(ids[1] == e, mix_weights[1], 0.0)
        return jnp.dot(place, ret[e], preferred_element_type=F32) * weight

    def spread_arrived(i):
        slot_arrival(nearest(i)).wait_recv()
        spread(nearest(i))

    each(n_fs - 1, spread_arrived)

    def hand_over(k):
        for j in range(1, n_x):
            gx_arrival(k, j).wait_recv()
            gf_copy(k, j).start()

    hand_over(0)

    each(n_fs - 1, lambda i: hand_over(nearest(i)))

    for m in range(3):
        each(n_fs - 1, lambda i: forward(m, nearest(i)))

    def all_in(m):
        own_weights[m].wait()
        for j in range(1, n_grp):
            each(n_fs - 1, lambda i: wy_arrival(m, i + 1, j).wait_recv())

    all_in(0)
    all_in(1)

    def make_hidden(k):
        source = fs_at(k)
        gd_arrival(k).wait_recv()
        for j in range(1, n_x):
            gf_arrival(k, j).wait_recv()
        gate = up = None
        for p in range(n_tp):
            rows = piece[p, source]
            cols = pl.ds(p * width, width)
            gate_part = jnp.dot(rows, gate_out[cols, :], preferred_element_type=F32)
            up_part = jnp.dot(rows, up_out[cols, :], preferred_element_type=F32)
            gate = gate_part if gate is None else gate + gate_part
            up = up_part if up is None else up + up_part
        hidden[k] = (gate / (1.0 + jnp.exp(-gate)) * up).astype(BF16)

    each(n_fs, lambda i: make_hidden(i))
    all_in(2)

    def term(k, j, to_core):
        column = (chip_at(j) * 2 + to_core) * width
        rows = down_out[pl.ds(pl.multiple_of(column, width), width), :]
        return lax.dot_general(hidden[k], rows, (((1,), (1,)), ((), ())), preferred_element_type=F32)

    def pr_copy(k):
        return rcopy(pair_send.at[k], pair_recv.at[k], pr_s.at[k], pr_r.at[k], "tp", partner)

    def stage_pair(k):
        for j in range(n_x):
            pair_send[k, j] = term(k, j, 1 - core).astype(BF16)
        pr_copy(k).start()
        for j in range(n_x):
            own[k, j] = term(k, j, core)

    def xx_copy(k, j):
        return rcopy(x_send.at[k, j], x_recv.at[k, n_x - j], xx_s.at[k, j], xx_r.at[k, n_x - j],
                     "tp", chip_at(j) * 2 + core)

    def xx_arrival(k, j):
        return rcopy(x_send.at[k, j], x_recv.at[k, j], xx_s.at[k, j], xx_r.at[k, j],
                     "tp", chip_at(j) * 2 + core)

    def stage_chip(k):
        pr_copy(k).wait_recv()
        for j in range(1, n_x):
            x_send[k, j] = (own[k, j] + pair_recv[k, j].astype(F32)).astype(BF16)
            xx_copy(k, j).start()
        own[k, 0] = own[k, 0] + pair_recv[k, 0].astype(F32)

    def rt_copy(k):
        return rcopy(result.at[k], ret.at[f], rt_s.at[k], rt_r.at[n_fs - k], "fs", fs_at(k))

    def rt_arrival(k):
        return rcopy(result.at[k], ret.at[fs_at(k)], rt_s.at[k], rt_r.at[k], "fs", fs_at(k))

    def total(k):
        acc = own[k, 0]
        for j in range(1, n_x):
            xx_arrival(k, j).wait_recv()
            acc = acc + x_recv[k, j].astype(F32)
        return acc.astype(BF16)

    def stage_home(k):
        result[k] = total(k)
        rt_copy(k).start()

    def order(i):
        return lax.rem(outward(i) + n_fs, n_fs)

    stage_pair(order(0))

    def pair_and_chip(i):
        stage_pair(order(i + 1))
        stage_chip(order(i))

    each(n_fs - 1, pair_and_chip)
    stage_chip(order(n_fs - 1))
    each(n_fs - 1, lambda i: stage_home(order(i)))
    ret[f] = total(0)
    mix[...] = blend(0)

    def collect(i):
        k = nearest(i)
        rt_arrival(k).wait_recv()
        mix[...] += blend(k)

    each(n_fs - 1, collect)
    mixed[...] = mix[...].astype(BF16)

    def drain_peer(i):
        k = i + 1
        slot_copy(k, f).wait_send()
        rt_copy(k).wait_send()
        for m in range(3):
            wz_copy(m, k).wait_send()
            for j in range(1, n_grp):
                wy_copy(m, k, j).wait_send()

    def drain_chunk(k):
        gd_copy(k).wait_send()
        pr_copy(k).wait_send()
        for j in range(1, n_x):
            gx_copy(k, j).wait_send()
            gf_copy(k, j).wait_send()
            xx_copy(k, j).wait_send()

    each(n_fs - 1, drain_peer)
    each(n_fs, drain_chunk)


def body(
    tokens, norm_gain, gate_weight, up_weight, down_weight, expert_ids, group_logits, pair_logits
):
    n_grp, n_fs, n_tp = (lax.axis_size(a) for a in ("grp", "fs", "tp"))
    n_x = n_tp // 2
    experts, block, hid = gate_weight.shape
    tok_rows, width = tokens.shape
    capacity = 5 * tok_rows * 2 // (4 * experts)
    cap = -(-capacity // 16) * 16
    vmem = pl.BlockSpec(memory_space=pltpu.VMEM)
    hbm = pl.BlockSpec(memory_space=pl.ANY)
    dma = pltpu.SemaphoreType.DMA
    matrix = jax.ShapeDtypeStruct((n_fs * block, hid), BF16)
    chunk = (n_fs, n_x, cap, width)
    sem_shapes = [
        (4,), (3,), (n_fs,), (n_fs,), (3, n_fs), (3, n_fs), (3, n_fs, n_grp), (3, n_fs, n_grp),
        (n_fs, n_x), (n_fs, n_x), (n_fs,), (n_fs,), (n_fs, n_x), (n_fs, n_x),
        (n_fs,), (n_fs,), (n_fs, n_x), (n_fs, n_x), (n_fs,), (n_fs,),
    ]
    mixed, *matrices = pl.pallas_call(
        functools.partial(exchange_kernel, n_grp, n_fs, n_tp, capacity),
        out_shape=(jax.ShapeDtypeStruct((tok_rows, width), BF16), matrix, matrix, matrix),
        in_specs=[vmem] * 5 + [hbm] * 3,
        out_specs=(vmem,) * 4,
        scratch_shapes=[
            pltpu.VMEM((n_fs, cap, width), BF16),
            pltpu.VMEM((3, n_fs, block, hid), F32),
            pltpu.VMEM((3, n_fs, block, hid), BF16),
            pltpu.VMEM((n_fs, cap, width), BF16),
            pltpu.VMEM((tok_rows, width), F32),
            pltpu.VMEM((n_tp, n_fs, cap, width), BF16),
            pltpu.VMEM((n_fs, cap, hid), BF16),
            pltpu.VMEM(chunk, F32),
            pltpu.VMEM(chunk, BF16),
            pltpu.VMEM(chunk, BF16),
            pltpu.VMEM(chunk, BF16),
            pltpu.VMEM(chunk, BF16),
            pltpu.VMEM((n_fs, cap, width), BF16),
        ] + [dma(s) for s in sem_shapes],
        compiler_params=pltpu.CompilerParams(
            collective_id=0, has_side_effects=True, vmem_limit_bytes=48 * 1024 * 1024
        ),
    )(
        tokens, norm_gain[:, None], expert_ids.T, group_logits.T, pair_logits.T,
        gate_weight, up_weight, down_weight,
    )
    return (mixed, *(m[None] for m in matrices))


def pair_kernel(
    n_grp, n_fs, n_tp, capacity, chunk,
    tokens_in, gain_in, ids_in, group_in, pair_in, gate_in, up_in, down_in,
    mixed, gate_out, up_out, down_out,
    tokens, gain, id_rows, group_logits, pair_logits, gain_col,
    raw_own, raw_far, cast, slots, place, back_place, wsend, wrecv, wcol,
    piece, acc, hid, dwn, part_send, part_recv, keep, home_send, back, mix,
    in_sem, raw_sem, send, sl_r, wm_r, wd_r, wz_r, wy_r, tx_r, td_r, tf_r,
    dw_r, hx_r, hd_r, hf_r, pt_r, hm_r,
):
    g, f, t = lax.axis_index("grp"), lax.axis_index("fs"), lax.axis_index("tp")
    cap, width = piece.shape[2], piece.shape[3]
    block, hidden_units = raw_own.shape[1], raw_own.shape[2]
    share = raw_far.shape[2]
    tok_rows = tokens.shape[0]
    lanes = place.shape[1]
    pair = n_fs // 2

    inner = (f == 1) | (f == 2)

    def flip(i, k):
        return (i, i + 1 - 2 * lax.rem(i, 2), lax.rem(i + 2, 4), 3 - i)[k]

    def fs_at(k):
        if isinstance(k, int):
            return flip(f, k)
        return jnp.where(k == 1, flip(f, 1), jnp.where(k == 2, flip(f, 2), flip(f, 3)))

    def by_role(at_inner, at_outer):
        return jnp.where(inner, at_inner, at_outer)

    def tp_at(j):
        return flip(t, j)

    other_grp = 1 - g

    def rcopy(src, dst, ssem, rsem, axis, peer):
        return pltpu.make_async_remote_copy(
            src_ref=src, dst_ref=dst, send_sem=ssem, recv_sem=rsem,
            device_id={axis: peer}, device_id_type=MESH,
        )

    def all_sent(index, ref):
        rcopy(ref, ref, send.at[index], send.at[index], "fs", fs_at(1)).wait_send()

    def all_here(sem, ref):
        rcopy(ref, ref, sem, sem, "fs", fs_at(1)).wait_recv()

    small = [
        pltpu.make_async_copy(src, dst, in_sem.at[i])
        for i, (src, dst) in enumerate((
            (ids_in, id_rows), (tokens_in, tokens), (gain_in, gain),
            (group_in, group_logits), (pair_in, pair_logits),
        ))
    ]
    w_in = (gate_in, up_in, down_in)
    w_out = (gate_out, up_out, down_out)

    def far_load(m, k):
        return pltpu.make_async_copy(
            w_in[m].at[fs_at(k), pl.ds(g * share, share)], raw_far.at[m, k - 1], raw_sem.at[m, 1]
        )

    def far_loaded(m):
        whole = w_in[m].at[pl.ds(0, 3), pl.ds(0, share)]
        pltpu.make_async_copy(whole, raw_far.at[m], raw_sem.at[m, 1]).wait()

    def own_load(m):
        return pltpu.make_async_copy(w_in[m].at[f], raw_own.at[m], raw_sem.at[m, 0])

    for copy in small:
        copy.start()
    for m in (2, 0, 1):
        for k in (1, 2, 3):
            far_load(m, k).start()
    for m in (2, 0, 1):
        own_load(m).start()

    barrier = pltpu.get_barrier_semaphore()

    def greet(axis, peer):
        pl.semaphore_signal(barrier, inc=1, device_id={axis: peer}, device_id_type=MESH)

    for k in (1, 2, 3):
        greet("fs", fs_at(k))
        greet("tp", tp_at(k))
    greet("grp", other_grp)

    cuts = wz_r.shape[2]

    def cuts_of(m):
        return range(1 if m == 2 else cuts)

    def piece_rows(m):
        return share if m == 2 else share // cuts

    def w_rows(source, part, m, h):
        return pl.ds(source * block + part * share + h * piece_rows(m), piece_rows(m))

    def far_rows(m, k, h):
        return cast.at[m, k - 1, pl.ds(h * piece_rows(m), piece_rows(m))]

    def wz_sem(m, k, h):
        return wd_r.at[k - 1] if m == 2 else wz_r.at[m, k - 1, h]

    def wz_copy(m, k, h):
        return rcopy(far_rows(m, k, h), w_out[m].at[w_rows(f, g, m, h)],
                     send.at[2], wz_sem(m, k, h), "fs", fs_at(k))

    def wz_arrival(m, k, h):
        return rcopy(far_rows(m, k, h), w_out[m].at[w_rows(fs_at(k), g, m, h)],
                     send.at[2], wz_sem(m, k, h), "fs", fs_at(k))

    def wy_sem(m, k):
        return wy_r.at[0] if m == 2 else wy_r.at[k]

    def wy_copy(m, k, h):
        rows = w_out[m].at[w_rows(fs_at(k), g, m, h)]
        return rcopy(rows, rows, send.at[2], wy_sem(m, k), "grp", other_grp)

    def wy_arrival(m, k, h):
        rows = w_out[m].at[w_rows(fs_at(k), other_grp, m, h)]
        return rcopy(rows, rows, send.at[2], wy_sem(m, k), "grp", other_grp)

    def ints(shape, axis):
        return lax.broadcasted_iota(jnp.int32, shape, axis)

    own_base = (f - lax.rem(f, 2))
    far_base = lax.rem(own_base + 2, 4)
    bases = (own_base, far_base)

    with scope("small_0_wait"):
        small[0].wait()
    first, second = id_rows[0:1, :], id_rows[1:2, :]
    members = [(first >= b) & (first < b + 2) for b in bases]
    square = (tok_rows, tok_rows)
    earlier = (ints(square, 0) < ints(square, 1)).astype(F32).astype(BF16)
    named = jnp.where(ints((8, tok_rows), 0) < 4, members[0].astype(F32), members[1].astype(F32))
    before = jnp.dot(named.astype(BF16), earlier, preferred_element_type=F32)
    ranks = [before[0:1, :], before[4:5, :]]
    kept = [m & (r < capacity) for m, r in zip(members, ranks)]
    seat = [jnp.where(k, r.astype(jnp.int32), -1) for k, r in zip(kept, ranks)]

    with scope("small_1_wait"):
        small[1].wait()

    def fill(i):
        one_hot = jnp.where(ints((lanes, tok_rows), 0) == seat[i], 1.0, 0.0)
        place[i] = one_hot.astype(BF16)
        rows = jnp.dot(place[i, 0:cap, :], tokens[...], preferred_element_type=F32).astype(BF16)
        slots[i] = rows
        return rows

    def slot_copy(k):
        src = slots.at[0] if k == 1 else slots.at[1]
        return rcopy(src, piece.at[t, k], send.at[0], sl_r.at[k], "fs", fs_at(k))

    def relay_copy():
        return rcopy(piece.at[t, 2], piece.at[t, 3], send.at[0], sl_r.at[3], "fs", fs_at(1))

    fill(1)
    with scope("barrier"):
        pl.semaphore_wait(barrier, 3 + 3 + 1)
    slot_copy(2).start()
    piece[t, 0] = fill(0)
    slot_copy(1).start()

    def tx_copy(k):
        src = piece.at[t, k]
        return rcopy(src, src, send.at[1], tx_r.at[k], "tp", tp_at(2))

    def td_copy(k):
        src = piece.at[t, k]
        return rcopy(src, src, send.at[1], td_r.at[k // 3], "tp", tp_at(1))

    def tf_copy(k):
        src = piece.at[tp_at(2), k]
        return rcopy(src, src, send.at[1], tf_r.at[k // 3], "tp", tp_at(1))

    def tx_arrival(k):
        src = piece.at[tp_at(2), k]
        return rcopy(src, src, send.at[1], tx_r.at[k], "tp", tp_at(2))

    def td_arrival(k):
        src = piece.at[tp_at(1), k]
        return rcopy(src, src, send.at[1], td_r.at[k // 3], "tp", tp_at(1))

    def tf_arrival(k):
        src = piece.at[tp_at(3), k]
        return rcopy(src, src, send.at[1], tf_r.at[k // 3], "tp", tp_at(1))

    def spread(k):
        tx_copy(k).start()
        td_copy(k).start()

    spread(0)

    small[2].wait()
    gain_col[...] = jnp.transpose(jnp.broadcast_to(gain[...], (8, block)))[:, 0:1]
    far_gain = gain_col[pl.ds(g * share, share), :]

    def send_far(m, k):
        with scope("far_load_m_k_wait"):
            cast[m, k - 1] = (far_gain * raw_far[m, k - 1]).astype(BF16)
        for h in cuts_of(m):
            wz_copy(m, k, h).start()

    def round_own(m):
        with scope("own_load_m_wait"):
            own_load(m).wait()
        values = raw_own[m]
        if m < 2:
            values = gain_col[...] * values
        w_out[m][pl.ds(f * block, block), :] = values.astype(BF16)

    far_loaded(2)
    for k in (1, 2, 3):
        cast[2, k - 1] = raw_far[2, k - 1].astype(BF16)
        wz_copy(2, k, 0).start()
    far_loaded(0)
    far_loaded(1)

    with scope("small_3_wait"):
        small[3].wait()
    with scope("small_4_wait"):
        small[4].wait()
    group_exp = jnp.exp(group_logits[...])
    group_sum = jnp.sum(group_exp, axis=0, keepdims=True)
    pair_exp = jnp.exp(pair_logits[...])
    pair_weight = pair_exp / jnp.sum(pair_exp, axis=0, keepdims=True)
    group_count = group_exp.shape[0]

    def wm_copy(k):
        return rcopy(wsend.at[k // 2], wrecv.at[k], send.at[3], wm_r.at[0], "fs", fs_at(k))

    chosen = jnp.zeros_like(group_sum)
    for i in range(group_count):
        chosen = chosen + jnp.where((first >= 2 * i) & (first < 2 * i + 2), group_exp[i : i + 1, :], 0.0)
    mix_weight = pair_weight * (chosen / group_sum)
    for i in range(2):
        expert = bases[i] + ints((8, tok_rows), 0)
        rest = jnp.where(first == expert, mix_weight[0:1, :], 0.0)
        rest = rest + jnp.where(second == expert, mix_weight[1:2, :], 0.0)
        total = None
        for _ in range(3):
            head = rest.astype(BF16)
            rest = rest - head.astype(F32)
            term = lax.dot_general(head, place[i], (((1,), (1,)), ((), ())), preferred_element_type=F32)
            total = term if total is None else total + term
        wsend[i] = total
    for k in (1, 2, 3):
        wm_copy(k).start()

    def slot_arrival(k):
        return rcopy(slots.at[0], piece.at[t, k], send.at[0], sl_r.at[k], "fs", fs_at(k))

    with scope("cross"):
        slot_arrival(2).wait_recv()
    relay_copy().start()
    spread(2)
    for k in (1, 2, 3):
        for m in (0, 1):
            send_far(m, k)

    def hand_over(k):
        with scope("hand%d" % k):
            tx_arrival(k).wait_recv()
        tf_copy(k).start()

    def forward(m, k, h):
        with scope("forward%d%d%d" % (m, k, h)):
            wz_arrival(m, k, h).wait_recv()
        wy_copy(m, k, h).start()

    def forward_all(steps, more):
        @pl.when(inner)
        def _():
            for step in steps:
                forward(*step)

        @pl.when(jnp.logical_not(inner))
        def _():
            for step in more:
                forward(*step)

    def arrived(k):
        with scope("arrived"):
            all_here(wy_r.at[k], gate_out.at[pl.ds(0, 2 * share)])

    def land(k):
        with scope("land%d" % k):
            slot_arrival(k).wait_recv()
        spread(k)

    def seat_weights(k, rows):
        cols = jnp.transpose(rows)
        wcol[k] = jnp.where(lax.rem(f, 2) == 0, cols[0:cap, 0:1], cols[0:cap, 1:2])

    hand_over(0)
    round_own(2)
    for i in range(2):
        back_place[i] = jnp.transpose(place[i].astype(F32))[:, 0:cap].astype(BF16)
    seat_weights(0, wsend[0])
    land(1)
    for k in (2, 1, 3):
        forward(2, k, 0)
    hand_over(2)
    hand_over(1)
    for m in (0, 1):
        round_own(m)

    def dw_copy(j):
        src = down_out.at[pl.ds(tp_at(j) * block, block)]
        return rcopy(src, dwn.at[j], send.at[4], dw_r.at[0], "tp", tp_at(j))

    with scope("down_in"):
        all_here(wy_r.at[0], down_out.at[pl.ds(0, 3 * share)])
    for j in (3, 2, 1):
        dw_copy(j).start()
    def steps(*turns):
        return [(m, k, h) for k in turns for m in (0, 1) for h in cuts_of(m)]

    turns = (by_role(1, 2), by_role(2, 1), 3)
    forward_all(steps(1), steps(2))
    land(3)
    forward_all(steps(2), steps(1))
    with scope("weights_in"):
        all_here(wm_r.at[0], wrecv.at[pl.ds(1, 3)])
        for k in (1, 2, 3):
            seat_weights(k, wrecv[k])
    with scope("rows_in"):
        all_here(td_r.at[0], piece.at[t, pl.ds(0, 3)])
        all_here(tf_r.at[0], piece.at[t, pl.ds(0, 3)])

    def products(k, source):
        rows = piece[source, k]
        cols = pl.ds(source * block, block)
        gate = jnp.dot(rows, gate_out[cols, :], preferred_element_type=F32)
        up = jnp.dot(rows, up_out[cols, :], preferred_element_type=F32)
        return gate, up

    def first_products(k, c):
        gate, up = products(k, f)
        acc[0, k], acc[1, k] = gate, up
        return c

    def more_products(kk):
        def step(k, c):
            gate, up = products(k, fs_at(kk))
            acc[0, k] += gate
            acc[1, k] += up
            return c
        return step

    def multiply(step, blocks):
        with scope("products"):
            lax.fori_loop(*blocks, step, 0)

    first = (0, n_fs - 1)
    multiply(first_products, first)
    arrived(turns[0])
    multiply(more_products(turns[0]), first)
    forward_all(steps(3), steps(3))
    hand_over(3)
    arrived(turns[1])
    multiply(more_products(turns[1]), first)
    with scope("rows_in"):
        all_here(td_r.at[1], piece.at[t, 3])
        all_here(tf_r.at[1], piece.at[t, 3])
    first_products(3, 0)
    more_products(turns[0])(3, 0)
    more_products(turns[1])(3, 0)
    arrived(turns[2])

    edges = (0, *chunk, cap)
    spans = [pl.ds(a, b - a) for a, b in zip(edges, edges[1:])]
    parts = range(len(spans))

    def h_copy(j, k, c, ssem, rsem, source):
        src, dst = hid.at[source, k, spans[c]], hid.at[source ^ j, k, spans[c]]
        return rcopy(src, dst, ssem, rsem, "tp", tp_at(j))

    def hx_copy(k, c):
        return h_copy(2, k, c, send.at[5], hx_r.at[k, c], 0)

    def hd_copy(k, c):
        return h_copy(1, k, c, send.at[5], hd_r.at[k], 0)

    def hf_copy(k, c):
        return h_copy(1, k, c, send.at[5], hf_r.at[k, c], 2)

    last = fs_at(turns[2])
    blocks = (by_role(1, 3), 2, by_role(3, 1), 0)
    def diagonal_copy(k, c):
        src, dst = hid.at[0, k, spans[c]], hid.at[3, k, spans[c]]
        return rcopy(src, dst, send.at[5], hf_r.at[k, c], "tp", tp_at(3))

    direct = 1

    def launch(i):
        for c in parts:
            if i == 0 and c < direct:
                diagonal_copy(blocks[i], c).start()
            hx_copy(blocks[i], c).start()

    for k in blocks:
        with scope("hidden"):
            gate, up = products(k, last)
            gate = acc[0, k] + gate
            up = acc[1, k] + up
            hid[0, k] = (gate / (1.0 + jnp.exp(-gate)) * up * wcol[k]).astype(BF16)
            if k is blocks[0]:
                launch(0)
            for c in parts:
                hd_copy(k, c).start()

    with scope("drain"):
        all_here(dw_r.at[0], dwn.at[pl.ds(1, 3)])
        all_sent(0, piece.at[t, pl.ds(0, 3)])
        all_sent(1, piece.at[pl.ds(0, 3)])
        all_sent(2, raw_far)
        all_sent(3, wrecv.at[pl.ds(1, 3)])
        all_sent(4, dwn.at[pl.ds(1, 3)])

    queue = [(k, c) for k in blocks for c in parts]

    def pass_on(n):
        if n < len(queue):
            with scope("hx"):
                hx_copy(*queue[n]).wait_recv()
            if n >= direct:
                hf_copy(*queue[n]).start()

    def result(n):
        k, c = queue[n]

        def term(j):
            rows = down_out[pl.ds(t * block, block), :] if j == 0 else dwn[j]
            return lax.dot_general(
                hid[j, k, spans[c], :], rows, (((1,), (1,)), ((), ())), preferred_element_type=F32)

        if c == 0:
            with scope("hd"):
                all_here(hd_r.at[k], hid.at[1, k])
        total = term(0) + term(1)
        if n == 0:
            pass_on(0)
        total = total + term(2)
        if n > 0:
            pass_on(n + 1)
        with scope("hf"):
            hf_copy(k, c).wait_recv()
        total = total + term(3)
        if n == 0:
            launch(1)
            pass_on(1)
        return total

    def part_copy(i, c):
        return rcopy(part_send.at[i, spans[c]], part_recv.at[i, spans[c]],
                     send.at[6 + i // 2], pt_r.at[i, c], "fs", fs_at(1))

    def home_copy(i, c):
        return rcopy(home_send.at[i, spans[c]], back.at[1, spans[c]],
                     send.at[8], hm_r.at[0], "fs", fs_at(2 + i))

    def home_step(n):
        if n < 0 or n >= 2 * len(parts):
            return
        i, c = divmod(n, len(parts))

        @pl.when(inner)
        def _():
            with scope("part%d" % i):
                part_copy(i, c).wait_recv()
            both = keep[i + 1, spans[c], :] + part_recv[i, spans[c], :].astype(F32)
            home_send[i, spans[c], :] = both.astype(BF16)
            home_copy(i, c).start()

    for n in range(len(queue)):
        i, c = divmod(n, len(parts))
        if c == 0 and i in (1, 2):
            launch(i + 1)
        keep[i, spans[c], :] = result(n)

        def send_part(to):
            part_send[to, spans[c], :] = keep[i, spans[c], :].astype(BF16)
            part_copy(to, c).start()

        if i < 3:
            pl.when(jnp.logical_not(inner))(functools.partial(send_part, i))
        if i == 0:
            pl.when(inner)(functools.partial(send_part, 2))
        home_step(n - len(parts) - 1)

    def finish_own():
        for c in parts:
            with scope("part2"):
                part_copy(2, c).wait_recv()
            both = keep[3, spans[c], :] + part_recv[2, spans[c], :].astype(F32)
            back[0, spans[c], :] = both.astype(BF16)

    def finish_far():
        with scope("home"):
            all_here(hm_r.at[0], back.at[1])

    pl.when(inner)(finish_own)
    pl.when(jnp.logical_not(inner))(finish_far)
    sooner, later = by_role(0, 1), by_role(1, 0)
    mix[...] = jnp.dot(back_place[sooner], back[sooner], preferred_element_type=F32)
    pl.when(inner)(finish_far)
    pl.when(jnp.logical_not(inner))(finish_own)
    with scope("last_dot"):
        more = jnp.dot(back_place[later], back[later], preferred_element_type=F32)
        mixed[...] = (mix[...] + more).astype(BF16)

    all_sent(5, hid.at[pl.ds(0, 3)])
    all_sent(7, part_send.at[2])

    @pl.when(inner)
    def _():
        all_sent(8, home_send)

    @pl.when(jnp.logical_not(inner))
    def _():
        all_sent(6, part_send.at[pl.ds(0, 2)])


def pair_body(
    tokens, norm_gain, gate_weight, up_weight, down_weight, expert_ids, group_logits, pair_logits
):
    n_grp, n_fs, n_tp = (lax.axis_size(a) for a in ("grp", "fs", "tp"))
    experts, block, hid = gate_weight.shape
    tok_rows, width = tokens.shape
    share = block // n_grp
    capacity = 5 * tok_rows * 2 // (4 * experts)
    cap = -(-capacity // 16) * 16
    lanes = -(-cap // 128) * 128
    vmem = pl.BlockSpec(memory_space=pltpu.VMEM)
    hbm = pl.BlockSpec(memory_space=pltpu.HBM)
    dma = pltpu.SemaphoreType.DMA
    matrix = jax.ShapeDtypeStruct((n_fs * block, hid), BF16)
    rows = (cap, width)
    chunk = (cap // 80 * 16, cap // 80 * 16 * 2, cap // 80 * 16 * 3)
    spans = len(chunk) + 1
    sem_shapes = [
        (5,), (3, 2), (9,), (n_fs,), (1,), (n_fs - 1,), (2, n_fs - 1, 4), (n_fs,), (n_fs,), (2,), (2,),
        (1,), (n_fs, spans), (n_fs,), (n_fs, spans), (3, spans), (1,),
    ]
    mixed, *matrices = pl.pallas_call(
        functools.partial(pair_kernel, n_grp, n_fs, n_tp, capacity, chunk),
        out_shape=(jax.ShapeDtypeStruct((tok_rows, width), BF16), matrix, matrix, matrix),
        in_specs=[hbm] * 8,
        out_specs=(vmem,) * 4,
        scratch_shapes=[
            pltpu.VMEM((tok_rows, width), BF16),
            pltpu.VMEM((1, block), F32),
            pltpu.VMEM((2, tok_rows), jnp.int32),
            pltpu.VMEM((group_logits.shape[1], tok_rows), F32),
            pltpu.VMEM((2, tok_rows), F32),
            pltpu.VMEM((block, 1), F32),
            pltpu.VMEM((3, block, hid), F32),
            pltpu.VMEM((3, n_fs - 1, share, hid), F32),
            pltpu.VMEM((3, n_fs - 1, share, hid), BF16),
            pltpu.VMEM((2, *rows), BF16),
            pltpu.VMEM((2, lanes, tok_rows), BF16),
            pltpu.VMEM((2, tok_rows, cap), BF16),
            pltpu.VMEM((2, 8, lanes), F32),
            pltpu.VMEM((n_fs, 8, lanes), F32),
            pltpu.VMEM((n_fs, cap, 1), F32),
            pltpu.VMEM((n_tp, n_fs, *rows), BF16),
            pltpu.VMEM((2, n_fs, cap, hid), F32),
            pltpu.VMEM((n_tp, n_fs, cap, hid), BF16),
            pltpu.VMEM((n_tp, block, hid), BF16),
            pltpu.VMEM((3, *rows), BF16),
            pltpu.VMEM((3, *rows), BF16),
            pltpu.VMEM((n_fs, *rows), F32),
            pltpu.VMEM((2, *rows), BF16),
            pltpu.VMEM((2, *rows), BF16),
            pltpu.VMEM((tok_rows, width), F32),
        ] + [dma(s) for s in sem_shapes],
        compiler_params=pltpu.CompilerParams(
            collective_id=0, has_side_effects=True, vmem_limit_bytes=40 * 1024 * 1024
        ),
    )(*(pltpu.with_memory_space_constraint(x, pltpu.HBM) for x in (
        tokens, norm_gain[None, :], expert_ids.T, group_logits.T, pair_logits.T,
        gate_weight, up_weight, down_weight,
    )))
    return write_out(mixed, *matrices)


def write_kernel(mixed, gate, up, down, *rest):
    outs, sem = rest[:4], rest[4]
    pairs = (
        (gate, outs[1].at[0]), (up, outs[2].at[0]), (down, outs[3].at[0]), (mixed, outs[0])
    )
    for i, (src, dst) in enumerate(pairs):
        rows = src.shape[0] // 4
        for c in range(4):
            at = pl.ds(c * rows, rows)
            pltpu.make_async_copy(src.at[at], dst.at[at], sem.at[i]).start()
    for i, (src, dst) in enumerate(pairs):
        pltpu.make_async_copy(src, dst, sem.at[i]).wait()


def write_out(mixed, *matrices):
    return pl.pallas_call(
        write_kernel,
        out_shape=(
            jax.ShapeDtypeStruct(mixed.shape, BF16),
            *(jax.ShapeDtypeStruct((1, *m.shape), BF16) for m in matrices),
        ),
        in_specs=[pl.BlockSpec(memory_space=pltpu.VMEM)] * 4,
        out_specs=(pl.BlockSpec(memory_space=pltpu.HBM),) * 4,
        scratch_shapes=[pltpu.SemaphoreType.DMA((4,))],
        compiler_params=pltpu.CompilerParams(vmem_limit_bytes=1024 * 1024),
    )(mixed, *matrices)


def paired(mesh, tokens, gate_weight, expert_ids, group_logits):
    n_grp, n_fs, n_tp = (mesh.shape[a] for a in ("grp", "fs", "tp"))
    experts, features, _ = gate_weight.shape
    return (
        experts // group_logits.shape[1] == expert_ids.shape[1] == 2
        and n_fs == n_tp == experts == 4
        and n_grp == 2
    )


def solution(mesh):
    placed = (
        P(("grp", "fs"), "tp"),
        P("fs"),
        P(None, "fs", "tp"),
        P(None, "fs", "tp"),
        P(None, "fs", "tp"),
        P(("grp", "fs"), None),
        P(("grp", "fs"), None),
        P(("grp", "fs"), None),
    )

    def run(tokens, norm_gain, gate_weight, up_weight, down_weight, expert_ids, group_logits, pair_logits):
        args = (tokens, norm_gain, gate_weight, up_weight, down_weight, expert_ids, group_logits, pair_logits)
        special = paired(mesh, tokens, gate_weight, expert_ids, group_logits)
        return jax.shard_map(
            pair_body if special else body,
            mesh=mesh,
            in_specs=placed,
            out_specs=(
                P(("grp", "fs"), "tp"),
                P(("grp", "fs"), None, "tp"),
                P(("grp", "fs"), None, "tp"),
                P(("grp", "fs"), None, "tp"),
            ),
            check_vma=False,
        )(*args)

    return run
```
